512 devices in a mesh: dp: 4 (over x), kv: 64 (over z, y), tp: 2 (over core).
Axes of the slice: x: 4, y: 4, z: 16, core: 2. Of those that a mesh axis runs over, the one named last changes fastest.
Arguments:
- residual: bfloat16 [32, 2048], P('dp', ('kv', 'tp')), may hold values from -6 to 6
- norm_gains: float32 [3, 2048], replicated, may hold values from 0.1 to 1.9
- ffn_gate: bfloat16 [2, 5632, 2048], P(None, ('kv', 'tp')), may hold values from -0.125 to 0.125
- ffn_up: bfloat16 [2, 5632, 2048], P(None, ('kv', 'tp')), may hold values from -0.125 to 0.125
- ffn_down: bfloat16 [2, 5632, 2048], P(None, ('kv', 'tp')), may hold values from -0.1875 to 0.1875
- proj_query: bfloat16 [2048, 1024], P('kv', 'tp'), may hold values from -0.44194174 to 0.44194174
- proj_key: bfloat16 [2048, 256], P('kv', 'tp'), may hold values from -0.125 to 0.125
- proj_value: bfloat16 [2048, 256], P('kv', 'tp'), may hold values from -0.125 to 0.125
- proj_out: bfloat16 [1024, 2048], P('tp', 'kv'), may hold values from -0.1875 to 0.1875
- head_lambda: float32 [8], P('tp'), may hold values from 0.3 to 0.8
- head_gain: float32 [128], replicated, may hold values from 0.1 to 1.9
- cache_keys: bfloat16 [32, 16384, 2, 128], P('dp', 'kv', 'tp'), may hold values from -12 to 12
- cache_values: bfloat16 [32, 16384, 2, 128], P('dp', 'kv', 'tp'), may hold values from -6 to 6
- live_length: int32 [32], P('dp'), may hold values from 1 to 16384, 131072 in all
Outputs:
- updated: bfloat16 [32, 2048], P('dp', ('kv', 'tp'))
The draws below stay inside these ranges and needn't reach their ends.
Inputs may be any that keep to these rules, and one draw needn't show every extreme that they name: `live_length`: the largest length of every draw equals 16384.
All inputs are finite; a program needn't handle non-finite values. No bound on the sum of `live_length` on one device may be relied on, other than what follows from the above.
Results may differ from the reference program's by a relative error of at most 0.014.
The reference program's roundings to bfloat16 on the way count: a program that leaves them out, or rounds other values in their place, can miss the bound.
Values may be sent and summed in bfloat16 or wider, within the bound.
A program may use at most 64 MiB of HBM per device.

```python
import math
import jax
import jax.numpy as jnp
import numpy as np
from jax import lax

D = 2048
FF = 5632
HEADS = 8
KV_HEADS = 2
HEAD = 64
VDIM = 128
P_DEV = 256
BATCH = 32
CTX = 16384
N_KV = 64


def sign_table(key):
    picked = jax.random.randint(jax.random.fold_in(key, 7001), (KV_HEADS, 2, HEAD), 0, 2)
    return (2 * picked - 1).astype(jnp.float32)


def draw_proj_query(key, part):
    shape_full = (D, HEADS, 2, HEAD)
    base_noise = jnp.clip(jax.random.normal(jax.random.fold_in(key, 7011), shape_full, jnp.float32), -4.0, 4.0)
    lift_rows = jnp.clip(jax.random.normal(jax.random.fold_in(key, 7012), (D, HEADS, 2), jnp.float32), -4.0, 4.0)
    head_signs = jnp.repeat(sign_table(key), HEADS // KV_HEADS, axis=0)
    strength = 16.0 / math.sqrt(HEAD)
    combined = (base_noise + strength * lift_rows[..., None] * head_signs[None]) * D ** (-0.5)
    limit_value = 20.0 * D ** (-0.5)
    combined = jnp.clip(combined, -limit_value, limit_value)
    return combined.reshape(D, HEADS * 2 * HEAD).astype(jnp.bfloat16)


def draw_cache_keys(key, part):
    shape_full = (BATCH, CTX, KV_HEADS, 2, HEAD)
    background = jnp.clip(1.2 * jax.random.normal(jax.random.fold_in(key, 7021), shape_full, jnp.float32), -6.0, 6.0)
    lowest_level = 4.0
    block_count = CTX // P_DEV
    small_shape = (BATCH, block_count, KV_HEADS, 2)
    offsets = jax.random.randint(jax.random.fold_in(key, 7022), small_shape, 0, P_DEV - 1)
    levels = jax.random.uniform(jax.random.fold_in(key, 7023), small_shape, jnp.float32, lowest_level, 10.0)
    level_drop = jax.random.uniform(jax.random.fold_in(key, 7024), small_shape, jnp.float32, 0.05, 0.15)
    offsets_full = jnp.repeat(offsets, P_DEV, axis=1)
    levels_full = jnp.repeat(levels, P_DEV, axis=1)
    drop_full = jnp.repeat(level_drop, P_DEV, axis=1)
    within = (jnp.arange(CTX, dtype=jnp.int32) % P_DEV)[None, :, None, None]
    first_key = within == offsets_full
    second_key = within == offsets_full + 1
    height = jnp.where(first_key, levels_full, jnp.where(second_key, levels_full - drop_full, 0.0))
    planted = height[..., None] * sign_table(key)[None, None] + 0.25 * background
    chosen = jnp.where((first_key | second_key)[..., None], planted, background)
    chosen = jnp.clip(chosen, -12.0, 12.0)
    return chosen.reshape(BATCH, CTX, KV_HEADS, 2 * HEAD).astype(jnp.bfloat16)


def level_of(rng, shape, pieces, low, top_value):
    level = 1.0
    for dim, shards_of in pieces:
        steps = jax.random.uniform(jax.random.fold_in(jax.random.fold_in(rng, 6), dim), (shards_of,), jnp.float32, low / len(pieces), top_value / len(pieces))
        level = level * jnp.repeat(jnp.exp(steps), shape[dim] // shards_of).reshape((-1,) + (1,) * (len(shape) - 1 - dim))
    return level


def length_profile(count, total, most, skew):
    portions = [(1 << 20) // math.isqrt(grade ** skew) + 1 for grade in range(2, count + 1)]
    spare, counts = total - most - (count - 1), [1] * (count - 1)
    while spare > 0:
        movable = [i for i in range(count - 1) if counts[i] < most]
        pool, budget = sum([portions[i] for i in movable]), spare
        for i in movable:
            more = min(most - counts[i], max(1, budget * portions[i] // pool), spare)
            counts[i] = counts[i] + more
            spare = spare - more
    return np.array([most] + counts)


def uneven_parts(key, count, total, most, lean):
    if count == 2:
        one = jax.random.randint(key, (), max(1, total - most), min(most, total - 1) + 1)
        return jnp.stack([one, total - one])
    tallies = jnp.asarray(length_profile(count, total, most, lean), jnp.int32)
    pairs = (count - 1) // 2
    donor, taker = tallies[1:1 + 2 * pairs:2], tallies[2:2 + 2 * pairs:2]
    room = jnp.minimum(donor - 1, most - taker)
    shifted = jax.random.randint(jax.random.fold_in(key, 1), (pairs,), 0, 1 << 20) % (room + 1)
    tallies = tallies.at[1:1 + 2 * pairs:2].set(donor - shifted).at[2:2 + 2 * pairs:2].set(taker + shifted)
    return tallies[jax.random.permutation(jax.random.fold_in(key, 2), count)]


def scatter_about(rng, extent, spread, most, cuts=(), held_as=jnp.bfloat16):
    entries = spread * jax.random.normal(rng, extent, jnp.float32)
    if cuts:
        entries = entries * level_of(rng, extent, cuts, -0.22, 0.18)
    return jnp.clip(entries, -most, most).astype(held_as)


def setup_inputs(seed: int = 0) -> dict:
    key_of = jax.random.split(jax.random.key(seed), 15)
    residual = scatter_about(key_of[0], (BATCH, D), 1.0, 6.0, ((0, 4), (1, 128)))
    norm_gains = jnp.clip(1.0 + 0.18 * jax.random.normal(key_of[1], (3, D), jnp.float32), 0.1, 1.9)
    ffn_gate = scatter_about(key_of[2], (2, FF, D), D ** -0.5, 0.125, ((1, 128),))
    ffn_up = scatter_about(key_of[3], (2, FF, D), D ** -0.5, 0.125, ((1, 128),))
    ffn_down = scatter_about(key_of[4], (2, FF, D), (FF // 6) ** -0.5, 0.1875, ((1, 128),))
    proj_query = draw_proj_query(jax.random.fold_in(key_of[14], 71), 0)
    proj_key = scatter_about(key_of[6], (D, KV_HEADS * 2 * HEAD), D ** -0.5, 0.125, ((0, 64), (1, 2)))
    proj_value = scatter_about(key_of[7], (D, KV_HEADS * VDIM), D ** -0.5, 0.125, ((0, 64), (1, 2)))
    proj_out = scatter_about(key_of[8], (HEADS * VDIM, D), (HEADS * VDIM) ** -0.5, 0.1875, ((0, 2), (1, 64)))
    head_lambda = jnp.clip(0.3 + 0.5 * jax.random.uniform(key_of[9], (HEADS,), jnp.float32) ** level_of(key_of[9], (HEADS,), ((0, 2),), -0.2, 0.2), 0.3, 0.8)
    head_gain = jnp.clip(1.0 + 0.18 * jax.random.normal(key_of[10], (VDIM,), jnp.float32), 0.1, 1.9)
    cache_keys = draw_cache_keys(jax.random.fold_in(key_of[14], 71), 0)
    cache_values = scatter_about(key_of[12], (BATCH, CTX, KV_HEADS, VDIM), 1.0, 6.0, ((0, 4), (1, 64), (2, 2)))
    live_length = uneven_parts(key_of[13], BATCH, BATCH * CTX // 4, CTX, 2).astype(jnp.int32)
    return {"residual": residual, "norm_gains": norm_gains, "ffn_gate": ffn_gate, "ffn_up": ffn_up, "ffn_down": ffn_down, "proj_query": proj_query, "proj_key": proj_key, "proj_value": proj_value, "proj_out": proj_out, "head_lambda": head_lambda, "head_gain": head_gain, "cache_keys": cache_keys, "cache_values": cache_values, "live_length": live_length}


epsilon = 1e-05

def row_scale(row_data):
    data32 = row_data.astype(jnp.float32)
    return lax.rsqrt(lax.optimization_barrier(jnp.mean(data32 * data32, axis=-1, keepdims=True)) + epsilon)

def channel_mix(row_data, gain, gate_part, up_part, down_part):
    normed = (row_data.astype(jnp.float32) * row_scale(row_data) * gain).astype(jnp.bfloat16)
    contract = (((1,), (1,)), ((), ()))
    gate_act = lax.dot_general(normed, gate_part, contract, preferred_element_type=jnp.float32)
    up_act = lax.dot_general(normed, up_part, contract, preferred_element_type=jnp.float32)
    hidden = (jax.nn.silu(gate_act) * up_act).astype(jnp.bfloat16)
    return 0.5 * jnp.dot(hidden, down_part, preferred_element_type=jnp.float32)

def join_parts(earlier, latter):
    highest = jnp.maximum(earlier[0], latter[0])
    weight_early = jnp.exp(earlier[0] - highest)
    weight_late = jnp.exp(latter[0] - highest)
    return (highest, earlier[1] * weight_early + latter[1] * weight_late, earlier[2] * weight_early[..., None] + latter[2] * weight_late[..., None])

def block_softmax(queries, block_keys, block_values, live_mask):
    scores = jnp.einsum('bkgcd,bpkcd->bkgcp', queries.astype(jnp.float32), block_keys.astype(jnp.float32)) * queries.shape[-1] ** (-0.5)
    mask_wide = live_mask[:, None, None, None, :]
    highest = lax.optimization_barrier(jnp.max(jnp.where(mask_wide, scores, -1e+30), axis=-1))
    exp_terms = jnp.where(mask_wide, jnp.exp(scores - highest[..., None]), 0.0)
    totals = lax.optimization_barrier(jnp.sum(exp_terms, axis=-1))
    weights = exp_terms.astype(jnp.bfloat16)
    partial_value = jnp.einsum('bkgcp,bpkv->bkgcv', weights.astype(jnp.float32), block_values.astype(jnp.float32))
    return (highest, totals, partial_value)

def reference(residual, norm_gains, ffn_gate, ffn_up, ffn_down, proj_query, proj_key, proj_value, proj_out, head_lambda, head_gain, cache_keys, cache_values, live_length):
    stream_one = (residual.astype(jnp.float32) + channel_mix(residual, norm_gains[0], ffn_gate[0], ffn_up[0], ffn_down[0])).astype(jnp.bfloat16)
    scaled = (stream_one.astype(jnp.float32) * norm_gains[1]).astype(jnp.bfloat16)
    factor = row_scale(stream_one)
    queries = (jnp.dot(scaled, proj_query, preferred_element_type=jnp.float32) * factor).astype(jnp.bfloat16)
    key_new = (jnp.dot(scaled, proj_key, preferred_element_type=jnp.float32) * factor).astype(jnp.bfloat16)
    value_new = (jnp.dot(scaled, proj_value, preferred_element_type=jnp.float32) * factor).astype(jnp.bfloat16)
    group_size = HEADS // KV_HEADS
    queries = queries.reshape(BATCH, KV_HEADS, group_size, 2, HEAD)
    key_new = key_new.reshape(BATCH, KV_HEADS, 2, HEAD)
    value_new = value_new.reshape(BATCH, KV_HEADS, VDIM)

    def block_step(block_index, running):
        start = (block_index * P_DEV).astype(jnp.int32)
        block_keys = lax.dynamic_slice_in_dim(cache_keys, start, P_DEV, 1).reshape(BATCH, P_DEV, KV_HEADS, 2, HEAD)
        block_values = lax.dynamic_slice_in_dim(cache_values, start, P_DEV, 1)
        positions = start + jnp.arange(P_DEV, dtype=jnp.int32)
        live_mask = positions[None, :] < live_length[:, None]
        return join_parts(running, block_softmax(queries, block_keys, block_values, live_mask))
    lead_shape = (BATCH, KV_HEADS, group_size, 2)
    running = (jnp.full(lead_shape, -1e+30, jnp.float32), jnp.zeros(lead_shape, jnp.float32), jnp.zeros(lead_shape + (VDIM,), jnp.float32))
    running = lax.fori_loop(0, N_KV, block_step, running)
    own_scores = jnp.einsum('bkgcd,bkcd->bkgc', queries.astype(jnp.float32), key_new.astype(jnp.float32)) * HEAD ** (-0.5)
    own_values = jnp.broadcast_to(value_new.astype(jnp.float32)[:, :, None, None, :], lead_shape + (VDIM,))
    highest, totals, accum = join_parts(running, (own_scores, jnp.ones(lead_shape, jnp.float32), own_values))
    ratios = accum / totals[..., None]
    lambdas = head_lambda.reshape(KV_HEADS, group_size)
    mixed_heads = ratios[:, :, :, 0] - lambdas[None, :, :, None] * ratios[:, :, :, 1]
    heads_out = (mixed_heads * row_scale(mixed_heads) * head_gain).astype(jnp.bfloat16).reshape(BATCH, HEADS * VDIM)
    mixer_out = jnp.dot(heads_out, proj_out, preferred_element_type=jnp.float32)
    stream_two = (stream_one.astype(jnp.float32) + mixer_out).astype(jnp.bfloat16)
    return (stream_two.astype(jnp.float32) + channel_mix(stream_two, norm_gains[2], ffn_gate[1], ffn_up[1], ffn_down[1])).astype(jnp.bfloat16)
```

```python
import functools

import jax
import jax.numpy as jnp
from jax import lax
from jax.experimental import pallas as pl
from jax.experimental.pallas import tpu as pltpu
from jax.sharding import Mesh
from jax.sharding import PartitionSpec as P

D = 2048
HEAD = 64
VDIM = 128
NZ = 16
NY = 4
NC = 2
NYC = NY * NC
LANES = 128
KV_TP = ("kv_0", "kv_1", "tp")
KV = ("kv_0", "kv_1")
MESH = pl.DeviceIdType.MESH
F32 = jnp.float32
BF16 = jnp.bfloat16
EPS = 1e-05
NT = (((1,), (1,)), ((), ()))

Z_STEPS = (8, 7, 9, 6, 10, 5, 11, 4, 12, 3, 13, 2, 14, 1, 15)
Y_STEPS = (2, 1, 3)
YC_STEPS = (4, 5, 2, 3, 6, 7, 1)

A1, A2, B1, B2, C1, C2, C3, D1, D2O, D2M, D3, F1, F2, G1, G2 = range(15)


def iota(shape, dim):
    return lax.broadcasted_iota(jnp.int32, shape, dim)


def mix_part(rows, gain, gate_w, up_w, down_w):
    scale = lax.rsqrt(jnp.mean(rows * rows, axis=1, keepdims=True) + EPS)
    normed = (rows * scale * gain).astype(BF16)
    gate = lax.dot_general(normed, gate_w, NT, preferred_element_type=F32)
    up = lax.dot_general(normed, up_w, NT, preferred_element_type=F32)
    hidden = (gate / (1.0 + jnp.exp(-gate)) * up).astype(BF16)
    return 0.5 * jnp.dot(hidden, down_w, preferred_element_type=F32)


def layer_kernel(
    res, gains, gate0, up0, down0, gate1, up1, down1, wq_h, wk_h, wv_h, po_h, lam, hgain, ck_h, cv_h, live,
    out,
    wst, po, kbuf, vbuf, wpl, popl,
    a1, a2, b1s, b1r, b2, c1s, c1r, c2, c3, d1s, d1r, d2o, d2m, d3, f1, f2, g1s, g1r, g2,
    hsem, ssem, rsem,
):
    z = lax.axis_index("kv_0")
    y = lax.axis_index("kv_1")
    c = lax.axis_index("tp")
    yc = y * NC + c

    loads = [
        pltpu.make_async_copy(wq_h, wst.at[:, pl.ds(0, 512)], hsem.at[0]),
        pltpu.make_async_copy(wk_h, wst.at[:, pl.ds(512, 128)], hsem.at[1]),
        pltpu.make_async_copy(wv_h, wst.at[:, pl.ds(640, 128)], hsem.at[2]),
        pltpu.make_async_copy(po_h, po, hsem.at[3]),
        pltpu.make_async_copy(ck_h, kbuf, hsem.at[4]),
        pltpu.make_async_copy(cv_h, vbuf, hsem.at[5]),
    ]
    for load in loads:
        load.start()

    def z_peer(k):
        return lax.rem(z + k, NZ)

    def y_peer(k):
        return lax.rem(y + k, NY)

    def yc_peer(k):
        p = lax.rem(yc + k, NYC)
        return p // NC, lax.rem(p, NC)

    barrier = pltpu.get_barrier_semaphore()
    for k in Z_STEPS:
        pl.semaphore_signal(barrier, inc=1, device_id={"kv_0": z_peer(k)}, device_id_type=MESH)
    for k in YC_STEPS:
        py, pc = yc_peer(k)
        pl.semaphore_signal(barrier, inc=1, device_id={"kv_1": py, "tp": pc}, device_id_type=MESH)

    sent = []

    def send(phase, src, dst, device):
        pltpu.make_async_remote_copy(
            src_ref=src, dst_ref=dst, send_sem=ssem.at[phase], recv_sem=rsem.at[phase],
            device_id=device, device_id_type=MESH,
        ).start()

    def arrive(phase, buf, count):
        whole = pltpu.make_async_remote_copy(
            src_ref=buf.at[pl.ds(0, count)], dst_ref=buf.at[pl.ds(0, count)],
            send_sem=ssem.at[phase], recv_sem=rsem.at[phase],
            device_id={"kv_0": z}, device_id_type=MESH,
        )
        whole.wait_recv()
        sent.append(whole)

    def to_z(phase, buf):
        for k in Z_STEPS:
            send(phase, buf.at[z], buf.at[z], {"kv_0": z_peer(k)})

    def to_yc(phase, buf):
        for k in YC_STEPS:
            py, pc = yc_peer(k)
            send(phase, buf.at[yc], buf.at[yc], {"kv_1": py, "tp": pc})

    def to_y(phase, buf):
        for k in Y_STEPS:
            send(phase, buf.at[y], buf.at[y], {"kv_1": y_peer(k)})

    def parts_to_z(phase, src, dst):
        for k in Z_STEPS:
            p = z_peer(k)
            send(phase, src.at[p], dst.at[z], {"kv_0": p})

    def total(buf, count):
        acc = buf[0].astype(F32)
        for k in range(1, count):
            acc = acc + buf[k].astype(F32)
        return acc

    own_lane = yc * 16
    spread = (iota((16, LANES), 1) == iota((16, LANES), 0) + own_lane).astype(F32).astype(BF16)
    a1[yc] = jnp.dot(res[...], spread, preferred_element_type=F32).astype(BF16)
    chip_rows = (iota((LANES, 32), 0) == iota((LANES, 32), 1) + y * 32).astype(F32).astype(BF16)
    for load in loads[:4]:
        load.wait()
    wpl[...] = jnp.dot(chip_rows, wst[...], preferred_element_type=F32).astype(BF16)
    popl[...] = jnp.dot(chip_rows, po[...], preferred_element_type=F32).astype(BF16)

    pl.semaphore_wait(barrier, len(Z_STEPS) + len(YC_STEPS))

    to_yc(A1, a1)
    arrive(A1, a1, NYC - 1)
    res_z = total(a1, NYC)
    a2[z] = res_z.astype(BF16)
    to_z(A2, a2)
    arrive(A2, a2, NZ - 1)
    rows = jnp.concatenate([a2[k].astype(F32) for k in range(NZ)], axis=1)

    part = mix_part(rows, gains[0:1, :], gate0[...], up0[...], down0[...])
    for k in range(NZ):
        b1s[k] = part[:, k * LANES : (k + 1) * LANES]
    parts_to_z(B1, b1s, b1r)
    b1r[z] = b1s[z]
    arrive(B1, b1r, NZ - 1)
    b2[yc] = total(b1r, NZ)
    to_yc(B2, b2)
    arrive(B2, b2, NYC - 1)
    stream_one = (res_z + total(b2, NYC)).astype(BF16).astype(F32)

    lane = iota((8, LANES), 1)
    mine = (lane >= y * 32) & (lane < y * 32 + 32)
    own = jnp.where(mine, stream_one, 0.0)
    squares = jnp.broadcast_to(jnp.sum(own * own, axis=1, keepdims=True), (8, LANES))
    gain_z = gains[1:2, pl.ds(pl.multiple_of(z * LANES, LANES), LANES)]
    scaled = (stream_one * gain_z).astype(BF16)
    qkv = jnp.dot(scaled, wpl[...], preferred_element_type=F32)
    for t in range(6):
        c1s[pl.ds(t, 8, stride=8), :] = qkv[:, t * LANES : (t + 1) * LANES]
    c1s[pl.ds(6, 8, stride=8), :] = squares
    c1s[pl.ds(7, 8, stride=8), :] = jnp.zeros((8, LANES), F32)
    for k in Y_STEPS:
        p = y_peer(k)
        send(C1, c1s.at[pl.ds(pl.multiple_of(p * 16, 16), 16)], c1r.at[y], {"kv_1": p})
    c1r[y] = c1s[pl.ds(pl.multiple_of(y * 16, 16), 16), :]
    arrive(C1, c1r, NY - 1)
    c2[z] = total(c1r, NY)
    to_z(C2, c2)
    arrive(C2, c2, NZ - 1)
    sums = total(c2, NZ)
    query_rows, key_rows, value_rows = [], [], []
    for s in range(2):
        block = sums[s * 8 : (s + 1) * 8]
        factor = lax.rsqrt(block[6:7] / D + EPS)
        block = (block * factor).astype(BF16).astype(F32)
        for g in range(4):
            query_rows += [block[g : g + 1], block[g : g + 1]]
        key_rows.append(jnp.broadcast_to(block[4:5], (8, LANES)))
        value_rows.append(jnp.broadcast_to(block[5:6], (8, LANES)))
    row16 = iota((16, LANES), 0)
    lane16 = iota((16, LANES), 1)
    component = lax.rem(row16, 2)
    queries = jnp.where((lane16 >= HEAD) == (component == 1), jnp.concatenate(query_rows, axis=0), 0.0)
    key_new = jnp.concatenate(key_rows, axis=0)
    value_new = jnp.concatenate(value_rows, axis=0)
    c3[y] = queries.astype(BF16)
    to_y(C3, c3)
    score_scale = HEAD**-0.5
    own_score = jnp.sum(queries * key_new, axis=1, keepdims=True) * score_scale
    loads[4].wait()
    loads[5].wait()
    arrive(C3, c3, NY - 1)

    span = kbuf.shape[1]
    position = (z * NY + y) * span + iota((8, span), 1)
    for b in range(8):
        query = c3[b // 2].astype(F32)[(b % 2) * 8 : (b % 2) * 8 + 8].astype(BF16)
        scores = lax.dot_general(query, kbuf[b], NT, preferred_element_type=F32) * score_scale
        alive = position < live[b]
        highest = jnp.max(jnp.where(alive, scores, -1e30), axis=1, keepdims=True)
        terms = jnp.where(alive, jnp.exp(scores - highest), 0.0)
        count = jnp.sum(terms, axis=1, keepdims=True)
        d1s[b // 2, (b % 2) * 8 : (b % 2) * 8 + 8, :] = jnp.dot(
            terms.astype(BF16), vbuf[b], preferred_element_type=F32
        )
        d1s[b // 2, 16 + (b % 2) * 8 : 24 + (b % 2) * 8, :] = jnp.where(lane < HEAD, highest, count)
    for k in Y_STEPS:
        p = y_peer(k)
        send(D1, d1s.at[p], d1r.at[y], {"kv_1": p})
    d1r[y] = d1s[y]
    arrive(D1, d1r, NY - 1)

    tops = [d1r[k, 16:32, 0:1] for k in range(NY)]
    counts = [d1r[k, 16:32, HEAD : HEAD + 1] for k in range(NY)]
    top = functools.reduce(jnp.maximum, tops)
    weights = [jnp.exp(t - top) for t in tops]
    count = sum(w * s for w, s in zip(weights, counts))
    values = sum(weights[k] * d1r[k, 0:16, :] for k in range(NY))
    d2o[z] = values.astype(BF16)
    line = jnp.where(lane16 == row16, top, 0.0) + jnp.where(lane16 == row16 + HEAD, count, 0.0)
    d2m[z] = jnp.sum(line, axis=0, keepdims=True)
    to_z(D2M, d2m)
    to_z(D2O, d2o)
    arrive(D2M, d2m, NZ - 1)
    tops = [
        jnp.sum(jnp.where(lane16 == row16, d2m[k], 0.0), axis=1, keepdims=True) for k in range(NZ)
    ]
    counts = [
        jnp.sum(jnp.where(lane16 == row16 + HEAD, d2m[k], 0.0), axis=1, keepdims=True) for k in range(NZ)
    ]
    top = functools.reduce(jnp.maximum, tops, own_score)
    weights = [jnp.exp(t - top) for t in tops]
    own_weight = jnp.exp(own_score - top)
    count = functools.reduce(jnp.add, [w * s for w, s in zip(weights, counts)], own_weight)
    arrive(D2O, d2o, NZ - 1)
    values = own_weight * value_new
    for k in range(NZ):
        values = values + weights[k] * d2o[k].astype(F32)
    ratio = values / count
    head = lax.rem(row16 // 2, 4)
    lambdas = jnp.where(
        head == 0, lam[0], jnp.where(head == 1, lam[1], jnp.where(head == 2, lam[2], lam[3]))
    )
    mixed = ratio - lambdas * pltpu.roll(ratio, 15, 0)
    scale = lax.rsqrt(jnp.mean(mixed * mixed, axis=1, keepdims=True) + EPS)
    heads = jnp.where(component == 0, mixed * scale * hgain[...], 0.0)
    d3[y] = heads.astype(BF16)
    to_y(D3, d3)
    arrive(D3, d3, NY - 1)

    heads = jnp.concatenate([d3[k].astype(F32) for k in range(NY)], axis=0)
    head = lax.rem(iota((64, LANES), 0) // 2, 4)
    wide = jnp.concatenate([jnp.where(head == g, heads, 0.0) for g in range(4)], axis=1).astype(BF16)
    projected = lax.dot_general(wide, popl[...], NT, preferred_element_type=F32)
    f1[yc] = jnp.sum(projected.reshape(8, 8, LANES), axis=1)
    to_yc(F1, f1)
    arrive(F1, f1, NYC - 1)
    stream_two = (stream_one + total(f1, NYC)).astype(BF16)
    f2[z] = stream_two
    to_z(F2, f2)
    arrive(F2, f2, NZ - 1)
    rows = jnp.concatenate([f2[k].astype(F32) for k in range(NZ)], axis=1)

    part = mix_part(rows, gains[2:3, :], gate1[...], up1[...], down1[...])
    for k in range(NZ):
        g1s[k] = part[:, k * LANES : (k + 1) * LANES].astype(g1s.dtype)
    parts_to_z(G1, g1s, g1r)
    g1r[z] = g1s[z]
    arrive(G1, g1r, NZ - 1)
    g2[yc] = total(g1r, NZ)
    to_yc(G2, g2)
    arrive(G2, g2, NYC - 1)
    updated = stream_two.astype(F32) + total(g2, NYC)
    out[...] = pltpu.roll(updated, lax.rem(LANES - own_lane, LANES), 1)[:, :16].astype(BF16)

    for whole in sent:
        whole.wait_send()


def local(
    residual, norm_gains, ffn_gate, ffn_up, ffn_down, proj_query, proj_key, proj_value, proj_out,
    head_lambda, head_gain, cache_keys, cache_values, live_length,
):
    batch = residual.shape[0]
    span = cache_keys.shape[1]
    vmem = pl.BlockSpec(memory_space=pltpu.VMEM)
    smem = pl.BlockSpec(memory_space=pltpu.SMEM)
    hbm = pl.BlockSpec(memory_space=pl.ANY)
    return pl.pallas_call(
        layer_kernel,
        out_shape=jax.ShapeDtypeStruct(residual.shape, BF16),
        in_specs=[vmem] * 8 + [hbm] * 4 + [smem, vmem, hbm, hbm, smem],
        out_specs=vmem,
        scratch_shapes=[
            pltpu.VMEM((32, 768), BF16),
            pltpu.VMEM((32, 512), BF16),
            pltpu.VMEM((batch, span, 128), BF16),
            pltpu.VMEM((batch, span, VDIM), BF16),
            pltpu.VMEM((LANES, 768), BF16),
            pltpu.VMEM((LANES, 512), BF16),
            pltpu.VMEM((NYC, 8, LANES), BF16),
            pltpu.VMEM((NZ, 8, LANES), BF16),
            pltpu.VMEM((NZ, 8, LANES), F32),
            pltpu.VMEM((NZ, 8, LANES), F32),
            pltpu.VMEM((NYC, 8, LANES), F32),
            pltpu.VMEM((64, LANES), F32),
            pltpu.VMEM((NY, 16, LANES), F32),
            pltpu.VMEM((NZ, 16, LANES), F32),
            pltpu.VMEM((NY, 16, LANES), BF16),
            pltpu.VMEM((NY, 32, LANES), F32),
            pltpu.VMEM((NY, 32, LANES), F32),
            pltpu.VMEM((NZ, 16, LANES), BF16),
            pltpu.VMEM((NZ, 1, LANES), F32),
            pltpu.VMEM((NY, 16, LANES), BF16),
            pltpu.VMEM((NYC, 8, LANES), F32),
            pltpu.VMEM((NZ, 8, LANES), BF16),
            pltpu.VMEM((NZ, 8, LANES), BF16),
            pltpu.VMEM((NZ, 8, LANES), BF16),
            pltpu.VMEM((NYC, 8, LANES), F32),
            pltpu.SemaphoreType.DMA((6,)),
            pltpu.SemaphoreType.DMA((15,)),
            pltpu.SemaphoreType.DMA((15,)),
        ],
        compiler_params=pltpu.CompilerParams(collective_id=0, has_side_effects=True),
    )(
        residual, norm_gains,
        ffn_gate[0], ffn_up[0], ffn_down[0], ffn_gate[1], ffn_up[1], ffn_down[1],
        proj_query, proj_key, proj_value, proj_out.T,
        head_lambda, head_gain.reshape(1, VDIM),
        cache_keys.reshape(batch, span, 128), cache_values.reshape(batch, span, VDIM), live_length,
    )


def solution(mesh):
    split = Mesh(
        mesh.devices.reshape(mesh.shape["dp"], NZ, NY, mesh.shape["tp"]),
        ("dp", "kv_0", "kv_1", "tp"),
    )
    return jax.shard_map(
        local,
        mesh=split,
        in_specs=(
            P("dp", KV_TP),
            P(),
            P(None, KV_TP, None),
            P(None, KV_TP, None),
            P(None, KV_TP, None),
            P(KV, "tp"),
            P(KV, "tp"),
            P(KV, "tp"),
            P("tp", KV),
            P("tp"),
            P(),
            P("dp", KV, "tp", None),
            P("dp", KV, "tp", None),
            P("dp"),
        ),
        out_specs=P("dp", KV_TP),
        check_vma=False,
    )
```

```python
import functools

import jax
import jax.numpy as jnp
from jax import lax
from jax.experimental import pallas as pl
from jax.experimental.pallas import tpu as pltpu
from jax.sharding import Mesh
from jax.sharding import PartitionSpec as P

D = 2048
HEAD = 64
VDIM = 128
NZ = 16
NY = 4
NC = 2
NYC = NY * NC
LANES = 128
KV_TP = ("kv_0", "kv_1", "tp")
KV = ("kv_0", "kv_1")
MESH = pl.DeviceIdType.MESH
F32 = jnp.float32
BF16 = jnp.bfloat16
EPS = 1e-05
NT = (((1,), (1,)), ((), ()))

Z_STEPS = (8, 7, 9, 6, 10, 5, 11, 4, 12, 3, 13, 2, 14, 1, 15)
Y_STEPS = (2, 1, 3)
WEIGHT_ROWS = 48


def iota(shape, dim):
    return lax.broadcasted_iota(jnp.int32, shape, dim)


def mix_part(rows, gain, weights):
    scale = lax.rsqrt(jnp.mean(rows * rows, axis=1, keepdims=True) + EPS)
    normed = (rows * scale * gain).astype(BF16)
    gate = lax.dot_general(normed, weights[0], NT, preferred_element_type=F32)
    up = lax.dot_general(normed, weights[1], NT, preferred_element_type=F32)
    hidden = (gate / (1.0 + jnp.exp(-gate)) * up).astype(BF16)
    return 0.5 * jnp.dot(hidden, weights[2], preferred_element_type=F32)


def layer_kernel(
    res, gains, gate_h, up_h, down_h, wq_h, wk_h, wv_h, po_h, lam, hgain, ck_h, cv_h, live,
    out,
    raw, stage, wts, wqb, wkb, wvb, pob, lams, kbuf, vbuf,
    a1, a2, b1s, b1r, b2, cs, csq, c2, c3s, c3, d1s, d1r, d2o, d2m, hs, d3s, d3, ps, f2, fs, g1s, g1r, g2,
    hsem, ssem, rsem,
):
    z = lax.axis_index("kv_0")
    y = lax.axis_index("kv_1")
    c = lax.axis_index("tp")
    hidden_rows = raw.shape[1]
    barrier = pltpu.get_barrier_semaphore()
    drains = []

    def z_peer(k):
        return lax.rem(z + k, NZ)

    def y_peer(k):
        return lax.rem(y + k, NY)

    def send(s, r, src, dst, device):
        pltpu.make_async_remote_copy(
            src_ref=src, dst_ref=dst, send_sem=ssem.at[s], recv_sem=rsem.at[r],
            device_id=device, device_id_type=MESH,
        ).start()

    def waits(s, r, ref):
        return pltpu.make_async_remote_copy(
            src_ref=ref, dst_ref=ref, send_sem=ssem.at[s], recv_sem=rsem.at[r],
            device_id={"kv_0": z}, device_id_type=MESH,
        )

    def arrive(r, ref):
        waits(r, r, ref).wait_recv()

    def drain(s, ref):
        drains.append(waits(s, s, ref))

    def signal(device):
        pl.semaphore_signal(barrier, inc=1, device_id=device, device_id_type=MESH)

    def to_z(phase, src_of, dst):
        for k in Z_STEPS:
            p = z_peer(k)
            send(phase, phase, src_of(p), dst.at[z], {"kv_0": p})

    def to_y(phase, src, dst):
        for k in Y_STEPS:
            send(phase, phase, src, dst, {"kv_1": y_peer(k)})

    def total(buf, count):
        acc = buf[0].astype(F32)
        for k in range(1, count):
            acc = acc + buf[k].astype(F32)
        return acc

    def load(k):
        if k < 3:
            return pltpu.make_async_copy((gate_h, up_h, down_h)[k], raw.at[k], hsem.at[k])
        return pltpu.make_async_copy((ck_h, cv_h)[k - 3], (kbuf, vbuf)[k - 3], hsem.at[k])

    for k in range(5):
        load(k).start()

    def own_tile():
        spread = (iota((16, LANES), 1) == iota((16, LANES), 0) + (y * NC + c) * 16).astype(F32).astype(BF16)
        return jnp.dot(res[...], spread, preferred_element_type=F32).astype(BF16)

    lane = iota((8, LANES), 1)
    row = iota((8, LANES), 0)

    def own_lambdas():
        head = row // 2
        return jnp.where(head == 0, lam[0], jnp.where(head == 1, lam[1], jnp.where(head == 2, lam[2], lam[3])))

    def attend():
        span = kbuf.shape[1]
        position = (z * NY + y) * span + iota((8, span), 1)
        for b in range(8):
            query = c3[b // 2].astype(F32)[(b % 2) * 8 : (b % 2) * 8 + 8].astype(BF16)
            scores = lax.dot_general(query, kbuf[b], NT, preferred_element_type=F32) * HEAD**-0.5
            alive = position < live[b]
            highest = jnp.max(jnp.where(alive, scores, -1e30), axis=1, keepdims=True)
            terms = jnp.where(alive, jnp.exp(scores - highest), 0.0)
            count = jnp.sum(terms, axis=1, keepdims=True)
            d1s[b // 2, (b % 2) * 8 : (b % 2) * 8 + 8, :] = jnp.dot(
                terms.astype(BF16), vbuf[b], preferred_element_type=F32
            )
            d1s[b // 2, 16 + (b % 2) * 8 : 24 + (b % 2) * 8, :] = jnp.where(lane < HEAD, highest, count)

    def finish(stream_two):
        updated = stream_two.astype(F32) + total(g2, NY)
        out[...] = pltpu.roll(updated, lax.rem(LANES - (y * NC + c) * 16, LANES), 1)[:, :16]
        for each in drains:
            each.wait_send()
        drains.clear()

    @pl.when(c == 0)
    def _():
        core1 = {"tp": 1}

        def all_core1(s, r, src, dst):
            for k in Y_STEPS + (0,):
                send(s, r, src, dst, {"kv_1": y_peer(k), "tp": 1})

        for k in Y_STEPS + (0,):
            signal({"kv_1": y_peer(k), "tp": 1})
        a1[y * NC] = own_tile()
        lams[0] = own_lambdas()
        pl.semaphore_wait(barrier, NY)

        all_core1(A1, A1, a1.at[y * NC], a1.at[y * NC])
        drain(A1, a1.at[pl.ds(0, NY)])
        send(LAM, LAM, lams.at[0], lams.at[0], core1)
        drain(LAM, lams.at[0])
        stage[:, :, 40:WEIGHT_ROWS, :] = jnp.zeros((2, 3, WEIGHT_ROWS - 40, D), BF16)
        for half in range(2):
            for m in range(3):
                if half == 0:
                    load(m).wait()
                stage[half, m, 0:hidden_rows, :] = raw.at[m][:, half, :]
            for m in range(3):
                send(W0 + half, W0 + half, stage.at[half, m], wts.at[half, m, pl.ds(WEIGHT_ROWS, WEIGHT_ROWS)], core1)
            drain(W0 + half, stage.at[half])
            if half == 0:
                part = pl.ds(pl.multiple_of(y * 32, 32), 32)
                all_core1(WQ, WQ, wq_h, wqb.at[0, part])
                all_core1(WK, WK, wk_h, wkb.at[0, part])
                all_core1(WV, WV, wv_h, wvb.at[0, part])
                drain(WQ, wqb.at[0])
                drain(WK, wkb.at[0])
                drain(WV, wvb.at[0])
        all_core1(WO, WO, po_h, pob.at[part, pl.ds(0, 512)])
        drain(WO, pob.at[:, pl.ds(0, 512)])

        load(3).wait()
        load(4).wait()
        arrive(C3, c3)
        attend()
        for k in Y_STEPS + (0,):
            p = y_peer(k)
            send(D1, D1, d1s.at[p], d1r.at[y * NC], {"kv_1": p, "tp": 1})
        drain(D1, d1s)
        arrive(FS, fs)
        arrive(G2, g2)
        finish(fs[...])

    @pl.when(c == 1)
    def _():
        for k in Z_STEPS:
            signal({"kv_0": z_peer(k)})
        for k in Y_STEPS + (0,):
            signal({"kv_1": y_peer(k), "tp": 0})
        for k in Y_STEPS:
            signal({"kv_1": y_peer(k)})
        part = pl.ds(pl.multiple_of(y * 32, 32), 32)
        pulls = [
            pltpu.make_async_copy(wq_h, wqb.at[1, part], hsem.at[5]),
            pltpu.make_async_copy(wk_h, wkb.at[1, part], hsem.at[6]),
            pltpu.make_async_copy(wv_h, wvb.at[1, part], hsem.at[7]),
            pltpu.make_async_copy(po_h, pob.at[part, pl.ds(512, 512)], hsem.at[8]),
        ]
        for pull in pulls:
            pull.start()
        a1[y * NC + 1] = own_tile()
        lams[1] = own_lambdas()

        def relayout(half):
            for m in range(3):
                wts[half, m, 0:hidden_rows, :] = raw.at[m][:, half, :]

        wts[:, :, 40:WEIGHT_ROWS, :] = jnp.zeros((2, 3, WEIGHT_ROWS - 40, D), BF16)
        for m in range(3):
            load(m).wait()
        relayout(0)
        pl.semaphore_wait(barrier, (NZ - 1) + NY + (NY - 1))

        to_y(A1, a1.at[y * NC + 1], a1.at[y * NC + 1])
        drain(A1, a1.at[pl.ds(0, NY - 1)])
        arrive(A1, a1.at[pl.ds(0, NYC - 1)])
        res_z = total(a1, NYC)
        a2[z] = res_z.astype(BF16)
        to_z(A2, lambda p: a2.at[z], a2)
        drain(A2, a2.at[pl.ds(0, NZ - 1)])
        to_y(WQ, wq_h, wqb.at[1, part])
        to_y(WK, wk_h, wkb.at[1, part])
        to_y(WV, wv_h, wvb.at[1, part])
        to_y(WO, po_h, pob.at[part, pl.ds(512, 512)])
        drain(WQ, wqb.at[1, pl.ds(0, 96)])
        drain(WK, wkb.at[1, pl.ds(0, 96)])
        drain(WV, wvb.at[1, pl.ds(0, 96)])
        drain(WO, pob.at[pl.ds(0, 96), pl.ds(512, 512)])
        relayout(1)
        for pull in pulls:
            pull.wait()
        arrive(W0, wts.at[0, :, pl.ds(WEIGHT_ROWS, WEIGHT_ROWS)])
        arrive(A2, a2.at[pl.ds(0, NZ - 1)])
        rows = jnp.concatenate([a2[k].astype(F32) for k in range(NZ)], axis=1)

        mixed = mix_part(rows, gains[0:1, :], [wts[0, m] for m in range(3)])
        for k in range(NZ):
            b1s[k] = mixed[:, k * LANES : (k + 1) * LANES]
        to_z(B1, lambda p: b1s.at[p], b1r)
        drain(B1, b1s.at[pl.ds(0, NZ - 1)])
        b1r[z] = b1s[z]
        arrive(B1, b1r.at[pl.ds(0, NZ - 1)])
        b2[y] = total(b1r, NZ)
        to_y(B2, b2.at[y], b2.at[y])
        drain(B2, b2.at[pl.ds(0, NY - 1)])
        arrive(WQ, wqb.at[:, pl.ds(0, 112)])
        arrive(WK, wkb.at[:, pl.ds(0, 112)])
        arrive(WV, wvb.at[:, pl.ds(0, 112)])
        arrive(B2, b2.at[pl.ds(0, NY - 1)])
        stream_one = (res_z + total(b2, NY)).astype(BF16).astype(F32)

        squares = jnp.sum(stream_one * stream_one, axis=1, keepdims=True)
        csq[z] = jnp.sum(jnp.where(lane == row, squares, 0.0), axis=0, keepdims=True)
        to_z(CQ, lambda p: csq.at[z], csq)
        drain(CQ, csq.at[pl.ds(0, NZ - 1)])
        gain_z = gains[1:2, pl.ds(pl.multiple_of(z * LANES, LANES), LANES)]
        scaled = (stream_one * gain_z).astype(BF16)
        for t in range(2):
            query = jnp.dot(scaled, wqb[t], preferred_element_type=F32)
            for g in range(4):
                cs[pl.ds(t * 4 + g, 8, stride=12), :] = query[:, g * LANES : (g + 1) * LANES]
            cs[pl.ds(8 + t, 8, stride=12), :] = jnp.dot(scaled, wkb[t], preferred_element_type=F32)
            cs[pl.ds(10 + t, 8, stride=12), :] = jnp.dot(scaled, wvb[t], preferred_element_type=F32)
        pair = pl.ds(pl.multiple_of(y * 24, 8), 24)
        to_z(C2, lambda p: cs.at[pair], c2)
        drain(C2, c2.at[pl.ds(0, NZ - 1)])
        c2[z] = cs[pair, :]
        arrive(CQ, csq.at[pl.ds(0, NZ - 1)])
        square_line = total(csq, NZ)
        arrive(C2, c2.at[pl.ds(0, NZ - 1)])
        sums = total(c2, NZ)
        query_rows, key_rows, value_rows = [], [], []
        lane1 = iota((1, LANES), 1)
        for s in range(2):
            square = jnp.sum(jnp.where(lane1 == 2 * y + s, square_line, 0.0), axis=1, keepdims=True)
            factor = lax.rsqrt(square / D + EPS)
            block = (sums[s * 12 : (s + 1) * 12] * factor).astype(BF16).astype(F32)
            for h in range(8):
                query_rows += [block[h : h + 1], block[h : h + 1]]
            for t in range(2):
                key_rows.append(jnp.broadcast_to(block[8 + t : 9 + t], (8, LANES)))
                value_rows.append(jnp.broadcast_to(block[10 + t : 11 + t], (8, LANES)))
        row32 = iota((32, LANES), 0)
        lane32 = iota((32, LANES), 1)
        component = lax.rem(row32, 2)
        queries = jnp.where((lane32 >= HEAD) == (component == 1), jnp.concatenate(query_rows, axis=0), 0.0)
        for t in range(2):
            c3s[t] = jnp.concatenate(
                [queries[t * 8 : t * 8 + 8], queries[16 + t * 8 : 24 + t * 8]], axis=0
            ).astype(BF16)
        for k in Y_STEPS:
            send(C3S, C3, c3s.at[0], c3.at[y], {"kv_1": y_peer(k), "tp": 0})
            send(C3, C3, c3s.at[1], c3.at[y], {"kv_1": y_peer(k)})
        send(C3S, C3, c3s.at[0], c3.at[y], {"tp": 0})
        drain(C3S, c3)
        drain(C3, c3.at[pl.ds(0, NY - 1)])
        c3[y] = c3s[1]
        key_new = jnp.concatenate(key_rows, axis=0)
        value_new = jnp.concatenate(value_rows, axis=0)
        own_score = jnp.sum(queries * key_new, axis=1, keepdims=True) * HEAD**-0.5
        load(3).wait()
        load(4).wait()
        arrive(C3, c3.at[pl.ds(0, NY - 1)])
        attend()
        for k in Y_STEPS:
            p = y_peer(k)
            send(D1, D1, d1s.at[p], d1r.at[y * NC + 1], {"kv_1": p})
        drain(D1, d1s.at[pl.ds(0, NY - 1)])
        d1r[y * NC + 1] = d1s[y]
        arrive(LAM, lams.at[0])
        arrive(WO, pob.at[pl.ds(0, 112)])
        arrive(W1, wts.at[1, :, pl.ds(WEIGHT_ROWS, WEIGHT_ROWS)])
        arrive(D1, d1r.at[pl.ds(0, NYC - 1)])

        def gathered(k, start, lanes):
            return jnp.concatenate(
                [d1r[k * NC + t, start + s * 8 : start + s * 8 + 8, lanes] for s in range(2) for t in range(2)], axis=0
            )

        tops = [gathered(k, 16, slice(0, 1)) for k in range(NY)]
        counts = [gathered(k, 16, slice(HEAD, HEAD + 1)) for k in range(NY)]
        top = functools.reduce(jnp.maximum, tops)
        weights = [jnp.exp(t - top) for t in tops]
        count = functools.reduce(jnp.add, [w * s for w, s in zip(weights, counts)])
        values = functools.reduce(jnp.add, [weights[k] * gathered(k, 0, slice(None)) for k in range(NY)])
        line = jnp.where(lane32 == row32, top, 0.0) + jnp.where(lane32 == row32 + HEAD, count, 0.0)
        d2m[z] = jnp.sum(line, axis=0, keepdims=True)
        to_z(D2M, lambda p: d2m.at[z], d2m)
        drain(D2M, d2m.at[pl.ds(0, NZ - 1)])
        d2o[z] = values.astype(BF16)
        to_z(D2O, lambda p: d2o.at[z], d2o)
        drain(D2O, d2o.at[pl.ds(0, NZ - 1)])
        arrive(D2M, d2m.at[pl.ds(0, NZ - 1)])
        tops = [jnp.sum(jnp.where(lane32 == row32, d2m[k], 0.0), axis=1, keepdims=True) for k in range(NZ)]
        counts = [jnp.sum(jnp.where(lane32 == row32 + HEAD, d2m[k], 0.0), axis=1, keepdims=True) for k in range(NZ)]
        top = functools.reduce(jnp.maximum, tops, own_score)
        weights = [jnp.exp(t - top) for t in tops]
        own_weight = jnp.exp(own_score - top)
        count = functools.reduce(jnp.add, [w * s for w, s in zip(weights, counts)], own_weight)
        arrive(D2O, d2o.at[pl.ds(0, NZ - 1)])
        values = own_weight * value_new
        for k in range(NZ):
            values = values + weights[k] * d2o[k].astype(F32)
        ratio = values / count
        lambdas = jnp.concatenate([lams[0], lams[1], lams[0], lams[1]], axis=0)
        mixed = ratio - lambdas * pltpu.roll(ratio, 31, 0)
        scale = lax.rsqrt(jnp.mean(mixed * mixed, axis=1, keepdims=True) + EPS)
        hs[...] = mixed * scale * hgain[...]
        d3s[...] = hs[pl.ds(0, 16, stride=2), :].astype(BF16)
        to_y(D3, d3s, d3.at[y])
        drain(D3, d3.at[pl.ds(0, NY - 1)])
        d3[y] = d3s[...]
        arrive(D3, d3.at[pl.ds(0, NY - 1)])

        for k in range(NY):
            ps[k * 16 : (k + 1) * 16, :] = d3[k].astype(F32)
        heads = jnp.concatenate([ps[pl.ds(h, 8, stride=8), :] for h in range(8)], axis=1).astype(BF16)
        projected = lax.dot_general(heads, pob[...], NT, preferred_element_type=F32)
        stream_two = (stream_one + projected).astype(BF16)
        f2[z] = stream_two
        fs[...] = stream_two
        to_z(F2, lambda p: f2.at[z], f2)
        drain(F2, f2.at[pl.ds(0, NZ - 1)])
        send(FS, FS, fs, fs, {"tp": 0})
        drain(FS, fs)
        arrive(F2, f2.at[pl.ds(0, NZ - 1)])
        rows = jnp.concatenate([f2[k].astype(F32) for k in range(NZ)], axis=1)

        mixed = mix_part(rows, gains[2:3, :], [wts[1, m] for m in range(3)])
        for k in range(NZ):
            g1s[k] = mixed[:, k * LANES : (k + 1) * LANES]
        to_z(G1, lambda p: g1s.at[p], g1r)
        drain(G1, g1s.at[pl.ds(0, NZ - 1)])
        g1r[z] = g1s[z]
        arrive(G1, g1r.at[pl.ds(0, NZ - 1)])
        g2[y] = total(g1r, NZ)
        for k in Y_STEPS:
            send(G2S, G2, g2.at[y], g2.at[y], {"kv_1": y_peer(k), "tp": 0})
            send(G2, G2, g2.at[y], g2.at[y], {"kv_1": y_peer(k)})
        send(G2S, G2, g2.at[y], g2.at[y], {"tp": 0})
        drain(G2S, g2)
        drain(G2, g2.at[pl.ds(0, NY - 1)])
        arrive(G2, g2.at[pl.ds(0, NY - 1)])
        finish(stream_two)


PHASES = 28
(
    A1, A2, B1, B2, CQ, C2, C3, C3S, D1, D2O, D2M, D3, F2, FS, G1, G2, G2S, LAM, W0, W1, WQ, WK, WV, WO,
) = range(24)


def local(
    residual, norm_gains, ffn_gate, ffn_up, ffn_down, proj_query, proj_key, proj_value, proj_out,
    head_lambda, head_gain, cache_keys, cache_values, live_length,
):
    batch = residual.shape[0]
    hidden = ffn_gate.shape[1]
    span = cache_keys.shape[1]
    vmem = pl.BlockSpec(memory_space=pltpu.VMEM)
    smem = pl.BlockSpec(memory_space=pltpu.SMEM)
    hbm = pl.BlockSpec(memory_space=pl.ANY)
    updated = pl.pallas_call(
        layer_kernel,
        out_shape=jax.ShapeDtypeStruct(residual.shape, F32),
        in_specs=[vmem] * 2 + [hbm] * 7 + [smem, vmem, hbm, hbm, smem],
        out_specs=vmem,
        scratch_shapes=[
            pltpu.VMEM((3, hidden, 2, D), BF16),
            pltpu.VMEM((2, 3, WEIGHT_ROWS, D), BF16),
            pltpu.VMEM((2, 3, 2 * WEIGHT_ROWS, D), BF16),
            pltpu.VMEM((2, LANES, 512), BF16),
            pltpu.VMEM((2, LANES, 128), BF16),
            pltpu.VMEM((2, LANES, 128), BF16),
            pltpu.VMEM((LANES, 1024), BF16),
            pltpu.VMEM((2, 8, LANES), F32),
            pltpu.VMEM((batch, span, 128), BF16),
            pltpu.VMEM((batch, span, VDIM), BF16),
            pltpu.VMEM((NYC, 8, LANES), BF16),
            pltpu.VMEM((NZ, 8, LANES), BF16),
            pltpu.VMEM((NZ, 8, LANES), F32),
            pltpu.VMEM((NZ, 8, LANES), F32),
            pltpu.VMEM((NY, 8, LANES), F32),
            pltpu.VMEM((96, LANES), F32),
            pltpu.VMEM((NZ, 1, LANES), F32),
            pltpu.VMEM((NZ, 24, LANES), F32),
            pltpu.VMEM((2, 16, LANES), BF16),
            pltpu.VMEM((NY, 16, LANES), BF16),
            pltpu.VMEM((NY, 32, LANES), F32),
            pltpu.VMEM((NYC, 32, LANES), F32),
            pltpu.VMEM((NZ, 32, LANES), BF16),
            pltpu.VMEM((NZ, 1, LANES), F32),
            pltpu.VMEM((32, LANES), F32),
            pltpu.VMEM((16, LANES), BF16),
            pltpu.VMEM((NY, 16, LANES), BF16),
            pltpu.VMEM((64, LANES), F32),
            pltpu.VMEM((NZ, 8, LANES), BF16),
            pltpu.VMEM((8, LANES), BF16),
            pltpu.VMEM((NZ, 8, LANES), F32),
            pltpu.VMEM((NZ, 8, LANES), F32),
            pltpu.VMEM((NY, 8, LANES), F32),
            pltpu.SemaphoreType.DMA((9,)),
            pltpu.SemaphoreType.DMA((PHASES,)),
            pltpu.SemaphoreType.DMA((PHASES,)),
        ],
        compiler_params=pltpu.CompilerParams(collective_id=0, has_side_effects=True),
    )(
        residual, norm_gains,
        jnp.swapaxes(ffn_gate, 0, 1), jnp.swapaxes(ffn_up, 0, 1), jnp.swapaxes(ffn_down, 0, 1),
        proj_query, proj_key, proj_value, proj_out.T,
        head_lambda, head_gain.reshape(1, VDIM),
        cache_keys.reshape(batch, span, 128), cache_values.reshape(batch, span, VDIM), live_length,
    )
    return updated.astype(BF16)


def solution(mesh):
    split = Mesh(
        mesh.devices.reshape(mesh.shape["dp"], NZ, NY, mesh.shape["tp"]),
        ("dp", "kv_0", "kv_1", "tp"),
    )
    return jax.shard_map(
        local,
        mesh=split,
        in_specs=(
            P("dp", KV_TP),
            P(),
            P(None, KV_TP, None),
            P(None, KV_TP, None),
            P(None, KV_TP, None),
            P(KV, "tp"),
            P(KV, "tp"),
            P(KV, "tp"),
            P("tp", KV),
            P("tp"),
            P(),
            P("dp", KV, "tp", None),
            P("dp", KV, "tp", None),
            P("dp"),
        ),
        out_specs=P("dp", KV_TP),
        check_vma=False,
    )
```

```python
import functools

import jax
import jax.numpy as jnp
from jax import lax
from jax.experimental import pallas as pl
from jax.experimental.pallas import tpu as pltpu
from jax.sharding import Mesh
from jax.sharding import PartitionSpec as P

D = 2048
HEAD = 64
VDIM = 128
NZ = 16
NY = 4
NC = 2
NYC = NY * NC
LANES = 128
KV_TP = ("kv_0", "kv_1", "tp")
KV = ("kv_0", "kv_1")
MESH = pl.DeviceIdType.MESH
F32 = jnp.float32
BF16 = jnp.bfloat16
EPS = 1e-05
NT = (((1,), (1,)), ((), ()))

Z_STEPS = (8, 7, 9, 6, 10, 5, 11, 4, 12, 3, 13, 2, 14, 1, 15)
Y_STEPS = (2, 1, 3)
REACH = 4
NEAR_STEPS = (4, 12, 3, 13, 2, 14, 1, 15)
WEIGHT_ROWS = 48


def iota(shape, dim):
    return lax.broadcasted_iota(jnp.int32, shape, dim)


def mix_part(rows, gain, weights):
    scale = lax.rsqrt(jnp.mean(rows * rows, axis=1, keepdims=True) + EPS)
    normed = (rows * scale * gain).astype(BF16)
    gate = lax.dot_general(normed, weights[0], NT, preferred_element_type=F32)
    up = lax.dot_general(normed, weights[1], NT, preferred_element_type=F32)
    hidden = (gate / (1.0 + jnp.exp(-gate)) * up).astype(BF16)
    return 0.5 * jnp.dot(hidden, weights[2], preferred_element_type=F32)


def layer_kernel(
    res_h, gains_h, gate_h, up_h, down_h, wq_h, wk_h, wv_h, po_h, lam_h, hgain_h, ck_h, cv_h, live_h,
    out,
    res, gains, lam, hgain, live,
    raw, stage, wts, wqb, wkb, wvb, pob, lams, kbuf, vbuf,
    a1, a2, b1s, b1r, b2, cs, csq, c2, c3s, c3, d1s, d1r, d2o, d2m, hs, d3s, d3, ps, f2, fs, g1s, g1r, g2,
    hsem, ssem, rsem,
):
    z = lax.axis_index("kv_0")
    y = lax.axis_index("kv_1")
    c = lax.axis_index("tp")
    hidden_rows = raw.shape[1]
    barrier = pltpu.get_barrier_semaphore()
    drains = []

    def z_peer(k):
        return lax.rem(z + k, NZ)

    def y_peer(k):
        return lax.rem(y + k, NY)

    def send(s, r, src, dst, device):
        pltpu.make_async_remote_copy(
            src_ref=src, dst_ref=dst, send_sem=ssem.at[s], recv_sem=rsem.at[r],
            device_id=device, device_id_type=MESH,
        ).start()

    def waits(s, r, ref):
        return pltpu.make_async_remote_copy(
            src_ref=ref, dst_ref=ref, send_sem=ssem.at[s], recv_sem=rsem.at[r],
            device_id={"kv_0": z}, device_id_type=MESH,
        )

    def arrive(r, ref):
        waits(r, r, ref).wait_recv()

    def drain(s, ref):
        drains.append(waits(s, s, ref))

    def signal(device):
        pl.semaphore_signal(barrier, inc=1, device_id=device, device_id_type=MESH)

    def to_z(phase, src_of, dst):
        for k in Z_STEPS:
            p = z_peer(k)
            send(phase, phase, src_of(p), dst.at[z], {"kv_0": p})

    def to_y(phase, src, dst):
        for k in Y_STEPS:
            send(phase, phase, src, dst, {"kv_1": y_peer(k)})

    def total(buf, count):
        acc = buf[0].astype(F32)
        for k in range(1, count):
            acc = acc + buf[k].astype(F32)
        return acc

    def load(k):
        if k < 3:
            return pltpu.make_async_copy((gate_h, up_h, down_h)[k], raw.at[k], hsem.at[k])
        src = (ck_h, cv_h, res_h, gains_h, lam_h, hgain_h, live_h)[k - 3]
        return pltpu.make_async_copy(src, (kbuf, vbuf, res, gains, lam, hgain, live)[k - 3], hsem.at[k])

    for k in (5, 7, 0, 1, 2, 6, 8, 9, 3, 4):
        load(k).start()

    def own_tile():
        spread = (iota((16, LANES), 1) == iota((16, LANES), 0) + (y * NC + c) * 16).astype(F32).astype(BF16)
        return jnp.dot(res[...], spread, preferred_element_type=F32).astype(BF16)

    lane = iota((8, LANES), 1)
    row = iota((8, LANES), 0)

    def own_lambdas():
        head = row // 2
        return jnp.where(head == 0, lam[0], jnp.where(head == 1, lam[1], jnp.where(head == 2, lam[2], lam[3])))

    def attend():
        span = kbuf.shape[1]
        position = (z * NY + y) * span + iota((8, span), 1)
        for b in range(8):
            query = c3[b // 2].astype(F32)[(b % 2) * 8 : (b % 2) * 8 + 8].astype(BF16)
            scores = lax.dot_general(query, kbuf[b], NT, preferred_element_type=F32) * HEAD**-0.5
            alive = position < live[b]
            highest = jnp.max(jnp.where(alive, scores, -1e30), axis=1, keepdims=True)
            terms = jnp.where(alive, jnp.exp(scores - highest), 0.0)
            count = jnp.sum(terms, axis=1, keepdims=True)
            d1s[b // 2, (b % 2) * 8 : (b % 2) * 8 + 8, :] = jnp.dot(
                terms.astype(BF16), vbuf[b], preferred_element_type=F32
            )
            pair = jnp.where(lax.rem(lane, HEAD) < HEAD // 2, highest, count)
            stats = pair if b % 2 == 0 else jnp.where(lane < HEAD, stats, pair)
            if b % 2 == 1:
                d1s[b // 2, 16:24, :] = stats

    def finish(stream_two):
        updated = stream_two.astype(F32) + total(g2, NY)
        out[...] = pltpu.roll(updated, lax.rem(LANES - (y * NC + c) * 16, LANES), 1)[:, :16]
        for each in drains:
            each.wait_send()
        drains.clear()

    @pl.when(c == 0)
    def _():
        core1 = {"tp": 1}

        def all_core1(s, r, src, dst):
            for k in Y_STEPS + (0,):
                send(s, r, src, dst, {"kv_1": y_peer(k), "tp": 1})

        for k in Y_STEPS + (0,):
            signal({"kv_1": y_peer(k), "tp": 1})
        load(5).wait()
        a1[y * NC] = own_tile()
        pl.semaphore_wait(barrier, NY)

        all_core1(A1, A1, a1.at[y * NC], a1.at[y * NC])
        drain(A1, a1.at[pl.ds(0, NY)])
        load(7).wait()
        lams[0] = own_lambdas()
        send(LAM, LAM, lams.at[0], lams.at[0], core1)
        drain(LAM, lams.at[0])
        stage[:, :, 40:WEIGHT_ROWS, :] = jnp.zeros((2, 3, WEIGHT_ROWS - 40, D), BF16)
        for half in range(2):
            for m in range(3):
                if half == 0:
                    load(m).wait()
                stage[half, m, 0:hidden_rows, :] = raw.at[m][:, half, :]
            for m in range(3):
                send(W0 + half, W0 + half, stage.at[half, m], wts.at[half, m, pl.ds(WEIGHT_ROWS, WEIGHT_ROWS)], core1)
            drain(W0 + half, stage.at[half])
            if half == 0:
                part = pl.ds(pl.multiple_of(y * 32, 32), 32)
                all_core1(WQ, WQ, wq_h, wqb.at[0, part])
                all_core1(WK, WK, wk_h, wkb.at[0, part])
                all_core1(WV, WV, wv_h, wvb.at[0, part])
                drain(WQ, wqb.at[0])
                drain(WK, wkb.at[0])
                drain(WV, wvb.at[0])
        all_core1(WO, WO, po_h, pob.at[part, pl.ds(0, 512)])
        drain(WO, pob.at[:, pl.ds(0, 512)])

        for k in (3, 4, 6, 8, 9):
            load(k).wait()
        arrive(C3, c3)
        attend()
        for k in Y_STEPS + (0,):
            p = y_peer(k)
            send(D1, D1, d1s.at[p], d1r.at[y * NC], {"kv_1": p, "tp": 1})
        drain(D1, d1s)
        arrive(FS, fs)
        arrive(G2, g2)
        finish(fs[...])

    @pl.when(c == 1)
    def _():
        for k in NEAR_STEPS:
            signal({"kv_0": z_peer(k)})
        for k in Y_STEPS + (0,):
            signal({"kv_1": y_peer(k), "tp": 0})
        for k in Y_STEPS:
            signal({"kv_1": y_peer(k)})
        part = pl.ds(pl.multiple_of(y * 32, 32), 32)
        pulls = [
            pltpu.make_async_copy(wq_h, wqb.at[1, part], hsem.at[10]),
            pltpu.make_async_copy(wk_h, wkb.at[1, part], hsem.at[11]),
            pltpu.make_async_copy(wv_h, wvb.at[1, part], hsem.at[12]),
            pltpu.make_async_copy(po_h, pob.at[part, pl.ds(512, 512)], hsem.at[13]),
        ]
        for pull in pulls:
            pull.start()
        load(5).wait()
        a1[y * NC + 1] = own_tile()

        def relayout(half):
            for m in range(3):
                wts[half, m, 0:hidden_rows, :] = raw.at[m][:, half, :]

        wts[:, :, 40:WEIGHT_ROWS, :] = jnp.zeros((2, 3, WEIGHT_ROWS - 40, D), BF16)
        for m in range(3):
            load(m).wait()
        relayout(0)
        pl.semaphore_wait(barrier, len(NEAR_STEPS) + NY + (NY - 1))

        to_y(A1, a1.at[y * NC + 1], a1.at[y * NC + 1])
        drain(A1, a1.at[pl.ds(0, NY - 1)])
        arrive(A1, a1.at[pl.ds(0, NYC - 1)])
        res_z = total(a1, NYC)
        a2[z] = res_z.astype(BF16)
        for k in NEAR_STEPS:
            send(A2, A2, a2.at[z], a2.at[z], {"kv_0": z_peer(k)})
        drain(A2, a2.at[pl.ds(0, len(NEAR_STEPS))])
        to_y(WQ, wq_h, wqb.at[1, part])
        to_y(WK, wk_h, wkb.at[1, part])
        to_y(WV, wv_h, wvb.at[1, part])
        to_y(WO, po_h, pob.at[part, pl.ds(512, 512)])
        drain(WQ, wqb.at[1, pl.ds(0, 96)])
        drain(WK, wkb.at[1, pl.ds(0, 96)])
        drain(WV, wvb.at[1, pl.ds(0, 96)])
        drain(WO, pob.at[pl.ds(0, 96), pl.ds(512, 512)])
        load(7).wait()
        lams[1] = own_lambdas()
        arrive(A2, a2.at[pl.ds(0, len(NEAR_STEPS))])
        for k in range(1, REACH + 1):
            far = z_peer(NZ - k)
            send(A3, A3, a2.at[far], a2.at[far], {"kv_0": z_peer(REACH)})
            if k < REACH:
                far = z_peer(k)
                send(A3, A3, a2.at[far], a2.at[far], {"kv_0": z_peer(NZ - REACH)})
        drain(A3, a2.at[pl.ds(0, 2 * REACH - 1)])
        relayout(1)
        for k in (6, 8, 9):
            load(k).wait()
        for pull in pulls:
            pull.wait()
        arrive(W0, wts.at[0, :, pl.ds(WEIGHT_ROWS, WEIGHT_ROWS)])
        arrive(A3, a2.at[pl.ds(0, 2 * REACH - 1)])
        rows = jnp.concatenate([a2[k].astype(F32) for k in range(NZ)], axis=1)

        mixed = mix_part(rows, gains[0:1, :], [wts[0, m] for m in range(3)])
        for k in range(NZ):
            b1s[k] = mixed[:, k * LANES : (k + 1) * LANES]
        to_z(B1, lambda p: b1s.at[p], b1r)
        drain(B1, b1s.at[pl.ds(0, NZ - 1)])
        b1r[z] = b1s[z]
        arrive(B1, b1r.at[pl.ds(0, NZ - 1)])
        b2[y] = total(b1r, NZ)
        to_y(B2, b2.at[y], b2.at[y])
        drain(B2, b2.at[pl.ds(0, NY - 1)])
        arrive(WQ, wqb.at[:, pl.ds(0, 112)])
        arrive(WK, wkb.at[:, pl.ds(0, 112)])
        arrive(WV, wvb.at[:, pl.ds(0, 112)])
        arrive(B2, b2.at[pl.ds(0, NY - 1)])
        stream_one = (res_z + total(b2, NY)).astype(BF16).astype(F32)

        squares = jnp.sum(stream_one * stream_one, axis=1, keepdims=True)
        csq[z] = jnp.sum(jnp.where(lane == row, squares, 0.0), axis=0, keepdims=True)
        to_z(CQ, lambda p: csq.at[z], csq)
        drain(CQ, csq.at[pl.ds(0, NZ - 1)])
        gain_z = gains[1:2, pl.ds(pl.multiple_of(z * LANES, LANES), LANES)]
        scaled = (stream_one * gain_z).astype(BF16)
        for t in range(2):
            query = jnp.dot(scaled, wqb[t], preferred_element_type=F32)
            for g in range(4):
                cs[pl.ds(t * 4 + g, 8, stride=12), :] = query[:, g * LANES : (g + 1) * LANES]
            cs[pl.ds(8 + t, 8, stride=12), :] = jnp.dot(scaled, wkb[t], preferred_element_type=F32)
            cs[pl.ds(10 + t, 8, stride=12), :] = jnp.dot(scaled, wvb[t], preferred_element_type=F32)
        pair = pl.ds(pl.multiple_of(y * 24, 8), 24)
        to_z(C2, lambda p: cs.at[pair], c2)
        drain(C2, c2.at[pl.ds(0, NZ - 1)])
        c2[z] = cs[pair, :]
        arrive(CQ, csq.at[pl.ds(0, NZ - 1)])
        square_line = total(csq, NZ)
        arrive(C2, c2.at[pl.ds(0, NZ - 1)])
        sums = total(c2, NZ)
        query_rows, key_rows, value_rows = [], [], []
        lane1 = iota((1, LANES), 1)
        for s in range(2):
            square = jnp.sum(jnp.where(lane1 == 2 * y + s, square_line, 0.0), axis=1, keepdims=True)
            factor = lax.rsqrt(square / D + EPS)
            block = (sums[s * 12 : (s + 1) * 12] * factor).astype(BF16).astype(F32)
            for h in range(8):
                query_rows += [block[h : h + 1], block[h : h + 1]]
            for t in range(2):
                key_rows.append(jnp.broadcast_to(block[8 + t : 9 + t], (8, LANES)))
                value_rows.append(jnp.broadcast_to(block[10 + t : 11 + t], (8, LANES)))
        row32 = iota((32, LANES), 0)
        lane32 = iota((32, LANES), 1)
        component = lax.rem(row32, 2)
        queries = jnp.where((lane32 >= HEAD) == (component == 1), jnp.concatenate(query_rows, axis=0), 0.0)
        for t in range(2):
            c3s[t] = jnp.concatenate(
                [queries[t * 8 : t * 8 + 8], queries[16 + t * 8 : 24 + t * 8]], axis=0
            ).astype(BF16)
        for k in Y_STEPS:
            send(C3S, C3, c3s.at[0], c3.at[y], {"kv_1": y_peer(k), "tp": 0})
            send(C3, C3, c3s.at[1], c3.at[y], {"kv_1": y_peer(k)})
        send(C3S, C3, c3s.at[0], c3.at[y], {"tp": 0})
        drain(C3S, c3)
        drain(C3, c3.at[pl.ds(0, NY - 1)])
        c3[y] = c3s[1]
        key_new = jnp.concatenate(key_rows, axis=0)
        value_new = jnp.concatenate(value_rows, axis=0)
        own_score = jnp.sum(queries * key_new, axis=1, keepdims=True) * HEAD**-0.5
        load(3).wait()
        load(4).wait()
        arrive(C3, c3.at[pl.ds(0, NY - 1)])
        attend()
        for k in Y_STEPS:
            p = y_peer(k)
            send(D1, D1, d1s.at[p], d1r.at[y * NC + 1], {"kv_1": p})
        drain(D1, d1s.at[pl.ds(0, NY - 1)])
        d1r[y * NC + 1] = d1s[y]
        arrive(LAM, lams.at[0])
        arrive(WO, pob.at[pl.ds(0, 112)])
        arrive(W1, wts.at[1, :, pl.ds(WEIGHT_ROWS, WEIGHT_ROWS)])
        arrive(D1, d1r.at[pl.ds(0, NYC - 1)])

        both = [(s, t) for s in range(2) for t in range(2)]

        def stat(k, at):
            return jnp.concatenate(
                [d1r[k * NC + t, 16:24, s * HEAD + at : s * HEAD + at + 1] for s, t in both], axis=0
            )

        def gathered(k):
            return jnp.concatenate([d1r[k * NC + t, s * 8 : s * 8 + 8, :] for s, t in both], axis=0)

        tops = [stat(k, 0) for k in range(NY)]
        counts = [stat(k, HEAD // 2) for k in range(NY)]
        top = functools.reduce(jnp.maximum, tops)
        weights = [jnp.exp(t - top) for t in tops]
        count = functools.reduce(jnp.add, [w * s for w, s in zip(weights, counts)])
        values = functools.reduce(jnp.add, [weights[k] * gathered(k) for k in range(NY)])
        line = jnp.where(lane32 == row32, top, 0.0) + jnp.where(lane32 == row32 + HEAD, count, 0.0)
        d2m[z] = jnp.sum(line, axis=0, keepdims=True)
        to_z(D2M, lambda p: d2m.at[z], d2m)
        drain(D2M, d2m.at[pl.ds(0, NZ - 1)])
        d2o[z] = values.astype(BF16)
        to_z(D2O, lambda p: d2o.at[z], d2o)
        drain(D2O, d2o.at[pl.ds(0, NZ - 1)])
        arrive(D2M, d2m.at[pl.ds(0, NZ - 1)])
        tops = [jnp.sum(jnp.where(lane32 == row32, d2m[k], 0.0), axis=1, keepdims=True) for k in range(NZ)]
        counts = [jnp.sum(jnp.where(lane32 == row32 + HEAD, d2m[k], 0.0), axis=1, keepdims=True) for k in range(NZ)]
        top = functools.reduce(jnp.maximum, tops, own_score)
        weights = [jnp.exp(t - top) for t in tops]
        own_weight = jnp.exp(own_score - top)
        count = functools.reduce(jnp.add, [w * s for w, s in zip(weights, counts)], own_weight)
        arrive(D2O, d2o.at[pl.ds(0, NZ - 1)])
        values = own_weight * value_new
        for k in range(NZ):
            values = values + weights[k] * d2o[k].astype(F32)
        ratio = values / count
        lambdas = jnp.concatenate([lams[0], lams[1], lams[0], lams[1]], axis=0)
        mixed = ratio - lambdas * pltpu.roll(ratio, 31, 0)
        scale = lax.rsqrt(jnp.mean(mixed * mixed, axis=1, keepdims=True) + EPS)
        hs[...] = mixed * scale * hgain[...]
        d3s[...] = hs[pl.ds(0, 16, stride=2), :].astype(BF16)
        to_y(D3, d3s, d3.at[y])
        drain(D3, d3.at[pl.ds(0, NY - 1)])
        d3[y] = d3s[...]
        arrive(D3, d3.at[pl.ds(0, NY - 1)])

        for k in range(NY):
            ps[k * 16 : (k + 1) * 16, :] = d3[k].astype(F32)
        heads = jnp.concatenate([ps[pl.ds(h, 8, stride=8), :] for h in range(8)], axis=1).astype(BF16)
        projected = lax.dot_general(heads, pob[...], NT, preferred_element_type=F32)
        stream_two = (stream_one + projected).astype(BF16)
        f2[z] = stream_two
        fs[...] = stream_two
        to_z(F2, lambda p: f2.at[z], f2)
        drain(F2, f2.at[pl.ds(0, NZ - 1)])
        send(FS, FS, fs, fs, {"tp": 0})
        drain(FS, fs)
        arrive(F2, f2.at[pl.ds(0, NZ - 1)])
        rows = jnp.concatenate([f2[k].astype(F32) for k in range(NZ)], axis=1)

        mixed = mix_part(rows, gains[2:3, :], [wts[1, m] for m in range(3)])
        for k in range(NZ):
            g1s[k] = mixed[:, k * LANES : (k + 1) * LANES]
        to_z(G1, lambda p: g1s.at[p], g1r)
        drain(G1, g1s.at[pl.ds(0, NZ - 1)])
        g1r[z] = g1s[z]
        arrive(G1, g1r.at[pl.ds(0, NZ - 1)])
        g2[y] = total(g1r, NZ)
        for k in Y_STEPS:
            send(G2S, G2, g2.at[y], g2.at[y], {"kv_1": y_peer(k), "tp": 0})
            send(G2, G2, g2.at[y], g2.at[y], {"kv_1": y_peer(k)})
        send(G2S, G2, g2.at[y], g2.at[y], {"tp": 0})
        drain(G2S, g2)
        drain(G2, g2.at[pl.ds(0, NY - 1)])
        arrive(G2, g2.at[pl.ds(0, NY - 1)])
        finish(stream_two)


PHASES = 28
(
    A1, A2, A3, B1, B2, CQ, C2, C3, C3S, D1, D2O, D2M, D3, F2, FS, G1, G2, G2S, LAM, W0, W1, WQ, WK, WV, WO,
) = range(25)


def local(
    residual, norm_gains, ffn_gate, ffn_up, ffn_down, proj_query, proj_key, proj_value, proj_out,
    head_lambda, head_gain, cache_keys, cache_values, live_length,
):
    batch = residual.shape[0]
    hidden = ffn_gate.shape[1]
    span = cache_keys.shape[1]
    vmem = pl.BlockSpec(memory_space=pltpu.VMEM)
    hbm = pl.BlockSpec(memory_space=pl.ANY)
    updated = pl.pallas_call(
        layer_kernel,
        out_shape=pltpu.VMEM(residual.shape, F32),
        in_specs=[hbm] * 14,
        out_specs=vmem,
        scratch_shapes=[
            pltpu.VMEM(residual.shape, BF16),
            pltpu.VMEM(norm_gains.shape, F32),
            pltpu.SMEM(head_lambda.shape, F32),
            pltpu.VMEM((1, VDIM), F32),
            pltpu.SMEM(live_length.shape, jnp.int32),
            pltpu.VMEM((3, hidden, 2, D), BF16),
            pltpu.VMEM((2, 3, WEIGHT_ROWS, D), BF16),
            pltpu.VMEM((2, 3, 2 * WEIGHT_ROWS, D), BF16),
            pltpu.VMEM((2, LANES, 512), BF16),
            pltpu.VMEM((2, LANES, 128), BF16),
            pltpu.VMEM((2, LANES, 128), BF16),
            pltpu.VMEM((LANES, 1024), BF16),
            pltpu.VMEM((2, 8, LANES), F32),
            pltpu.VMEM((batch, span, 128), BF16),
            pltpu.VMEM((batch, span, VDIM), BF16),
            pltpu.VMEM((NYC, 8, LANES), BF16),
            pltpu.VMEM((NZ, 8, LANES), BF16),
            pltpu.VMEM((NZ, 8, LANES), F32),
            pltpu.VMEM((NZ, 8, LANES), F32),
            pltpu.VMEM((NY, 8, LANES), F32),
            pltpu.VMEM((96, LANES), F32),
            pltpu.VMEM((NZ, 1, LANES), F32),
            pltpu.VMEM((NZ, 24, LANES), F32),
            pltpu.VMEM((2, 16, LANES), BF16),
            pltpu.VMEM((NY, 16, LANES), BF16),
            pltpu.VMEM((NY, 24, LANES), F32),
            pltpu.VMEM((NYC, 24, LANES), F32),
            pltpu.VMEM((NZ, 32, LANES), BF16),
            pltpu.VMEM((NZ, 1, LANES), F32),
            pltpu.VMEM((32, LANES), F32),
            pltpu.VMEM((16, LANES), BF16),
            pltpu.VMEM((NY, 16, LANES), BF16),
            pltpu.VMEM((64, LANES), F32),
            pltpu.VMEM((NZ, 8, LANES), BF16),
            pltpu.VMEM((8, LANES), BF16),
            pltpu.VMEM((NZ, 8, LANES), F32),
            pltpu.VMEM((NZ, 8, LANES), F32),
            pltpu.VMEM((NY, 8, LANES), F32),
            pltpu.SemaphoreType.DMA((14,)),
            pltpu.SemaphoreType.DMA((PHASES,)),
            pltpu.SemaphoreType.DMA((PHASES,)),
        ],
        compiler_params=pltpu.CompilerParams(
            collective_id=0, has_side_effects=True,
        ),
    )(
        residual, norm_gains,
        jnp.swapaxes(ffn_gate, 0, 1), jnp.swapaxes(ffn_up, 0, 1), jnp.swapaxes(ffn_down, 0, 1),
        proj_query, proj_key, proj_value, proj_out.T,
        head_lambda, head_gain.reshape(1, VDIM),
        cache_keys.reshape(batch, span, 128), cache_values.reshape(batch, span, VDIM), live_length,
    )
    return updated.astype(BF16)


def solution(mesh):
    split = Mesh(
        mesh.devices.reshape(mesh.shape["dp"], NZ, NY, mesh.shape["tp"]),
        ("dp", "kv_0", "kv_1", "tp"),
    )
    return jax.shard_map(
        local,
        mesh=split,
        in_specs=(
            P("dp", KV_TP),
            P(),
            P(None, KV_TP, None),
            P(None, KV_TP, None),
            P(None, KV_TP, None),
            P(KV, "tp"),
            P(KV, "tp"),
            P(KV, "tp"),
            P("tp", KV),
            P("tp"),
            P(),
            P("dp", KV, "tp", None),
            P("dp", KV, "tp", None),
            P("dp"),
        ),
        out_specs=P("dp", KV_TP),
        check_vma=False,
    )
```

```python
import functools

import jax
import jax.numpy as jnp
from jax import lax
from jax.experimental import pallas as pl
from jax.experimental.pallas import tpu as pltpu
from jax.sharding import Mesh
from jax.sharding import PartitionSpec as P

D = 2048
HEAD = 64
VDIM = 128
NZ = 16
NY = 4
NC = 2
NYC = NY * NC
LANES = 128
KV_TP = ("kv_0", "kv_1", "tp")
KV = ("kv_0", "kv_1")
MESH = pl.DeviceIdType.MESH
F32 = jnp.float32
BF16 = jnp.bfloat16
EPS = 1e-05
NT = (((1,), (1,)), ((), ()))

Z_STEPS = (8, 7, 9, 6, 10, 5, 11, 4, 12, 3, 13, 2, 14, 1, 15)
Y_STEPS = (2, 1, 3)
REACH = 4
NEAR_STEPS = (4, 12, 3, 13, 2, 14, 1, 15)
FAR_STEPS = (8, 7, 9, 6, 10, 5, 11)
WEIGHT_ROWS = 48


def iota(shape, dim):
    return lax.broadcasted_iota(jnp.int32, shape, dim)


def mix_part(rows, gain, weights):
    scale = lax.rsqrt(jnp.mean(rows * rows, axis=1, keepdims=True) + EPS)
    normed = (rows * scale * gain).astype(BF16)
    gate = lax.dot_general(normed, weights[0], NT, preferred_element_type=F32)
    up = lax.dot_general(normed, weights[1], NT, preferred_element_type=F32)
    hidden = (gate / (1.0 + jnp.exp(-gate)) * up).astype(BF16)
    return 0.5 * jnp.dot(hidden, weights[2], preferred_element_type=F32)


def layer_kernel(
    res_h, gains_h, gate_h, up_h, down_h, wq_h, wk_h, wv_h, po_h, lam_h, hgain_h, ck_h, cv_h, live_h,
    out,
    res, gains, lam, hgain, live,
    raw, stage, wts, wqb, wkb, wvb, pob, lams, kbuf, vbuf,
    a1, a2, b1s, b1r, b2, cs, ckvs, csq, c2, ckv, c3s, c3, d1s, d1r, d2o, d2m, hs, d3s, d3, ps, f2, fs, g1s, g1r, g2,
    hsem, ssem, rsem,
):
    z = lax.axis_index("kv_0")
    y = lax.axis_index("kv_1")
    c = lax.axis_index("tp")
    hidden_rows = raw.shape[1]
    barrier = pltpu.get_barrier_semaphore()
    drains = []

    def z_peer(k):
        return lax.rem(z + k, NZ)

    def lateness(p):
        return jnp.minimum(p, NZ - p)

    def y_peer(k):
        return lax.rem(y + k, NY)

    def send(s, r, src, dst, device):
        pltpu.make_async_remote_copy(
            src_ref=src, dst_ref=dst, send_sem=ssem.at[s], recv_sem=rsem.at[r],
            device_id=device, device_id_type=MESH,
        ).start()

    def waits(s, r, ref):
        return pltpu.make_async_remote_copy(
            src_ref=ref, dst_ref=ref, send_sem=ssem.at[s], recv_sem=rsem.at[r],
            device_id={"kv_0": z}, device_id_type=MESH,
        )

    def arrive(r, ref):
        waits(r, r, ref).wait_recv()

    def drain(s, ref):
        drains.append(waits(s, s, ref))

    def signal(device):
        pl.semaphore_signal(barrier, inc=1, device_id=device, device_id_type=MESH)

    def to_z(phase, src_of, dst):
        for k in Z_STEPS:
            p = z_peer(k)
            send(phase, phase, src_of(p), dst.at[z], {"kv_0": p})

    def to_y(phase, src, dst):
        for k in Y_STEPS:
            send(phase, phase, src, dst, {"kv_1": y_peer(k)})

    def total(buf, count):
        acc = buf[0].astype(F32)
        for k in range(1, count):
            acc = acc + buf[k].astype(F32)
        return acc

    def load(k):
        if k < 3:
            return pltpu.make_async_copy((gate_h, up_h, down_h)[k], raw.at[k], hsem.at[k])
        src = (ck_h, cv_h, res_h, gains_h, lam_h, hgain_h, live_h)[k - 3]
        return pltpu.make_async_copy(src, (kbuf, vbuf, res, gains, lam, hgain, live)[k - 3], hsem.at[k])

    for k in (5, 7, 0, 1, 2, 6, 8, 9, 3, 4):
        load(k).start()

    def own_tile():
        spread = (iota((16, LANES), 1) == iota((16, LANES), 0) + (y * NC + c) * 16).astype(F32).astype(BF16)
        return jnp.dot(res[...], spread, preferred_element_type=F32).astype(BF16)

    lane = iota((8, LANES), 1)
    row = iota((8, LANES), 0)

    def own_lambdas():
        head = row // 2
        return jnp.where(head == 0, lam[0], jnp.where(head == 1, lam[1], jnp.where(head == 2, lam[2], lam[3])))

    def attend():
        span = kbuf.shape[1]
        position = (z * NY + y) * span + iota((8, span), 1)
        queries = jnp.concatenate([c3[k] for k in range(NY)], axis=0).astype(F32)
        scores = jnp.concatenate(
            [
                lax.dot_general(
                    queries[b * 8 : b * 8 + 8].astype(BF16), kbuf[b], NT, preferred_element_type=F32
                )
                for b in range(8)
            ],
            axis=0,
        ) * HEAD**-0.5
        alive = jnp.concatenate([(position < live[b]).astype(F32) for b in range(8)], axis=0) > 0.0
        highest = jnp.max(jnp.where(alive, scores, -1e30), axis=1, keepdims=True)
        terms = jnp.where(alive, jnp.exp(scores - highest), 0.0)
        weights = terms.astype(BF16)
        values = [jnp.dot(weights[b * 8 : b * 8 + 8], vbuf[b], preferred_element_type=F32) for b in range(8)]
        count = jnp.sum(terms, axis=1, keepdims=True)
        for k in range(NY):
            pairs = [
                jnp.where(
                    lax.rem(lane, HEAD) < HEAD // 2, highest[b * 8 : b * 8 + 8], count[b * 8 : b * 8 + 8]
                )
                for b in (2 * k, 2 * k + 1)
            ]
            d1s[k, 0:8, :] = values[2 * k]
            d1s[k, 8:16, :] = values[2 * k + 1]
            d1s[k, 16:24, :] = jnp.where(lane < HEAD, pairs[0], pairs[1])

    def sent_all():
        for each in drains:
            each.wait_send()
        drains.clear()

    def finish(stream_two):
        updated = stream_two.astype(F32) + total(g2, NY)
        sent_all()
        out[...] = pltpu.roll(updated, lax.rem(LANES - (y * NC + c) * 16, LANES), 1)[:, :16]

    @pl.when(c == 0)
    def _():
        core1 = {"tp": 1}

        def all_core1(s, r, src, dst):
            for k in Y_STEPS + (0,):
                send(s, r, src, dst, {"kv_1": y_peer(k), "tp": 1})

        for k in Y_STEPS + (0,):
            signal({"kv_1": y_peer(k), "tp": 1})
        load(5).wait()
        a1[y * NC] = own_tile()
        pl.semaphore_wait(barrier, NY)

        all_core1(A1, A1, a1.at[y * NC], a1.at[y * NC])
        drain(A1, a1.at[pl.ds(0, NY)])
        load(7).wait()
        lams[0] = own_lambdas()
        send(LAM, LAM, lams.at[0], lams.at[0], core1)
        drain(LAM, lams.at[0])
        stage[:, :, 40:WEIGHT_ROWS, :] = jnp.zeros((2, 3, WEIGHT_ROWS - 40, D), BF16)
        for half in range(2):
            for m in range(3):
                if half == 0:
                    load(m).wait()
                stage[half, m, 0:hidden_rows, :] = raw.at[m][:, half, :]
            for m in range(3):
                send(W0 + half, W0 + half, stage.at[half, m], wts.at[half, m, pl.ds(WEIGHT_ROWS, WEIGHT_ROWS)], core1)
            drain(W0 + half, stage.at[half])
            if half == 0:
                part = pl.ds(pl.multiple_of(y * 32, 32), 32)
                all_core1(WQ, WQ, wq_h, wqb.at[0, part])
                all_core1(WK, WK, wk_h, wkb.at[0, part])
                all_core1(WV, WV, wv_h, wvb.at[0, part])
                drain(WQ, wqb.at[0])
                drain(WK, wkb.at[0])
                drain(WV, wvb.at[0])
        all_core1(WO, WO, po_h, pob.at[part, pl.ds(0, 512)])
        drain(WO, pob.at[:, pl.ds(0, 512)])

        for k in (3, 4, 6, 8, 9):
            load(k).wait()
        arrive(C3, c3)
        attend()
        for k in Y_STEPS + (0,):
            p = y_peer(k)
            send(D1, D1, d1s.at[p], d1r.at[y * NC], {"kv_1": p, "tp": 1})
        drain(D1, d1s)
        sent_all()
        arrive(FS, fs)
        arrive(G2, g2)
        finish(fs[...])

    @pl.when(c == 1)
    def _():
        for k in Y_STEPS + (0,):
            signal({"kv_1": y_peer(k), "tp": 0})
        for k in Y_STEPS:
            signal({"kv_1": y_peer(k)})
        for k in NEAR_STEPS:
            signal({"kv_0": z_peer(k)})
        greeted = len(NEAR_STEPS) + NY + (NY - 1)
        for k in FAR_STEPS:
            p = z_peer(k)

            @pl.when(lateness(z) <= lateness(p))
            def _():
                signal({"kv_0": p})

            greeted = greeted + (lateness(p) <= lateness(z)).astype(jnp.int32)
        part = pl.ds(pl.multiple_of(y * 32, 32), 32)
        pulls = [
            pltpu.make_async_copy(wq_h, wqb.at[1, part], hsem.at[10]),
            pltpu.make_async_copy(wk_h, wkb.at[1, part], hsem.at[11]),
            pltpu.make_async_copy(wv_h, wvb.at[1, part], hsem.at[12]),
            pltpu.make_async_copy(po_h, pob.at[part, pl.ds(512, 512)], hsem.at[13]),
        ]
        for pull in pulls:
            pull.start()
        load(5).wait()
        a1[y * NC + 1] = own_tile()

        def relayout(half):
            for m in range(3):
                wts[half, m, 0:hidden_rows, :] = raw.at[m][:, half, :]

        pl.semaphore_wait(barrier, greeted)

        to_y(A1, a1.at[y * NC + 1], a1.at[y * NC + 1])
        drain(A1, a1.at[pl.ds(0, NY - 1)])
        wts[:, :, 40:WEIGHT_ROWS, :] = jnp.zeros((2, 3, WEIGHT_ROWS - 40, D), BF16)
        for m in range(3):
            load(m).wait()
        relayout(0)
        arrive(A1, a1.at[pl.ds(0, NYC - 1)])
        res_z = total(a1, NYC)
        a2[z] = res_z.astype(BF16)
        far_sends = 0
        for k in FAR_STEPS:
            p = z_peer(k)
            known = lateness(z) >= lateness(p)

            @pl.when(known)
            def _():
                send(A3, A3, a2.at[z], a2.at[z], {"kv_0": p})

            far_sends = far_sends + known.astype(jnp.int32)
        for k in range(REACH, 0, -1):
            send(A2R, A2L, a2.at[z], a2.at[z], {"kv_0": z_peer(k)})
            send(A2L, A2R, a2.at[z], a2.at[z], {"kv_0": z_peer(NZ - k)})
        drain(A2R, a2.at[pl.ds(0, REACH)])
        drain(A2L, a2.at[pl.ds(0, REACH)])
        to_y(WQ, wq_h, wqb.at[1, part])
        to_y(WK, wk_h, wkb.at[1, part])
        to_y(WV, wv_h, wvb.at[1, part])
        to_y(WO, po_h, pob.at[part, pl.ds(512, 512)])
        drain(WQ, wqb.at[1, pl.ds(0, 96)])
        drain(WK, wkb.at[1, pl.ds(0, 96)])
        drain(WV, wvb.at[1, pl.ds(0, 96)])
        drain(WO, pob.at[pl.ds(0, 96), pl.ds(512, 512)])
        load(7).wait()
        lams[1] = own_lambdas()
        def hand_on(side, beyond, target):
            for k in range(1, beyond + 1):
                block = z_peer(side * k + NZ)
                asked = lateness(block) < lateness(target)

                @pl.when(asked)
                def _():
                    send(A3, A3, a2.at[block], a2.at[block], {"kv_0": target})


        def from_left():
            arrive(A2L, a2.at[pl.ds(0, REACH)])
            hand_on(-1, REACH, z_peer(REACH))

        def from_right():
            arrive(A2R, a2.at[pl.ds(0, REACH)])
            hand_on(1, REACH - 1, z_peer(NZ - REACH))

        @pl.when(z < NZ // 2)
        def _():
            from_left()
            from_right()

        @pl.when(z >= NZ // 2)
        def _():
            from_right()
            from_left()

        for k in range(1, REACH + 1):
            far_sends = far_sends + (lateness(z_peer(NZ - k)) < lateness(z_peer(REACH))).astype(jnp.int32)
            if k < REACH:
                far_sends = far_sends + (lateness(z_peer(k)) < lateness(z_peer(NZ - REACH))).astype(jnp.int32)

        relayout(1)
        for k in (6, 8, 9):
            load(k).wait()
        for pull in pulls:
            pull.wait()
        arrive(W0, wts.at[0, :, pl.ds(WEIGHT_ROWS, WEIGHT_ROWS)])
        arrive(A3, a2.at[pl.ds(0, 2 * REACH - 1)])
        rows = jnp.concatenate([a2[k].astype(F32) for k in range(NZ)], axis=1)

        mixed = mix_part(rows, gains[0:1, :], [wts[0, m] for m in range(3)])
        for k in range(NZ):
            b1s[k] = mixed[:, k * LANES : (k + 1) * LANES]
        to_z(B1, lambda p: b1s.at[p], b1r)
        drain(B1, b1s.at[pl.ds(0, NZ - 1)])
        b1r[z] = b1s[z]
        arrive(B1, b1r.at[pl.ds(0, NZ - 1)])
        b2[y] = total(b1r, NZ)
        to_y(B2, b2.at[y], b2.at[y])
        drain(B2, b2.at[pl.ds(0, NY - 1)])
        arrive(WQ, wqb.at[:, pl.ds(0, 112)])
        arrive(WK, wkb.at[:, pl.ds(0, 112)])
        arrive(WV, wvb.at[:, pl.ds(0, 112)])
        arrive(B2, b2.at[pl.ds(0, NY - 1)])
        stream_one = (res_z + total(b2, NY)).astype(BF16).astype(F32)

        squares = jnp.sum(stream_one * stream_one, axis=1, keepdims=True)
        csq[z] = jnp.sum(jnp.where(lane == row, squares, 0.0), axis=0, keepdims=True)
        to_z(CQ, lambda p: csq.at[z], csq)
        drain(CQ, csq.at[pl.ds(0, NZ - 1)])
        gain_z = gains[1:2, pl.ds(pl.multiple_of(z * LANES, LANES), LANES)]
        scaled = (stream_one * gain_z).astype(BF16)
        for t in range(2):
            query = jnp.dot(scaled, wqb[t], preferred_element_type=F32)
            for g in range(4):
                cs[pl.ds(t * 4 + g, 8, stride=8), :] = query[:, g * LANES : (g + 1) * LANES]
        pair = pl.ds(pl.multiple_of(y * 16, 16), 16)
        to_z(C2, lambda p: cs.at[pair], c2)
        drain(C2, c2.at[pl.ds(0, NZ - 1)])
        c2[z] = cs[pair, :]
        for t in range(2):
            ckvs[pl.ds(t, 8, stride=4), :] = jnp.dot(scaled, wkb[t], preferred_element_type=F32)
            ckvs[pl.ds(2 + t, 8, stride=4), :] = jnp.dot(scaled, wvb[t], preferred_element_type=F32)
        pair_kv = pl.ds(pl.multiple_of(y * 8, 8), 8)
        to_z(CKV, lambda p: ckvs.at[pair_kv], ckv)
        drain(CKV, ckv.at[pl.ds(0, NZ - 1)])
        ckv[z] = ckvs[pair_kv, :]
        arrive(CQ, csq.at[pl.ds(0, NZ - 1)])
        square_line = total(csq, NZ)
        arrive(C2, c2.at[pl.ds(0, NZ - 1)])
        sums = total(c2, NZ)
        query_rows, factors = [], []
        lane1 = iota((1, LANES), 1)
        for s in range(2):
            square = jnp.sum(jnp.where(lane1 == 2 * y + s, square_line, 0.0), axis=1, keepdims=True)
            factors.append(lax.rsqrt(square / D + EPS))
            block = (sums[s * 8 : (s + 1) * 8] * factors[s]).astype(BF16).astype(F32)
            for h in range(8):
                query_rows += [block[h : h + 1], block[h : h + 1]]
        row32 = iota((32, LANES), 0)
        lane32 = iota((32, LANES), 1)
        component = lax.rem(row32, 2)
        queries = jnp.where((lane32 >= HEAD) == (component == 1), jnp.concatenate(query_rows, axis=0), 0.0)
        for t in range(2):
            c3s[t] = jnp.concatenate(
                [queries[t * 8 : t * 8 + 8], queries[16 + t * 8 : 24 + t * 8]], axis=0
            ).astype(BF16)
        for k in Y_STEPS:
            send(C3S, C3, c3s.at[0], c3.at[y], {"kv_1": y_peer(k), "tp": 0})
            send(C3, C3, c3s.at[1], c3.at[y], {"kv_1": y_peer(k)})
        send(C3S, C3, c3s.at[0], c3.at[y], {"tp": 0})
        drain(C3S, c3)
        drain(C3, c3.at[pl.ds(0, NY - 1)])
        c3[y] = c3s[1]
        load(3).wait()
        load(4).wait()
        arrive(C3, c3.at[pl.ds(0, NY - 1)])
        attend()
        for k in Y_STEPS:
            p = y_peer(k)
            send(D1, D1, d1s.at[p], d1r.at[y * NC + 1], {"kv_1": p})
        drain(D1, d1s.at[pl.ds(0, NY - 1)])
        d1r[y * NC + 1] = d1s[y]
        arrive(CKV, ckv.at[pl.ds(0, NZ - 1)])
        sums = total(ckv, NZ)
        key_rows, value_rows = [], []
        for s in range(2):
            block = (sums[s * 4 : s * 4 + 4] * factors[s]).astype(BF16).astype(F32)
            for t in range(2):
                key_rows.append(jnp.broadcast_to(block[t : t + 1], (8, LANES)))
                value_rows.append(jnp.broadcast_to(block[2 + t : 3 + t], (8, LANES)))
        key_new = jnp.concatenate(key_rows, axis=0)
        value_new = jnp.concatenate(value_rows, axis=0)
        own_score = jnp.sum(queries * key_new, axis=1, keepdims=True) * HEAD**-0.5
        arrive(LAM, lams.at[0])
        arrive(WO, pob.at[pl.ds(0, 112)])
        arrive(W1, wts.at[1, :, pl.ds(WEIGHT_ROWS, WEIGHT_ROWS)])
        arrive(D1, d1r.at[pl.ds(0, NYC - 1)])

        both = [(s, t) for s in range(2) for t in range(2)]

        def stat(k, at):
            return jnp.concatenate(
                [d1r[k * NC + t, 16:24, s * HEAD + at : s * HEAD + at + 1] for s, t in both], axis=0
            )

        def gathered(k):
            return jnp.concatenate([d1r[k * NC + t, s * 8 : s * 8 + 8, :] for s, t in both], axis=0)

        tops = [stat(k, 0) for k in range(NY)]
        counts = [stat(k, HEAD // 2) for k in range(NY)]
        top = functools.reduce(jnp.maximum, tops)
        weights = [jnp.exp(t - top) for t in tops]
        count = functools.reduce(jnp.add, [w * s for w, s in zip(weights, counts)])
        values = functools.reduce(jnp.add, [weights[k] * gathered(k) for k in range(NY)])
        line = jnp.where(lane32 == row32, top, 0.0) + jnp.where(lane32 == row32 + HEAD, count, 0.0)
        d2m[z] = jnp.sum(line, axis=0, keepdims=True)
        to_z(D2M, lambda p: d2m.at[z], d2m)
        drain(D2M, d2m.at[pl.ds(0, NZ - 1)])
        d2o[z] = values.astype(BF16)
        to_z(D2O, lambda p: d2o.at[z], d2o)
        drain(D2O, d2o.at[pl.ds(0, NZ - 1)])
        arrive(D2M, d2m.at[pl.ds(0, NZ - 1)])
        tops = [jnp.sum(jnp.where(lane32 == row32, d2m[k], 0.0), axis=1, keepdims=True) for k in range(NZ)]
        counts = [jnp.sum(jnp.where(lane32 == row32 + HEAD, d2m[k], 0.0), axis=1, keepdims=True) for k in range(NZ)]
        top = functools.reduce(jnp.maximum, tops, own_score)
        weights = [jnp.exp(t - top) for t in tops]
        own_weight = jnp.exp(own_score - top)
        count = functools.reduce(jnp.add, [w * s for w, s in zip(weights, counts)], own_weight)
        arrive(D2O, d2o.at[pl.ds(0, NZ - 1)])
        values = own_weight * value_new
        for k in range(NZ):
            values = values + weights[k] * d2o[k].astype(F32)
        ratio = values / count
        lambdas = jnp.concatenate([lams[0], lams[1], lams[0], lams[1]], axis=0)
        mixed = ratio - lambdas * pltpu.roll(ratio, 31, 0)
        scale = lax.rsqrt(jnp.mean(mixed * mixed, axis=1, keepdims=True) + EPS)
        hs[...] = mixed * scale * hgain[...]
        d3s[...] = hs[pl.ds(0, 16, stride=2), :].astype(BF16)
        to_y(D3, d3s, d3.at[y])
        drain(D3, d3.at[pl.ds(0, NY - 1)])
        d3[y] = d3s[...]
        arrive(D3, d3.at[pl.ds(0, NY - 1)])

        for k in range(NY):
            ps[k * 16 : (k + 1) * 16, :] = d3[k].astype(F32)
        heads = jnp.concatenate([ps[pl.ds(h, 8, stride=8), :] for h in range(8)], axis=1).astype(BF16)
        projected = lax.dot_general(heads, pob[...], NT, preferred_element_type=F32)
        stream_two = (stream_one + projected).astype(BF16)
        f2[z] = stream_two
        fs[...] = stream_two
        to_z(F2, lambda p: f2.at[z], f2)
        drain(F2, f2.at[pl.ds(0, NZ - 1)])
        send(FS, FS, fs, fs, {"tp": 0})
        drain(FS, fs)
        arrive(F2, f2.at[pl.ds(0, NZ - 1)])
        rows = jnp.concatenate([f2[k].astype(F32) for k in range(NZ)], axis=1)

        mixed = mix_part(rows, gains[2:3, :], [wts[1, m] for m in range(3)])
        for k in range(NZ):
            g1s[k] = mixed[:, k * LANES : (k + 1) * LANES]
        to_z(G1, lambda p: g1s.at[p], g1r)
        drain(G1, g1s.at[pl.ds(0, NZ - 1)])
        g1r[z] = g1s[z]
        arrive(G1, g1r.at[pl.ds(0, NZ - 1)])
        g2[y] = total(g1r, NZ)
        for k in Y_STEPS:
            send(G2S, G2, g2.at[y], g2.at[y], {"kv_1": y_peer(k), "tp": 0})
            send(G2, G2, g2.at[y], g2.at[y], {"kv_1": y_peer(k)})
        send(G2S, G2, g2.at[y], g2.at[y], {"tp": 0})
        sent_all()

        @pl.loop(0, far_sends)
        def _(_):
            waits(A3, A3, a2.at[0]).wait_send()

        drain(G2S, g2)
        drain(G2, g2.at[pl.ds(0, NY - 1)])
        arrive(G2, g2.at[pl.ds(0, NY - 1)])
        finish(stream_two)


PHASES = 27
(
    A1, A2L, A2R, A3, B1, B2, CQ, C2, CKV, C3, C3S, D1, D2O, D2M, D3, F2, FS, G1, G2, G2S, LAM, W0, W1, WQ, WK, WV, WO,
) = range(27)


def local(
    residual, norm_gains, ffn_gate, ffn_up, ffn_down, proj_query, proj_key, proj_value, proj_out,
    head_lambda, head_gain, cache_keys, cache_values, live_length,
):
    batch = residual.shape[0]
    hidden = ffn_gate.shape[1]
    span = cache_keys.shape[1]
    vmem = pl.BlockSpec(memory_space=pltpu.VMEM)
    hbm = pl.BlockSpec(memory_space=pl.ANY)
    updated = pl.pallas_call(
        layer_kernel,
        out_shape=pltpu.VMEM(residual.shape, F32),
        in_specs=[hbm] * 14,
        out_specs=vmem,
        scratch_shapes=[
            pltpu.VMEM(residual.shape, BF16),
            pltpu.VMEM(norm_gains.shape, F32),
            pltpu.SMEM(head_lambda.shape, F32),
            pltpu.VMEM((1, VDIM), F32),
            pltpu.SMEM(live_length.shape, jnp.int32),
            pltpu.VMEM((3, hidden, 2, D), BF16),
            pltpu.VMEM((2, 3, WEIGHT_ROWS, D), BF16),
            pltpu.VMEM((2, 3, 2 * WEIGHT_ROWS, D), BF16),
            pltpu.VMEM((2, LANES, 512), BF16),
            pltpu.VMEM((2, LANES, 128), BF16),
            pltpu.VMEM((2, LANES, 128), BF16),
            pltpu.VMEM((LANES, 1024), BF16),
            pltpu.VMEM((2, 8, LANES), F32),
            pltpu.VMEM((batch, span, 128), BF16),
            pltpu.VMEM((batch, span, VDIM), BF16),
            pltpu.VMEM((NYC, 8, LANES), BF16),
            pltpu.VMEM((NZ, 8, LANES), BF16),
            pltpu.VMEM((NZ, 8, LANES), F32),
            pltpu.VMEM((NZ, 8, LANES), F32),
            pltpu.VMEM((NY, 8, LANES), F32),
            pltpu.VMEM((64, LANES), F32),
            pltpu.VMEM((32, LANES), F32),
            pltpu.VMEM((NZ, 1, LANES), F32),
            pltpu.VMEM((NZ, 16, LANES), F32),
            pltpu.VMEM((NZ, 8, LANES), F32),
            pltpu.VMEM((2, 16, LANES), BF16),
            pltpu.VMEM((NY, 16, LANES), BF16),
            pltpu.VMEM((NY, 24, LANES), F32),
            pltpu.VMEM((NYC, 24, LANES), F32),
            pltpu.VMEM((NZ, 32, LANES), BF16),
            pltpu.VMEM((NZ, 1, LANES), F32),
            pltpu.VMEM((32, LANES), F32),
            pltpu.VMEM((16, LANES), BF16),
            pltpu.VMEM((NY, 16, LANES), BF16),
            pltpu.VMEM((64, LANES), F32),
            pltpu.VMEM((NZ, 8, LANES), BF16),
            pltpu.VMEM((8, LANES), BF16),
            pltpu.VMEM((NZ, 8, LANES), F32),
            pltpu.VMEM((NZ, 8, LANES), F32),
            pltpu.VMEM((NY, 8, LANES), F32),
            pltpu.SemaphoreType.DMA((14,)),
            pltpu.SemaphoreType.DMA((PHASES,)),
            pltpu.SemaphoreType.DMA((PHASES,)),
        ],
        compiler_params=pltpu.CompilerParams(
            collective_id=0, has_side_effects=True,
        ),
    )(
        residual, norm_gains,
        jnp.swapaxes(ffn_gate, 0, 1), jnp.swapaxes(ffn_up, 0, 1), jnp.swapaxes(ffn_down, 0, 1),
        proj_query, proj_key, proj_value, proj_out.T,
        head_lambda, head_gain.reshape(1, VDIM),
        cache_keys.reshape(batch, span, 128), cache_values.reshape(batch, span, VDIM), live_length,
    )
    return updated.astype(BF16)


def solution(mesh):
    split = Mesh(
        mesh.devices.reshape(mesh.shape["dp"], NZ, NY, mesh.shape["tp"]),
        ("dp", "kv_0", "kv_1", "tp"),
    )
    return jax.shard_map(
        local,
        mesh=split,
        in_specs=(
            P("dp", KV_TP),
            P(),
            P(None, KV_TP, None),
            P(None, KV_TP, None),
            P(None, KV_TP, None),
            P(KV, "tp"),
            P(KV, "tp"),
            P(KV, "tp"),
            P("tp", KV),
            P("tp"),
            P(),
            P("dp", KV, "tp", None),
            P("dp", KV, "tp", None),
            P("dp"),
        ),
        out_specs=P("dp", KV_TP),
        check_vma=False,
    )
```

```python
import functools

import jax
import jax.numpy as jnp
from jax import lax
from jax.experimental import pallas as pl
from jax.experimental.pallas import tpu as pltpu
from jax.sharding import Mesh
from jax.sharding import PartitionSpec as P

D = 2048
HEAD = 64
VDIM = 128
NZ = 16
NY = 4
NC = 2
NYC = NY * NC
LANES = 128
KV_TP = ("kv_0", "kv_1", "tp")
KV = ("kv_0", "kv_1")
MESH = pl.DeviceIdType.MESH
F32 = jnp.float32
BF16 = jnp.bfloat16
EPS = 1e-05
NT = (((1,), (1,)), ((), ()))

Z_STEPS = (8, 7, 9, 6, 10, 5, 11, 4, 12, 3, 13, 2, 14, 1, 15)
Y_STEPS = (2, 1, 3)
WEIGHT_ROWS = 48


def iota(shape, dim):
    return lax.broadcasted_iota(jnp.int32, shape, dim)


def mix_part(rows, gain, weights):
    scale = lax.rsqrt(jnp.mean(rows * rows, axis=1, keepdims=True) + EPS)
    normed = (rows * scale * gain).astype(BF16)
    gate = lax.dot_general(normed, weights[0], NT, preferred_element_type=F32)
    up = lax.dot_general(normed, weights[1], NT, preferred_element_type=F32)
    hidden = (gate / (1.0 + jnp.exp(-gate)) * up).astype(BF16)
    return 0.5 * jnp.dot(hidden, weights[2], preferred_element_type=F32)


def layer_kernel(
    res_h, gains_h, gate_h, up_h, down_h, wq_h, wk_h, wv_h, po_h, lam_h, hgain_h, ck_h, cv_h, live_h,
    out,
    res, gains, lam, hgain, live,
    raw, stage, wts, wqb, wkb, wvb, pob, lams, kbuf, vbuf,
    a1, a2, b1s, b1r, b2, cs, ckvs, csq, c2, ckv, own, c3s, c3, d1s, d1r, d2o, d2m, hs, d3s, d3, ps, f2, fs, g1s, g1r, g2,
    hsem, ssem, rsem, hello,
):
    z = lax.axis_index("kv_0")
    y = lax.axis_index("kv_1")
    c = lax.axis_index("tp")
    hidden_rows = raw.shape[1]
    barrier = pltpu.get_barrier_semaphore()
    drains = []

    def z_peer(k):
        return lax.rem(z + k, NZ)

    def y_peer(k):
        return lax.rem(y + k, NY)

    def send(s, r, src, dst, device):
        pltpu.make_async_remote_copy(
            src_ref=src, dst_ref=dst, send_sem=ssem.at[s], recv_sem=rsem.at[r],
            device_id=device, device_id_type=MESH,
        ).start()

    def waits(s, r, ref):
        return pltpu.make_async_remote_copy(
            src_ref=ref, dst_ref=ref, send_sem=ssem.at[s], recv_sem=rsem.at[r],
            device_id={"kv_0": z}, device_id_type=MESH,
        )

    def arrive(r, ref):
        waits(r, r, ref).wait_recv()

    def drain(s, ref):
        drains.append(waits(s, s, ref))

    def signal(device):
        pl.semaphore_signal(barrier, inc=1, device_id=device, device_id_type=MESH)

    def to_z(phase, src_of, dst):
        for k in Z_STEPS:
            p = z_peer(k)
            send(phase, phase, src_of(p), dst.at[z], {"kv_0": p})

    def to_y(phase, src, dst):
        for k in Y_STEPS:
            send(phase, phase, src, dst, {"kv_1": y_peer(k)})

    def total(buf, count):
        acc = buf[0].astype(F32)
        for k in range(1, count):
            acc = acc + buf[k].astype(F32)
        return acc

    def load(k):
        if k < 3:
            return pltpu.make_async_copy((gate_h, up_h, down_h)[k], raw.at[k], hsem.at[k])
        src = (ck_h, cv_h, res_h, gains_h, lam_h, hgain_h, live_h)[k - 3]
        return pltpu.make_async_copy(src, (kbuf, vbuf, res, gains, lam, hgain, live)[k - 3], hsem.at[k])

    for k in (5, 7, 0, 1, 2, 6, 8, 9, 3, 4):
        load(k).start()

    def own_tile():
        spread = (iota((16, LANES), 1) == iota((16, LANES), 0) + (y * NC + c) * 16).astype(F32).astype(BF16)
        return jnp.dot(res[...], spread, preferred_element_type=F32).astype(BF16)

    lane = iota((8, LANES), 1)
    row = iota((8, LANES), 0)

    def own_lambdas():
        head = row // 2
        return jnp.where(head == 0, lam[0], jnp.where(head == 1, lam[1], jnp.where(head == 2, lam[2], lam[3])))

    def attend():
        span = kbuf.shape[1]
        position = (z * NY + y) * span + iota((8, span), 1)
        queries = jnp.concatenate([c3[k] for k in range(NY)], axis=0).astype(F32)
        scores = jnp.concatenate(
            [
                lax.dot_general(
                    queries[b * 8 : b * 8 + 8].astype(BF16), kbuf[b], NT, preferred_element_type=F32
                )
                for b in range(8)
            ],
            axis=0,
        ) * HEAD**-0.5
        alive = jnp.concatenate([(position < live[b]).astype(F32) for b in range(8)], axis=0) > 0.0
        highest = jnp.max(jnp.where(alive, scores, -1e30), axis=1, keepdims=True)
        terms = jnp.where(alive, jnp.exp(scores - highest), 0.0)
        weights = terms.astype(BF16)
        values = [jnp.dot(weights[b * 8 : b * 8 + 8], vbuf[b], preferred_element_type=F32) for b in range(8)]
        count = jnp.sum(terms, axis=1, keepdims=True)
        for k in range(NY):
            pairs = [
                jnp.where(
                    lax.rem(lane, HEAD) < HEAD // 2, highest[b * 8 : b * 8 + 8], count[b * 8 : b * 8 + 8]
                )
                for b in (2 * k, 2 * k + 1)
            ]
            d1s[k, 0:8, :] = values[2 * k]
            d1s[k, 8:16, :] = values[2 * k + 1]
            d1s[k, 16:24, :] = jnp.where(lane < HEAD, pairs[0], pairs[1])

    def sent_all():
        for each in drains:
            each.wait_send()
        drains.clear()

    def finish(stream_two):
        updated = stream_two.astype(F32) + total(g2, NY)
        sent_all()
        out[...] = pltpu.roll(updated, lax.rem(LANES - (y * NC + c) * 16, LANES), 1)[:, :16]

    @pl.when(c == 0)
    def _():
        core1 = {"tp": 1}

        def all_core1(s, r, src, dst):
            for k in Y_STEPS + (0,):
                send(s, r, src, dst, {"kv_1": y_peer(k), "tp": 1})

        load(5).wait()
        a1[y * NC] = own_tile()
        pl.semaphore_wait(barrier, NY)
        for k in Y_STEPS + (0,):
            pl.semaphore_signal(hello, inc=1, device_id={"kv_1": y_peer(k), "tp": 1}, device_id_type=MESH)

        all_core1(A1, A1, a1.at[y * NC], a1.at[y * NC])
        drain(A1, a1.at[pl.ds(0, NY)])
        load(7).wait()
        lams[0] = own_lambdas()
        send(LAM, LAM, lams.at[0], lams.at[0], core1)
        drain(LAM, lams.at[0])
        stage[:, :, 40:WEIGHT_ROWS, :] = jnp.zeros((2, 3, WEIGHT_ROWS - 40, D), BF16)
        for half in range(2):
            for m in range(3):
                if half == 0:
                    load(m).wait()
                stage[half, m, 0:hidden_rows, :] = raw.at[m][:, half, :]
            for m in range(3):
                send(W0 + half, W0 + half, stage.at[half, m], wts.at[half, m, pl.ds(WEIGHT_ROWS, WEIGHT_ROWS)], core1)
            drain(W0 + half, stage.at[half])
            if half == 0:
                part = pl.ds(pl.multiple_of(y * 32, 32), 32)
                all_core1(WQ, WQ, wq_h, wqb.at[0, part])
                all_core1(WK, WK, wk_h, wkb.at[0, part])
                all_core1(WV, WV, wv_h, wvb.at[0, part])
                drain(WQ, wqb.at[0])
                drain(WK, wkb.at[0])
                drain(WV, wvb.at[0])
        all_core1(WO, WO, po_h, pob.at[part, pl.ds(0, 512)])
        drain(WO, pob.at[:, pl.ds(0, 512)])

        for k in (3, 4, 6, 8, 9):
            load(k).wait()
        arrive(C3, c3)
        attend()
        for k in Y_STEPS + (0,):
            p = y_peer(k)
            send(D1, D1, d1s.at[p], d1r.at[y * NC], {"kv_1": p, "tp": 1})
        drain(D1, d1s)
        sent_all()
        arrive(FS, fs)
        arrive(G2, g2)
        finish(fs[...])

    @pl.when(c == 1)
    def _():
        for k in Y_STEPS + (0,):
            signal({"kv_1": y_peer(k), "tp": 0})
        for k in Z_STEPS:
            signal({"kv_0": z_peer(k)})
        part = pl.ds(pl.multiple_of(y * 32, 32), 32)
        pulls = [
            pltpu.make_async_copy(wq_h, wqb.at[1, part], hsem.at[10]),
            pltpu.make_async_copy(wk_h, wkb.at[1, part], hsem.at[11]),
            pltpu.make_async_copy(wv_h, wvb.at[1, part], hsem.at[12]),
            pltpu.make_async_copy(po_h, pob.at[part, pl.ds(512, 512)], hsem.at[13]),
        ]
        for pull in pulls:
            pull.start()
        load(5).wait()
        a1[y * NC + 1] = own_tile()

        def relayout(half):
            for m in range(3):
                wts[half, m, 0:hidden_rows, :] = raw.at[m][:, half, :]

        pl.semaphore_wait(hello, NY)

        to_y(A1, a1.at[y * NC + 1], a1.at[y * NC + 1])
        drain(A1, a1.at[pl.ds(0, NY - 1)])
        wts[:, :, 40:WEIGHT_ROWS, :] = jnp.zeros((2, 3, WEIGHT_ROWS - 40, D), BF16)
        for m in range(3):
            load(m).wait()
        relayout(0)
        arrive(A1, a1.at[pl.ds(0, NYC - 1)])
        res_z = total(a1, NYC)
        a2[z] = res_z.astype(BF16)
        pl.semaphore_wait(barrier, NZ - 1)
        to_z(A2, lambda p: a2.at[z], a2)
        drain(A2, a2.at[pl.ds(0, NZ - 1)])
        to_y(WQ, wq_h, wqb.at[1, part])
        to_y(WK, wk_h, wkb.at[1, part])
        to_y(WV, wv_h, wvb.at[1, part])
        to_y(WO, po_h, pob.at[part, pl.ds(512, 512)])
        drain(WQ, wqb.at[1, pl.ds(0, 96)])
        drain(WK, wkb.at[1, pl.ds(0, 96)])
        drain(WV, wvb.at[1, pl.ds(0, 96)])
        drain(WO, pob.at[pl.ds(0, 96), pl.ds(512, 512)])
        load(7).wait()
        lams[1] = own_lambdas()
        relayout(1)
        for k in (6, 8, 9):
            load(k).wait()
        for pull in pulls:
            pull.wait()
        arrive(W0, wts.at[0, :, pl.ds(WEIGHT_ROWS, WEIGHT_ROWS)])
        arrive(A2, a2.at[pl.ds(0, NZ - 1)])
        rows = jnp.concatenate([a2[k].astype(F32) for k in range(NZ)], axis=1)

        mixed = mix_part(rows, gains[0:1, :], [wts[0, m] for m in range(3)])
        for k in range(NZ):
            b1s[k] = mixed[:, k * LANES : (k + 1) * LANES]
        to_z(B1, lambda p: b1s.at[p], b1r)
        drain(B1, b1s.at[pl.ds(0, NZ - 1)])
        b1r[z] = b1s[z]
        arrive(B1, b1r.at[pl.ds(0, NZ - 1)])
        b2[y] = total(b1r, NZ)
        to_y(B2, b2.at[y], b2.at[y])
        drain(B2, b2.at[pl.ds(0, NY - 1)])
        arrive(WQ, wqb.at[:, pl.ds(0, 112)])
        arrive(WK, wkb.at[:, pl.ds(0, 112)])
        arrive(WV, wvb.at[:, pl.ds(0, 112)])
        arrive(B2, b2.at[pl.ds(0, NY - 1)])
        stream_one = (res_z + total(b2, NY)).astype(BF16).astype(F32)

        squares = jnp.sum(stream_one * stream_one, axis=1, keepdims=True)
        csq[z] = jnp.sum(jnp.where(lane == row, squares, 0.0), axis=0, keepdims=True)
        to_z(CQ, lambda p: csq.at[z], csq)
        drain(CQ, csq.at[pl.ds(0, NZ - 1)])
        gain_z = gains[1:2, pl.ds(pl.multiple_of(z * LANES, LANES), LANES)]
        scaled = (stream_one * gain_z).astype(BF16)
        for t in range(2):
            query = jnp.dot(scaled, wqb[t], preferred_element_type=F32)
            for g in range(4):
                cs[pl.ds(t * 4 + g, 8, stride=8), :] = query[:, g * LANES : (g + 1) * LANES]
        pair = pl.ds(pl.multiple_of(y * 16, 16), 16)
        to_z(C2, lambda p: cs.at[pair], c2)
        drain(C2, c2.at[pl.ds(0, NZ - 1)])
        c2[z] = cs[pair, :]
        for t in range(2):
            ckvs[pl.ds(t, 8, stride=4), :] = jnp.dot(scaled, wkb[t], preferred_element_type=F32)
            ckvs[pl.ds(2 + t, 8, stride=4), :] = jnp.dot(scaled, wvb[t], preferred_element_type=F32)
        pair_kv = pl.ds(pl.multiple_of(y * 8, 8), 8)
        owner = y * NY

        @pl.when(z != owner)
        def _():
            send(CKV, CKV, ckvs.at[pair_kv], ckv.at[z], {"kv_0": owner})

        arrive(CQ, csq.at[pl.ds(0, NZ - 1)])
        square_line = total(csq, NZ)
        arrive(C2, c2.at[pl.ds(0, NZ - 1)])
        sums = total(c2, NZ)
        query_rows, factors = [], []
        lane1 = iota((1, LANES), 1)
        for s in range(2):
            square = jnp.sum(jnp.where(lane1 == 2 * y + s, square_line, 0.0), axis=1, keepdims=True)
            factors.append(lax.rsqrt(square / D + EPS))
            block = (sums[s * 8 : (s + 1) * 8] * factors[s]).astype(BF16).astype(F32)
            for h in range(8):
                query_rows += [block[h : h + 1], block[h : h + 1]]
        row32 = iota((32, LANES), 0)
        lane32 = iota((32, LANES), 1)
        component = lax.rem(row32, 2)
        queries = jnp.where((lane32 >= HEAD) == (component == 1), jnp.concatenate(query_rows, axis=0), 0.0)
        for t in range(2):
            c3s[t] = jnp.concatenate(
                [queries[t * 8 : t * 8 + 8], queries[16 + t * 8 : 24 + t * 8]], axis=0
            ).astype(BF16)
        for k in Y_STEPS:
            send(C3S, C3, c3s.at[0], c3.at[y], {"kv_1": y_peer(k), "tp": 0})
            send(C3, C3, c3s.at[1], c3.at[y], {"kv_1": y_peer(k)})
        send(C3S, C3, c3s.at[0], c3.at[y], {"tp": 0})
        drain(C3S, c3)
        drain(C3, c3.at[pl.ds(0, NY - 1)])
        c3[y] = c3s[1]
        load(3).wait()
        load(4).wait()
        arrive(C3, c3.at[pl.ds(0, NY - 1)])
        attend()
        for k in Y_STEPS:
            p = y_peer(k)
            send(D1, D1, d1s.at[p], d1r.at[y * NC + 1], {"kv_1": p})
        drain(D1, d1s.at[pl.ds(0, NY - 1)])
        d1r[y * NC + 1] = d1s[y]

        @pl.when(z == owner)
        def _():
            ckv[z] = ckvs[pair_kv, :]
            arrive(CKV, ckv.at[pl.ds(0, NZ - 1)])
            sums = total(ckv, NZ)
            key_rows, value_rows = [], []
            for s in range(2):
                block = (sums[s * 4 : s * 4 + 4] * factors[s]).astype(BF16).astype(F32)
                for t in range(2):
                    key_rows.append(jnp.broadcast_to(block[t : t + 1], (8, LANES)))
                    value_rows.append(jnp.broadcast_to(block[2 + t : 3 + t], (8, LANES)))
            products = queries * jnp.concatenate(key_rows, axis=0)
            own[0] = jnp.broadcast_to(jnp.sum(products, axis=1, keepdims=True) * HEAD**-0.5, (32, LANES))
            own[1] = jnp.concatenate(value_rows, axis=0)

        @pl.when(z != owner)
        def _():
            own[0] = jnp.full((32, LANES), -1e30, F32)
            own[1] = jnp.zeros((32, LANES), F32)

        arrive(LAM, lams.at[0])
        arrive(WO, pob.at[pl.ds(0, 112)])
        arrive(W1, wts.at[1, :, pl.ds(WEIGHT_ROWS, WEIGHT_ROWS)])
        arrive(D1, d1r.at[pl.ds(0, NYC - 1)])

        both = [(s, t) for s in range(2) for t in range(2)]

        def stat(k, at):
            return jnp.concatenate(
                [d1r[k * NC + t, 16:24, s * HEAD + at : s * HEAD + at + 1] for s, t in both], axis=0
            )

        def gathered(k):
            return jnp.concatenate([d1r[k * NC + t, s * 8 : s * 8 + 8, :] for s, t in both], axis=0)

        tops = [stat(k, 0) for k in range(NY)]
        counts = [stat(k, HEAD // 2) for k in range(NY)]
        own_score = own[0, :, 0:1]
        top = functools.reduce(jnp.maximum, tops, own_score)
        weights = [jnp.exp(t - top) for t in tops]
        own_weight = jnp.exp(own_score - top)
        own_count = own_weight * (z == owner).astype(F32)
        count = functools.reduce(jnp.add, [w * s for w, s in zip(weights, counts)], own_count)
        values = functools.reduce(jnp.add, [weights[k] * gathered(k) for k in range(NY)], own_weight * own[1])
        line = jnp.where(lane32 == row32, top, 0.0) + jnp.where(lane32 == row32 + HEAD, count, 0.0)
        d2m[z] = jnp.sum(line, axis=0, keepdims=True)
        to_z(D2M, lambda p: d2m.at[z], d2m)
        drain(D2M, d2m.at[pl.ds(0, NZ - 1)])
        d2o[z] = values.astype(BF16)
        to_z(D2O, lambda p: d2o.at[z], d2o)
        drain(D2O, d2o.at[pl.ds(0, NZ - 1)])
        arrive(D2M, d2m.at[pl.ds(0, NZ - 1)])
        tops = [jnp.sum(jnp.where(lane32 == row32, d2m[k], 0.0), axis=1, keepdims=True) for k in range(NZ)]
        counts = [jnp.sum(jnp.where(lane32 == row32 + HEAD, d2m[k], 0.0), axis=1, keepdims=True) for k in range(NZ)]
        top = functools.reduce(jnp.maximum, tops)
        weights = [jnp.exp(t - top) for t in tops]
        count = functools.reduce(jnp.add, [w * s for w, s in zip(weights, counts)])
        arrive(D2O, d2o.at[pl.ds(0, NZ - 1)])
        values = functools.reduce(jnp.add, [weights[k] * d2o[k].astype(F32) for k in range(NZ)])
        ratio = values / count
        lambdas = jnp.concatenate([lams[0], lams[1], lams[0], lams[1]], axis=0)
        mixed = ratio - lambdas * pltpu.roll(ratio, 31, 0)
        scale = lax.rsqrt(jnp.mean(mixed * mixed, axis=1, keepdims=True) + EPS)
        hs[...] = mixed * scale * hgain[...]
        d3s[...] = hs[pl.ds(0, 16, stride=2), :].astype(BF16)
        to_y(D3, d3s, d3.at[y])
        drain(D3, d3.at[pl.ds(0, NY - 1)])
        d3[y] = d3s[...]
        arrive(D3, d3.at[pl.ds(0, NY - 1)])

        for k in range(NY):
            ps[k * 16 : (k + 1) * 16, :] = d3[k].astype(F32)
        heads = jnp.concatenate([ps[pl.ds(h, 8, stride=8), :] for h in range(8)], axis=1).astype(BF16)
        projected = lax.dot_general(heads, pob[...], NT, preferred_element_type=F32)
        stream_two = (stream_one + projected).astype(BF16)
        f2[z] = stream_two
        fs[...] = stream_two
        to_z(F2, lambda p: f2.at[z], f2)
        drain(F2, f2.at[pl.ds(0, NZ - 1)])
        send(FS, FS, fs, fs, {"tp": 0})
        drain(FS, fs)
        arrive(F2, f2.at[pl.ds(0, NZ - 1)])
        rows = jnp.concatenate([f2[k].astype(F32) for k in range(NZ)], axis=1)

        mixed = mix_part(rows, gains[2:3, :], [wts[1, m] for m in range(3)])
        for k in range(NZ):
            g1s[k] = mixed[:, k * LANES : (k + 1) * LANES]
        to_z(G1, lambda p: g1s.at[p], g1r)
        drain(G1, g1s.at[pl.ds(0, NZ - 1)])
        g1r[z] = g1s[z]
        arrive(G1, g1r.at[pl.ds(0, NZ - 1)])
        g2[y] = total(g1r, NZ)
        for k in Y_STEPS:
            send(G2S, G2, g2.at[y], g2.at[y], {"kv_1": y_peer(k), "tp": 0})
            send(G2, G2, g2.at[y], g2.at[y], {"kv_1": y_peer(k)})
        send(G2S, G2, g2.at[y], g2.at[y], {"tp": 0})
        sent_all()

        @pl.when(z != owner)
        def _():
            waits(CKV, CKV, ckv.at[0]).wait_send()

        drain(G2S, g2)
        drain(G2, g2.at[pl.ds(0, NY - 1)])
        arrive(G2, g2.at[pl.ds(0, NY - 1)])
        finish(stream_two)


PHASES = 25
(
    A1, A2, B1, B2, CQ, C2, CKV, C3, C3S, D1, D2O, D2M, D3, F2, FS, G1, G2, G2S, LAM, W0, W1, WQ, WK, WV, WO,
) = range(25)


def local(
    residual, norm_gains, ffn_gate, ffn_up, ffn_down, proj_query, proj_key, proj_value, proj_out,
    head_lambda, head_gain, cache_keys, cache_values, live_length,
):
    batch = residual.shape[0]
    hidden = ffn_gate.shape[1]
    span = cache_keys.shape[1]
    vmem = pl.BlockSpec(memory_space=pltpu.VMEM)
    hbm = pl.BlockSpec(memory_space=pl.ANY)
    updated = pl.pallas_call(
        layer_kernel,
        out_shape=pltpu.VMEM(residual.shape, F32),
        in_specs=[hbm] * 14,
        out_specs=vmem,
        scratch_shapes=[
            pltpu.VMEM(residual.shape, BF16),
            pltpu.VMEM(norm_gains.shape, F32),
            pltpu.SMEM(head_lambda.shape, F32),
            pltpu.VMEM((1, VDIM), F32),
            pltpu.SMEM(live_length.shape, jnp.int32),
            pltpu.VMEM((3, hidden, 2, D), BF16),
            pltpu.VMEM((2, 3, WEIGHT_ROWS, D), BF16),
            pltpu.VMEM((2, 3, 2 * WEIGHT_ROWS, D), BF16),
            pltpu.VMEM((2, LANES, 512), BF16),
            pltpu.VMEM((2, LANES, 128), BF16),
            pltpu.VMEM((2, LANES, 128), BF16),
            pltpu.VMEM((LANES, 1024), BF16),
            pltpu.VMEM((2, 8, LANES), F32),
            pltpu.VMEM((batch, span, 128), BF16),
            pltpu.VMEM((batch, span, VDIM), BF16),
            pltpu.VMEM((NYC, 8, LANES), BF16),
            pltpu.VMEM((NZ, 8, LANES), BF16),
            pltpu.VMEM((NZ, 8, LANES), F32),
            pltpu.VMEM((NZ, 8, LANES), F32),
            pltpu.VMEM((NY, 8, LANES), F32),
            pltpu.VMEM((64, LANES), F32),
            pltpu.VMEM((32, LANES), F32),
            pltpu.VMEM((NZ, 1, LANES), F32),
            pltpu.VMEM((NZ, 16, LANES), F32),
            pltpu.VMEM((NZ, 8, LANES), F32),
            pltpu.VMEM((2, 32, LANES), F32),
            pltpu.VMEM((2, 16, LANES), BF16),
            pltpu.VMEM((NY, 16, LANES), BF16),
            pltpu.VMEM((NY, 24, LANES), F32),
            pltpu.VMEM((NYC, 24, LANES), F32),
            pltpu.VMEM((NZ, 32, LANES), BF16),
            pltpu.VMEM((NZ, 1, LANES), F32),
            pltpu.VMEM((32, LANES), F32),
            pltpu.VMEM((16, LANES), BF16),
            pltpu.VMEM((NY, 16, LANES), BF16),
            pltpu.VMEM((64, LANES), F32),
            pltpu.VMEM((NZ, 8, LANES), BF16),
            pltpu.VMEM((8, LANES), BF16),
            pltpu.VMEM((NZ, 8, LANES), F32),
            pltpu.VMEM((NZ, 8, LANES), F32),
            pltpu.VMEM((NY, 8, LANES), F32),
            pltpu.SemaphoreType.DMA((14,)),
            pltpu.SemaphoreType.DMA((PHASES,)),
            pltpu.SemaphoreType.DMA((PHASES,)),
            pltpu.SemaphoreType.REGULAR,
        ],
        compiler_params=pltpu.CompilerParams(
            collective_id=0, has_side_effects=True,
        ),
    )(
        residual, norm_gains,
        jnp.swapaxes(ffn_gate, 0, 1), jnp.swapaxes(ffn_up, 0, 1), jnp.swapaxes(ffn_down, 0, 1),
        proj_query, proj_key, proj_value, proj_out.T,
        head_lambda, head_gain.reshape(1, VDIM),
        cache_keys.reshape(batch, span, 128), cache_values.reshape(batch, span, VDIM), live_length,
    )
    return updated.astype(BF16)


def solution(mesh):
    split = Mesh(
        mesh.devices.reshape(mesh.shape["dp"], NZ, NY, mesh.shape["tp"]),
        ("dp", "kv_0", "kv_1", "tp"),
    )
    return jax.shard_map(
        local,
        mesh=split,
        in_specs=(
            P("dp", KV_TP),
            P(),
            P(None, KV_TP, None),
            P(None, KV_TP, None),
            P(None, KV_TP, None),
            P(KV, "tp"),
            P(KV, "tp"),
            P(KV, "tp"),
            P("tp", KV),
            P("tp"),
            P(),
            P("dp", KV, "tp", None),
            P("dp", KV, "tp", None),
            P("dp"),
        ),
        out_specs=P("dp", KV_TP),
        check_vma=False,
    )
```

```python
import functools

import jax
import jax.numpy as jnp
from jax import lax
from jax.experimental import pallas as pl
from jax.experimental.pallas import tpu as pltpu
from jax.sharding import Mesh
from jax.sharding import PartitionSpec as P

D = 2048
HEAD = 64
VDIM = 128
NZ = 16
NY = 4
NC = 2
NYC = NY * NC
LANES = 128
KV_TP = ("kv_0", "kv_1", "tp")
KV = ("kv_0", "kv_1")
MESH = pl.DeviceIdType.MESH
F32 = jnp.float32
BF16 = jnp.bfloat16
EPS = 1e-05
NT = (((1,), (1,)), ((), ()))

Z_STEPS = (8, 7, 9, 6, 10, 5, 11, 4, 12, 3, 13, 2, 14, 1, 15)
Y_STEPS = (2, 1, 3)
WEIGHT_ROWS = 48


def iota(shape, dim):
    return lax.broadcasted_iota(jnp.int32, shape, dim)


def mix_part(rows, gain, weights):
    scale = lax.rsqrt(jnp.mean(rows * rows, axis=1, keepdims=True) + EPS)
    normed = (rows * scale * gain).astype(BF16)
    gate = lax.dot_general(normed, weights[0], NT, preferred_element_type=F32)
    up = lax.dot_general(normed, weights[1], NT, preferred_element_type=F32)
    hidden = (gate / (1.0 + jnp.exp(-gate)) * up).astype(BF16)
    return 0.5 * jnp.dot(hidden, weights[2], preferred_element_type=F32)


def layer_kernel(
    res_h, gains_h, gate_h, up_h, down_h, wq_h, wk_h, wv_h, po_h, lam_h, hgain_h, ck_h, cv_h, live_h,
    out,
    res, gains, lam, hgain, live,
    raw, stage, wts, wqb, wkb, wvb, pob, lams, kbuf, vbuf,
    a1, a2, b1s, b1r, b2, cs, ckvs, csq, c2, ckv, own, c3s, c3, d1s, d1r, d2o, d2m, hs, d3s, d3, ps, f2, fs, g1s, g1r, g2,
    hsem, ssem, rsem, hello,
):
    z = lax.axis_index("kv_0")
    y = lax.axis_index("kv_1")
    c = lax.axis_index("tp")
    hidden_rows = raw.shape[1]
    barrier = pltpu.get_barrier_semaphore()
    drains = []

    def z_peer(k):
        return lax.rem(z + k, NZ)

    def y_peer(k):
        return lax.rem(y + k, NY)

    def send(s, r, src, dst, device):
        pltpu.make_async_remote_copy(
            src_ref=src, dst_ref=dst, send_sem=ssem.at[s], recv_sem=rsem.at[r],
            device_id=device, device_id_type=MESH,
        ).start()

    def waits(s, r, ref):
        return pltpu.make_async_remote_copy(
            src_ref=ref, dst_ref=ref, send_sem=ssem.at[s], recv_sem=rsem.at[r],
            device_id={"kv_0": z}, device_id_type=MESH,
        )

    def arrive(r, ref):
        waits(r, r, ref).wait_recv()

    def drain(s, ref):
        drains.append(waits(s, s, ref))

    def signal(device):
        pl.semaphore_signal(barrier, inc=1, device_id=device, device_id_type=MESH)

    def to_z(phase, src_of, dst):
        for k in Z_STEPS:
            p = z_peer(k)
            send(phase, phase, src_of(p), dst.at[z], {"kv_0": p})

    def to_y(phase, src, dst):
        for k in Y_STEPS:
            send(phase, phase, src, dst, {"kv_1": y_peer(k)})

    def total(buf, count):
        acc = buf[0].astype(F32)
        for k in range(1, count):
            acc = acc + buf[k].astype(F32)
        return acc

    def load(k):
        if k < 3:
            return pltpu.make_async_copy((gate_h, up_h, down_h)[k], raw.at[k], hsem.at[k])
        src = (ck_h, cv_h, res_h, gains_h, lam_h, hgain_h, live_h)[k - 3]
        return pltpu.make_async_copy(src, (kbuf, vbuf, res, gains, lam, hgain, live)[k - 3], hsem.at[k])

    def start_loads():
        for k in (5, 0, 1, 2, 7, 6, 8, 9, 3, 4):
            load(k).start()

    def own_tile():
        spread = (iota((16, LANES), 1) == iota((16, LANES), 0) + (y * NC + c) * 16).astype(F32).astype(BF16)
        return jnp.dot(res[...], spread, preferred_element_type=F32).astype(BF16)

    lane = iota((8, LANES), 1)
    row = iota((8, LANES), 0)

    def own_lambdas():
        head = row // 2
        return jnp.where(head == 0, lam[0], jnp.where(head == 1, lam[1], jnp.where(head == 2, lam[2], lam[3])))

    def attend():
        span = kbuf.shape[1]
        position = (z * NY + y) * span + iota((8, span), 1)
        queries = jnp.concatenate([c3[k] for k in range(NY)], axis=0).astype(F32)
        scores = jnp.concatenate(
            [
                lax.dot_general(
                    queries[b * 8 : b * 8 + 8].astype(BF16), kbuf[b], NT, preferred_element_type=F32
                )
                for b in range(8)
            ],
            axis=0,
        ) * HEAD**-0.5
        alive = jnp.concatenate([(position < live[b]).astype(F32) for b in range(8)], axis=0) > 0.0
        highest = jnp.max(jnp.where(alive, scores, -1e30), axis=1, keepdims=True)
        terms = jnp.where(alive, jnp.exp(scores - highest), 0.0)
        weights = terms.astype(BF16)
        values = [jnp.dot(weights[b * 8 : b * 8 + 8], vbuf[b], preferred_element_type=F32) for b in range(8)]
        count = jnp.sum(terms, axis=1, keepdims=True)
        for k in range(NY):
            pairs = [
                jnp.where(
                    lax.rem(lane, HEAD) < HEAD // 2, highest[b * 8 : b * 8 + 8], count[b * 8 : b * 8 + 8]
                )
                for b in (2 * k, 2 * k + 1)
            ]
            d1s[k, 0:8, :] = values[2 * k]
            d1s[k, 8:16, :] = values[2 * k + 1]
            d1s[k, 16:24, :] = jnp.where(lane < HEAD, pairs[0], pairs[1])

    def sent_all():
        for each in drains:
            each.wait_send()
        drains.clear()

    def finish(stream_two):
        updated = stream_two.astype(F32) + total(g2, NY)
        sent_all()
        out[...] = pltpu.roll(updated, lax.rem(LANES - (y * NC + c) * 16, LANES), 1)[:, :16]

    @pl.when(c == 0)
    def _():
        core1 = {"tp": 1}

        def all_core1(s, r, src, dst):
            for k in Y_STEPS + (0,):
                send(s, r, src, dst, {"kv_1": y_peer(k), "tp": 1})

        start_loads()
        load(5).wait()
        a1[y * NC] = own_tile()
        pl.semaphore_wait(barrier, NY)
        pl.semaphore_signal(hello, inc=1, device_id=core1, device_id_type=MESH)

        all_core1(A1, A1, a1.at[y * NC], a1.at[y * NC])
        drain(A1, a1.at[pl.ds(0, NY)])
        load(7).wait()
        lams[0] = own_lambdas()
        send(LAM, LAM, lams.at[0], lams.at[0], core1)
        drain(LAM, lams.at[0])
        stage[:, :, 40:WEIGHT_ROWS, :] = jnp.zeros((2, 3, WEIGHT_ROWS - 40, D), BF16)
        for half in range(2):
            for m in range(3):
                if half == 0:
                    load(m).wait()
                stage[half, m, 0:hidden_rows, :] = raw.at[m][:, half, :]
            for m in range(3):
                send(W0 + half, W0 + half, stage.at[half, m], wts.at[half, m, pl.ds(WEIGHT_ROWS, WEIGHT_ROWS)], core1)
            drain(W0 + half, stage.at[half])
            if half == 0:
                part = pl.ds(pl.multiple_of(y * 32, 32), 32)
                all_core1(WQ, WQ, wq_h, wqb.at[0, part])
                all_core1(WK, WK, wk_h, wkb.at[0, part])
                all_core1(WV, WV, wv_h, wvb.at[0, part])
                drain(WQ, wqb.at[0])
                drain(WK, wkb.at[0])
                drain(WV, wvb.at[0])
        all_core1(WO, WO, po_h, pob.at[part, pl.ds(0, 512)])
        drain(WO, pob.at[:, pl.ds(0, 512)])

        for k in (3, 4, 6, 8, 9):
            load(k).wait()
        arrive(C3, c3)
        attend()
        for k in Y_STEPS + (0,):
            p = y_peer(k)
            send(D1, D1, d1s.at[p], d1r.at[y * NC], {"kv_1": p, "tp": 1})
        drain(D1, d1s)
        sent_all()
        arrive(FS, fs)
        arrive(G2, g2)
        finish(fs[...])

    @pl.when(c == 1)
    def _():
        for k in Z_STEPS:
            signal({"kv_0": z_peer(k)})
        for k in Y_STEPS + (0,):
            signal({"kv_1": y_peer(k), "tp": 0})
        start_loads()
        part = pl.ds(pl.multiple_of(y * 32, 32), 32)
        pulls = [
            pltpu.make_async_copy(wq_h, wqb.at[1, part], hsem.at[10]),
            pltpu.make_async_copy(wk_h, wkb.at[1, part], hsem.at[11]),
            pltpu.make_async_copy(wv_h, wvb.at[1, part], hsem.at[12]),
            pltpu.make_async_copy(po_h, pob.at[part, pl.ds(512, 512)], hsem.at[13]),
        ]
        for pull in pulls:
            pull.start()
        load(5).wait()
        a1[y * NC + 1] = own_tile()

        def relayout(half):
            for m in range(3):
                wts[half, m, 0:hidden_rows, :] = raw.at[m][:, half, :]

        pl.semaphore_wait(hello, 1)

        to_y(A1, a1.at[y * NC + 1], a1.at[y * NC + 1])
        drain(A1, a1.at[pl.ds(0, NY - 1)])
        wts[:, :, 40:WEIGHT_ROWS, :] = jnp.zeros((2, 3, WEIGHT_ROWS - 40, D), BF16)
        for m in range(3):
            load(m).wait()
        relayout(0)
        arrive(A1, a1.at[pl.ds(0, NYC - 1)])
        res_z = total(a1, NYC)
        a2[z] = res_z.astype(BF16)
        pl.semaphore_wait(barrier, NZ - 1)
        to_z(A2, lambda p: a2.at[z], a2)
        drain(A2, a2.at[pl.ds(0, NZ - 1)])
        to_y(WQ, wq_h, wqb.at[1, part])
        to_y(WK, wk_h, wkb.at[1, part])
        to_y(WV, wv_h, wvb.at[1, part])
        to_y(WO, po_h, pob.at[part, pl.ds(512, 512)])
        drain(WQ, wqb.at[1, pl.ds(0, 96)])
        drain(WK, wkb.at[1, pl.ds(0, 96)])
        drain(WV, wvb.at[1, pl.ds(0, 96)])
        drain(WO, pob.at[pl.ds(0, 96), pl.ds(512, 512)])
        load(7).wait()
        lams[1] = own_lambdas()
        relayout(1)
        for k in (6, 8, 9):
            load(k).wait()
        for pull in pulls:
            pull.wait()
        arrive(W0, wts.at[0, :, pl.ds(WEIGHT_ROWS, WEIGHT_ROWS)])
        arrive(A2, a2.at[pl.ds(0, NZ - 1)])
        rows = jnp.concatenate([a2[k].astype(F32) for k in range(NZ)], axis=1)

        mixed = mix_part(rows, gains[0:1, :], [wts[0, m] for m in range(3)])
        for k in range(NZ):
            b1s[k] = mixed[:, k * LANES : (k + 1) * LANES]
        to_z(B1, lambda p: b1s.at[p], b1r)
        drain(B1, b1s.at[pl.ds(0, NZ - 1)])
        b1r[z] = b1s[z]
        arrive(B1, b1r.at[pl.ds(0, NZ - 1)])
        b2[y] = total(b1r, NZ)
        to_y(B2, b2.at[y], b2.at[y])
        drain(B2, b2.at[pl.ds(0, NY - 1)])
        arrive(WQ, wqb.at[:, pl.ds(0, 112)])
        arrive(WK, wkb.at[:, pl.ds(0, 112)])
        arrive(WV, wvb.at[:, pl.ds(0, 112)])
        arrive(B2, b2.at[pl.ds(0, NY - 1)])
        stream_one = (res_z + total(b2, NY)).astype(BF16).astype(F32)

        gain_z = gains[1:2, pl.ds(pl.multiple_of(z * LANES, LANES), LANES)]
        scaled = (stream_one * gain_z).astype(BF16)
        query = [jnp.dot(scaled, wqb[t], preferred_element_type=F32) for t in range(2)]
        squares = jnp.sum(stream_one * stream_one, axis=1, keepdims=True)
        csq[z] = jnp.sum(jnp.where(lane == row, squares, 0.0), axis=0, keepdims=True)
        for t in range(2):
            for g in range(4):
                cs[pl.ds(t * 4 + g, 8, stride=8), :] = query[t][:, g * LANES : (g + 1) * LANES]
        pair = pl.ds(pl.multiple_of(y * 16, 16), 16)
        for k in Z_STEPS:
            p = z_peer(k)
            send(CQ, CQ, csq.at[z], csq.at[z], {"kv_0": p})
            send(C2, C2, cs.at[pair], c2.at[z], {"kv_0": p})
        drain(CQ, csq.at[pl.ds(0, NZ - 1)])
        drain(C2, c2.at[pl.ds(0, NZ - 1)])
        c2[z] = cs[pair, :]
        for t in range(2):
            ckvs[pl.ds(t, 8, stride=4), :] = jnp.dot(scaled, wkb[t], preferred_element_type=F32)
            ckvs[pl.ds(2 + t, 8, stride=4), :] = jnp.dot(scaled, wvb[t], preferred_element_type=F32)
        pair_kv = pl.ds(pl.multiple_of(y * 8, 8), 8)
        owner = y * NY

        @pl.when(z != owner)
        def _():
            send(CKV, CKV, ckvs.at[pair_kv], ckv.at[z], {"kv_0": owner})

        arrive(CQ, csq.at[pl.ds(0, NZ - 1)])
        square_line = total(csq, NZ)
        arrive(C2, c2.at[pl.ds(0, NZ - 1)])
        sums = total(c2, NZ)
        query_rows, factors = [], []
        lane1 = iota((1, LANES), 1)
        for s in range(2):
            square = jnp.sum(jnp.where(lane1 == 2 * y + s, square_line, 0.0), axis=1, keepdims=True)
            factors.append(lax.rsqrt(square / D + EPS))
            block = (sums[s * 8 : (s + 1) * 8] * factors[s]).astype(BF16).astype(F32)
            for h in range(8):
                query_rows += [block[h : h + 1], block[h : h + 1]]
        row32 = iota((32, LANES), 0)
        lane32 = iota((32, LANES), 1)
        component = lax.rem(row32, 2)
        queries = jnp.where((lane32 >= HEAD) == (component == 1), jnp.concatenate(query_rows, axis=0), 0.0)
        for t in range(2):
            c3s[t] = jnp.concatenate(
                [queries[t * 8 : t * 8 + 8], queries[16 + t * 8 : 24 + t * 8]], axis=0
            ).astype(BF16)
        for k in Y_STEPS:
            send(C3S, C3, c3s.at[0], c3.at[y], {"kv_1": y_peer(k), "tp": 0})
            send(C3, C3, c3s.at[1], c3.at[y], {"kv_1": y_peer(k)})
        send(C3S, C3, c3s.at[0], c3.at[y], {"tp": 0})
        drain(C3S, c3)
        drain(C3, c3.at[pl.ds(0, NY - 1)])
        c3[y] = c3s[1]
        load(3).wait()
        load(4).wait()
        arrive(C3, c3.at[pl.ds(0, NY - 1)])
        attend()
        for k in Y_STEPS:
            p = y_peer(k)
            send(D1, D1, d1s.at[p], d1r.at[y * NC + 1], {"kv_1": p})
        drain(D1, d1s.at[pl.ds(0, NY - 1)])
        d1r[y * NC + 1] = d1s[y]

        @pl.when(z == owner)
        def _():
            ckv[z] = ckvs[pair_kv, :]
            arrive(CKV, ckv.at[pl.ds(0, NZ - 1)])
            sums = total(ckv, NZ)
            key_rows, value_rows = [], []
            for s in range(2):
                block = (sums[s * 4 : s * 4 + 4] * factors[s]).astype(BF16).astype(F32)
                for t in range(2):
                    key_rows.append(jnp.broadcast_to(block[t : t + 1], (8, LANES)))
                    value_rows.append(jnp.broadcast_to(block[2 + t : 3 + t], (8, LANES)))
            products = queries * jnp.concatenate(key_rows, axis=0)
            scores = jnp.sum(products, axis=1, keepdims=True) * HEAD**-0.5
            for t in range(2):
                pair = jnp.where(lane < HEAD, scores[t * 8 : t * 8 + 8], scores[16 + t * 8 : 24 + t * 8])
                own[t] = jnp.where(lax.rem(lane, HEAD) < HEAD // 2, pair, 1.0)
            for k in range(4):
                own[2 + k] = value_rows[k]

        @pl.when(z != owner)
        def _():
            for t in range(2):
                own[t] = jnp.where(lax.rem(lane, HEAD) < HEAD // 2, -1e30, 0.0)
            for k in range(4):
                own[2 + k] = jnp.zeros((8, LANES), F32)

        arrive(LAM, lams.at[0])
        arrive(WO, pob.at[pl.ds(0, 112)])
        arrive(W1, wts.at[1, :, pl.ds(WEIGHT_ROWS, WEIGHT_ROWS)])
        arrive(D1, d1r.at[pl.ds(0, NYC - 1)])

        is_top = lax.rem(lane, HEAD) < HEAD // 2
        joined, line = [[], []], jnp.zeros((1, LANES), F32)
        for t in range(2):
            stats = [d1r[k * NC + t, 16:24, :] for k in range(NY)] + [own[t]]
            blocks = [[d1r[k * NC + t, s * 8 : s * 8 + 8, :] for s in range(2)] for k in range(NY)]
            blocks += [[own[2 + t], own[4 + t]]]
            top = functools.reduce(jnp.maximum, stats)
            weights = [jnp.where(is_top, jnp.exp(jnp.where(is_top, each - top, 0.0)), 0.0) for each in stats]
            count = functools.reduce(
                jnp.add, [pltpu.roll(w, HEAD // 2, 1) * each for w, each in zip(weights, stats)]
            )
            packed = jnp.where(is_top, top, count)
            line += jnp.sum(jnp.where(lax.rem(lane, HEAD // 2) == row + t * 8, packed, 0.0), axis=0, keepdims=True)
            for s in range(2):
                joined[s].append(
                    functools.reduce(
                        jnp.add, [w[:, s * HEAD : s * HEAD + 1] * each[s] for w, each in zip(weights, blocks)]
                    )
                )
        d2m[z] = line
        d2o[z] = jnp.concatenate(joined[0] + joined[1], axis=0).astype(BF16)
        for k in Z_STEPS:
            p = z_peer(k)
            send(D2M, D2M, d2m.at[z], d2m.at[z], {"kv_0": p})
            send(D2O, D2O, d2o.at[z], d2o.at[z], {"kv_0": p})
        drain(D2M, d2m.at[pl.ds(0, NZ - 1)])
        drain(D2O, d2o.at[pl.ds(0, NZ - 1)])
        arrive(D2M, d2m.at[pl.ds(0, NZ - 1)])
        spot = row32 // 16 * HEAD + lax.rem(row32, 16)
        tops = [jnp.sum(jnp.where(lane32 == spot, d2m[k], 0.0), axis=1, keepdims=True) for k in range(NZ)]
        counts = [
            jnp.sum(jnp.where(lane32 == spot + HEAD // 2, d2m[k], 0.0), axis=1, keepdims=True) for k in range(NZ)
        ]
        top = functools.reduce(jnp.maximum, tops)
        weights = [jnp.exp(t - top) for t in tops]
        count = functools.reduce(jnp.add, [w * s for w, s in zip(weights, counts)])
        arrive(D2O, d2o.at[pl.ds(0, NZ - 1)])
        values = functools.reduce(jnp.add, [weights[k] * d2o[k].astype(F32) for k in range(NZ)])
        ratio = values / count
        lambdas = jnp.concatenate([lams[0], lams[1], lams[0], lams[1]], axis=0)
        mixed = ratio - lambdas * pltpu.roll(ratio, 31, 0)
        scale = lax.rsqrt(jnp.mean(mixed * mixed, axis=1, keepdims=True) + EPS)
        hs[...] = mixed * scale * hgain[...]
        d3s[...] = hs[pl.ds(0, 16, stride=2), :].astype(BF16)
        to_y(D3, d3s, d3.at[y])
        drain(D3, d3.at[pl.ds(0, NY - 1)])
        d3[y] = d3s[...]
        arrive(D3, d3.at[pl.ds(0, NY - 1)])

        for k in range(NY):
            ps[k * 16 : (k + 1) * 16, :] = d3[k].astype(F32)
        heads = jnp.concatenate([ps[pl.ds(h, 8, stride=8), :] for h in range(8)], axis=1).astype(BF16)
        projected = lax.dot_general(heads, pob[...], NT, preferred_element_type=F32)
        stream_two = (stream_one + projected).astype(BF16)
        f2[z] = stream_two
        fs[...] = stream_two
        to_z(F2, lambda p: f2.at[z], f2)
        drain(F2, f2.at[pl.ds(0, NZ - 1)])
        send(FS, FS, fs, fs, {"tp": 0})
        drain(FS, fs)
        arrive(F2, f2.at[pl.ds(0, NZ - 1)])
        rows = jnp.concatenate([f2[k].astype(F32) for k in range(NZ)], axis=1)

        mixed = mix_part(rows, gains[2:3, :], [wts[1, m] for m in range(3)])
        for k in range(NZ):
            g1s[k] = mixed[:, k * LANES : (k + 1) * LANES]
        to_z(G1, lambda p: g1s.at[p], g1r)
        drain(G1, g1s.at[pl.ds(0, NZ - 1)])
        g1r[z] = g1s[z]
        arrive(G1, g1r.at[pl.ds(0, NZ - 1)])
        g2[y] = total(g1r, NZ)
        for k in Y_STEPS:
            send(G2S, G2, g2.at[y], g2.at[y], {"kv_1": y_peer(k), "tp": 0})
            send(G2, G2, g2.at[y], g2.at[y], {"kv_1": y_peer(k)})
        send(G2S, G2, g2.at[y], g2.at[y], {"tp": 0})
        sent_all()

        @pl.when(z != owner)
        def _():
            waits(CKV, CKV, ckv.at[0]).wait_send()

        drain(G2S, g2)
        drain(G2, g2.at[pl.ds(0, NY - 1)])
        arrive(G2, g2.at[pl.ds(0, NY - 1)])
        finish(stream_two)


PHASES = 25
(
    A1, A2, B1, B2, CQ, C2, CKV, C3, C3S, D1, D2O, D2M, D3, F2, FS, G1, G2, G2S, LAM, W0, W1, WQ, WK, WV, WO,
) = range(25)


def local(
    residual, norm_gains, ffn_gate, ffn_up, ffn_down, proj_query, proj_key, proj_value, proj_out,
    head_lambda, head_gain, cache_keys, cache_values, live_length,
):
    batch = residual.shape[0]
    hidden = ffn_gate.shape[1]
    span = cache_keys.shape[1]
    vmem = pl.BlockSpec(memory_space=pltpu.VMEM)
    hbm = pl.BlockSpec(memory_space=pl.ANY)
    updated = pl.pallas_call(
        layer_kernel,
        out_shape=pltpu.VMEM(residual.shape, F32),
        in_specs=[hbm] * 14,
        out_specs=vmem,
        scratch_shapes=[
            pltpu.VMEM(residual.shape, BF16),
            pltpu.VMEM(norm_gains.shape, F32),
            pltpu.SMEM(head_lambda.shape, F32),
            pltpu.VMEM((1, VDIM), F32),
            pltpu.SMEM(live_length.shape, jnp.int32),
            pltpu.VMEM((3, hidden, 2, D), BF16),
            pltpu.VMEM((2, 3, WEIGHT_ROWS, D), BF16),
            pltpu.VMEM((2, 3, 2 * WEIGHT_ROWS, D), BF16),
            pltpu.VMEM((2, LANES, 512), BF16),
            pltpu.VMEM((2, LANES, 128), BF16),
            pltpu.VMEM((2, LANES, 128), BF16),
            pltpu.VMEM((LANES, 1024), BF16),
            pltpu.VMEM((2, 8, LANES), F32),
            pltpu.VMEM((batch, span, 128), BF16),
            pltpu.VMEM((batch, span, VDIM), BF16),
            pltpu.VMEM((NYC, 8, LANES), BF16),
            pltpu.VMEM((NZ, 8, LANES), BF16),
            pltpu.VMEM((NZ, 8, LANES), F32),
            pltpu.VMEM((NZ, 8, LANES), F32),
            pltpu.VMEM((NY, 8, LANES), F32),
            pltpu.VMEM((64, LANES), F32),
            pltpu.VMEM((32, LANES), F32),
            pltpu.VMEM((NZ, 1, LANES), F32),
            pltpu.VMEM((NZ, 16, LANES), F32),
            pltpu.VMEM((NZ, 8, LANES), F32),
            pltpu.VMEM((6, 8, LANES), F32),
            pltpu.VMEM((2, 16, LANES), BF16),
            pltpu.VMEM((NY, 16, LANES), BF16),
            pltpu.VMEM((NY, 24, LANES), F32),
            pltpu.VMEM((NYC, 24, LANES), F32),
            pltpu.VMEM((NZ, 32, LANES), BF16),
            pltpu.VMEM((NZ, 1, LANES), F32),
            pltpu.VMEM((32, LANES), F32),
            pltpu.VMEM((16, LANES), BF16),
            pltpu.VMEM((NY, 16, LANES), BF16),
            pltpu.VMEM((64, LANES), F32),
            pltpu.VMEM((NZ, 8, LANES), BF16),
            pltpu.VMEM((8, LANES), BF16),
            pltpu.VMEM((NZ, 8, LANES), F32),
            pltpu.VMEM((NZ, 8, LANES), F32),
            pltpu.VMEM((NY, 8, LANES), F32),
            pltpu.SemaphoreType.DMA((14,)),
            pltpu.SemaphoreType.DMA((PHASES,)),
            pltpu.SemaphoreType.DMA((PHASES,)),
            pltpu.SemaphoreType.REGULAR,
        ],
        compiler_params=pltpu.CompilerParams(
            collective_id=0, has_side_effects=True,
        ),
    )(
        residual, norm_gains,
        jnp.swapaxes(ffn_gate, 0, 1), jnp.swapaxes(ffn_up, 0, 1), jnp.swapaxes(ffn_down, 0, 1),
        proj_query, proj_key, proj_value, proj_out.T,
        head_lambda, head_gain.reshape(1, VDIM),
        cache_keys.reshape(batch, span, 128), cache_values.reshape(batch, span, VDIM), live_length,
    )
    return updated.astype(BF16)


def solution(mesh):
    split = Mesh(
        mesh.devices.reshape(mesh.shape["dp"], NZ, NY, mesh.shape["tp"]),
        ("dp", "kv_0", "kv_1", "tp"),
    )
    return jax.shard_map(
        local,
        mesh=split,
        in_specs=(
            P("dp", KV_TP),
            P(),
            P(None, KV_TP, None),
            P(None, KV_TP, None),
            P(None, KV_TP, None),
            P(KV, "tp"),
            P(KV, "tp"),
            P(KV, "tp"),
            P("tp", KV),
            P("tp"),
            P(),
            P("dp", KV, "tp", None),
            P("dp", KV, "tp", None),
            P("dp"),
        ),
        out_specs=P("dp", KV_TP),
        check_vma=False,
    )
```

```python
import functools

import jax
import jax.numpy as jnp
from jax import lax
from jax.experimental import pallas as pl
from jax.experimental.pallas import tpu as pltpu
from jax.sharding import Mesh
from jax.sharding import PartitionSpec as P

D = 2048
HEAD = 64
VDIM = 128
NZ = 16
NY = 4
NC = 2
NYC = NY * NC
LANES = 128
KV_TP = ("kv_0", "kv_1", "tp")
KV = ("kv_0", "kv_1")
MESH = pl.DeviceIdType.MESH
F32 = jnp.float32
BF16 = jnp.bfloat16
EPS = 1e-05
NT = (((1,), (1,)), ((), ()))

Z_STEPS = (8, 7, 9, 6, 10, 5, 11, 4, 12, 3, 13, 2, 14, 1, 15)
Y_STEPS = (2, 1, 3)
WEIGHT_ROWS = 48


def iota(shape, dim):
    return lax.broadcasted_iota(jnp.int32, shape, dim)


def mix_part(rows, gain, weights):
    scale = lax.rsqrt(jnp.mean(rows * rows, axis=1, keepdims=True) + EPS)
    normed = (rows * scale * gain).astype(BF16)
    gate = lax.dot_general(normed, weights[0], NT, preferred_element_type=F32)
    up = lax.dot_general(normed, weights[1], NT, preferred_element_type=F32)
    hidden = (gate / (1.0 + jnp.exp(-gate)) * up).astype(BF16)
    return 0.5 * jnp.dot(hidden, weights[2], preferred_element_type=F32)


def layer_kernel(
    res_h, gains_h, gate_h, up_h, down_h, wq_h, wk_h, wv_h, po_h, lam_h, hgain_h, ck_h, cv_h, live_h,
    out,
    res, gains, lam, hgain, live,
    raw, stage, wts, wqb, wkb, wvb, pob, lams, kbuf, vbuf,
    a1, a2, b1s, b1r, b2, cs, ckvs, csq, c2, ckv, own, c3s, c3, d1s, d1r, d2o, d2m, hs, d3s, d3, ps, f2, fs, g1s, g1r, g2,
    hsem, ssem, rsem, hello,
):
    z = lax.axis_index("kv_0")
    y = lax.axis_index("kv_1")
    c = lax.axis_index("tp")
    hidden_rows = raw.shape[1]
    barrier = pltpu.get_barrier_semaphore()
    drains = []

    def z_peer(k):
        return lax.rem(z + k, NZ)

    def y_peer(k):
        return lax.rem(y + k, NY)

    def send(s, r, src, dst, device):
        pltpu.make_async_remote_copy(
            src_ref=src, dst_ref=dst, send_sem=ssem.at[s], recv_sem=rsem.at[r],
            device_id=device, device_id_type=MESH,
        ).start()

    def waits(s, r, ref):
        return pltpu.make_async_remote_copy(
            src_ref=ref, dst_ref=ref, send_sem=ssem.at[s], recv_sem=rsem.at[r],
            device_id={"kv_0": z}, device_id_type=MESH,
        )

    def arrive(r, ref):
        waits(r, r, ref).wait_recv()

    def drain(s, ref):
        drains.append(waits(s, s, ref))

    def signal(device):
        pl.semaphore_signal(barrier, inc=1, device_id=device, device_id_type=MESH)

    def to_z(phase, src_of, dst):
        for k in Z_STEPS:
            p = z_peer(k)
            send(phase, phase, src_of(p), dst.at[z], {"kv_0": p})

    def to_y(phase, src, dst):
        for k in Y_STEPS:
            send(phase, phase, src, dst, {"kv_1": y_peer(k)})

    def total(buf, count):
        acc = buf[0].astype(F32)
        for k in range(1, count):
            acc = acc + buf[k].astype(F32)
        return acc

    def load(k):
        if k < 3:
            return pltpu.make_async_copy((gate_h, up_h, down_h)[k], raw.at[k], hsem.at[k])
        src = (ck_h, cv_h, res_h, gains_h, lam_h, hgain_h, live_h)[k - 3]
        if k < 5:
            src = src.at[pl.ds(2 * y, 2)]
        return pltpu.make_async_copy(src, (kbuf.at[y], vbuf.at[y], res, gains, lam, hgain, live)[k - 3], hsem.at[k])

    def start_loads():
        for k in (5, 0, 1, 2, 7, 6, 8, 9, 3, 4):
            load(k).start()

    def own_tile():
        spread = (iota((16, LANES), 1) == iota((16, LANES), 0) + (y * NC + c) * 16).astype(F32).astype(BF16)
        return jnp.dot(res[...], spread, preferred_element_type=F32).astype(BF16)

    lane = iota((8, LANES), 1)
    row = iota((8, LANES), 0)

    def own_lambdas():
        head = row // 2
        return jnp.where(head == 0, lam[0], jnp.where(head == 1, lam[1], jnp.where(head == 2, lam[2], lam[3])))

    def attend(tile):
        span = kbuf.shape[2]
        queries = tile.astype(F32)
        queries = [queries[t * 8 : t * 8 + 8].astype(BF16) for t in range(2)]
        scores = jnp.concatenate(
            [
                lax.dot_general(queries[b % 2], kbuf[b // 2, b % 2], NT, preferred_element_type=F32)
                for b in range(8)
            ],
            axis=0,
        ) * HEAD**-0.5
        place = z * NY * span + iota((8, span), 1)
        length = [live[2 * y], live[2 * y + 1]]
        alive = jnp.concatenate(
            [(place + (b // 2) * span < length[b % 2]).astype(F32) for b in range(8)], axis=0
        ) > 0.0
        highest = jnp.max(jnp.where(alive, scores, -1e30), axis=1, keepdims=True)
        terms = jnp.where(alive, jnp.exp(scores - highest), 0.0)
        weights = terms.astype(BF16)
        values = [jnp.dot(weights[b * 8 : b * 8 + 8], vbuf[b // 2, b % 2], preferred_element_type=F32) for b in range(8)]
        count = jnp.sum(terms, axis=1, keepdims=True)
        for k in range(NY):
            pairs = [
                jnp.where(
                    lax.rem(lane, HEAD) < HEAD // 2, highest[b * 8 : b * 8 + 8], count[b * 8 : b * 8 + 8]
                )
                for b in (2 * k, 2 * k + 1)
            ]
            d1s[k, 0:8, :] = values[2 * k]
            d1s[k, 8:16, :] = values[2 * k + 1]
            d1s[k, 16:24, :] = jnp.where(lane < HEAD, pairs[0], pairs[1])

    def give(phase, cache, buf):
        for k in Y_STEPS:
            p = y_peer(k)
            send(phase, phase, cache.at[pl.ds(2 * p, 2)], buf.at[y], {"kv_1": p})
        drain(phase, buf.at[pl.ds(0, NY - 1)])

    def sent_all():
        for each in drains:
            each.wait_send()
        drains.clear()

    def finish(stream_two):
        updated = stream_two.astype(F32) + total(g2, NY)
        sent_all()
        out[...] = pltpu.roll(updated, lax.rem(LANES - (y * NC + c) * 16, LANES), 1)[:, :16]

    @pl.when(c == 0)
    def _():
        core1 = {"tp": 1}

        def all_core1(s, r, src, dst):
            for k in Y_STEPS + (0,):
                send(s, r, src, dst, {"kv_1": y_peer(k), "tp": 1})

        for k in Y_STEPS:
            signal({"kv_1": y_peer(k)})
        start_loads()
        load(5).wait()
        a1[y * NC] = own_tile()
        pl.semaphore_wait(barrier, NY + NY - 1)
        pl.semaphore_signal(hello, inc=1, device_id=core1, device_id_type=MESH)

        all_core1(A1, A1, a1.at[y * NC], a1.at[y * NC])
        drain(A1, a1.at[pl.ds(0, NY)])
        load(7).wait()
        lams[0] = own_lambdas()
        send(LAM, LAM, lams.at[0], lams.at[0], core1)
        drain(LAM, lams.at[0])
        stage[:, :, 40:WEIGHT_ROWS, :] = jnp.zeros((2, 3, WEIGHT_ROWS - 40, D), BF16)
        part = pl.ds(pl.multiple_of(y * 32, 32), 32)
        all_core1(WQ, WQ, wq_h, wqb.at[0, part])
        all_core1(WK, WK, wk_h, wkb.at[0, part])
        all_core1(WV, WV, wv_h, wvb.at[0, part])
        drain(WQ, wqb.at[0])
        drain(WK, wkb.at[0])
        drain(WV, wvb.at[0])
        for m in range(3):
            load(m).wait()

        @pl.loop(0, 3)
        def _(m):
            for half in range(2):
                stage[half, m, 0:hidden_rows, :] = raw.at[m][:, half, :]
                send(W0 + half, W0 + half, stage.at[half, m], wts.at[half, m, pl.ds(WEIGHT_ROWS, WEIGHT_ROWS)], core1)

        drain(W0, stage.at[0])
        drain(W1, stage.at[1])
        all_core1(WO, WO, po_h, pob.at[part, pl.ds(0, 512)])
        drain(WO, pob.at[:, pl.ds(0, 512)])
        give(KX, ck_h, kbuf)
        give(VX, cv_h, vbuf)

        for k in (3, 4, 6, 8, 9):
            load(k).wait()
        arrive(KX, kbuf.at[pl.ds(0, NY - 1)])
        arrive(VX, vbuf.at[pl.ds(0, NY - 1)])
        arrive(C3, c3)
        attend(c3[...])
        send(D1, D1, d1s, d1r, core1)
        drain(D1, d1s)
        sent_all()
        arrive(FS, fs)
        arrive(G2, g2)
        finish(fs[...])

    @pl.when(c == 1)
    def _():
        for k in Z_STEPS:
            signal({"kv_0": z_peer(k)})
        for k in Y_STEPS + (0,):
            signal({"kv_1": y_peer(k), "tp": 0})
        start_loads()
        part = pl.ds(pl.multiple_of(y * 32, 32), 32)
        pulls = [
            pltpu.make_async_copy(wq_h, wqb.at[1, part], hsem.at[10]),
            pltpu.make_async_copy(wk_h, wkb.at[1, part], hsem.at[11]),
            pltpu.make_async_copy(wv_h, wvb.at[1, part], hsem.at[12]),
            pltpu.make_async_copy(po_h, pob.at[part, pl.ds(512, 512)], hsem.at[13]),
        ]
        for pull in pulls:
            pull.start()
        load(5).wait()
        a1[y * NC + 1] = own_tile()

        pl.semaphore_wait(hello, 1)

        to_y(A1, a1.at[y * NC + 1], a1.at[y * NC + 1])
        drain(A1, a1.at[pl.ds(0, NY - 1)])
        arrive(A1, a1.at[pl.ds(0, NYC - 1)])
        res_z = total(a1, NYC)
        a2[z] = res_z.astype(BF16)
        pl.semaphore_wait(barrier, NZ - 1)
        to_z(A2, lambda p: a2.at[z], a2)
        drain(A2, a2.at[pl.ds(0, NZ - 1)])
        to_y(WQ, wq_h, wqb.at[1, part])
        to_y(WK, wk_h, wkb.at[1, part])
        to_y(WV, wv_h, wvb.at[1, part])
        to_y(WO, po_h, pob.at[part, pl.ds(512, 512)])
        drain(WQ, wqb.at[1, pl.ds(0, 96)])
        drain(WK, wkb.at[1, pl.ds(0, 96)])
        drain(WV, wvb.at[1, pl.ds(0, 96)])
        drain(WO, pob.at[pl.ds(0, 96), pl.ds(512, 512)])
        give(KX, ck_h, kbuf)
        load(7).wait()
        lams[1] = own_lambdas()
        wts[:, :, 40:WEIGHT_ROWS, :] = jnp.zeros((2, 3, WEIGHT_ROWS - 40, D), BF16)
        for m in range(3):
            load(m).wait()

        @pl.loop(0, 3)
        def _(m):
            for half in range(2):
                wts[half, m, 0:hidden_rows, :] = raw.at[m][:, half, :]

        for k in (6, 8, 9):
            load(k).wait()
        for pull in pulls:
            pull.wait()
        arrive(W0, wts.at[0, :, pl.ds(WEIGHT_ROWS, WEIGHT_ROWS)])
        arrive(A2, a2.at[pl.ds(0, NZ - 1)])
        rows = jnp.concatenate([a2[k].astype(F32) for k in range(NZ)], axis=1)

        mixed = mix_part(rows, gains[0:1, :], [wts[0, m] for m in range(3)])
        for k in range(NZ):
            b1s[k] = mixed[:, k * LANES : (k + 1) * LANES]
        to_z(B1, lambda p: b1s.at[p], b1r)
        drain(B1, b1s.at[pl.ds(0, NZ - 1)])
        b1r[z] = b1s[z]
        arrive(B1, b1r.at[pl.ds(0, NZ - 1)])
        b2[y] = total(b1r, NZ)
        to_y(B2, b2.at[y], b2.at[y])
        drain(B2, b2.at[pl.ds(0, NY - 1)])
        give(VX, cv_h, vbuf)
        arrive(WQ, wqb.at[:, pl.ds(0, 112)])
        arrive(WK, wkb.at[:, pl.ds(0, 112)])
        arrive(WV, wvb.at[:, pl.ds(0, 112)])
        arrive(B2, b2.at[pl.ds(0, NY - 1)])
        stream_one = (res_z + total(b2, NY)).astype(BF16).astype(F32)

        gain_z = gains[1:2, pl.ds(pl.multiple_of(z * LANES, LANES), LANES)]
        scaled = (stream_one * gain_z).astype(BF16)
        query = [jnp.dot(scaled, wqb[t], preferred_element_type=F32) for t in range(2)]
        squares = jnp.sum(stream_one * stream_one, axis=1, keepdims=True)
        csq[z] = jnp.sum(jnp.where(lane == row, squares, 0.0), axis=0, keepdims=True)
        to_z(CQ, lambda p: csq.at[z], csq)
        for t in range(2):
            for g in range(4):
                cs[pl.ds(t * 4 + g, 8, stride=8), :] = query[t][:, g * LANES : (g + 1) * LANES]
        pair = pl.ds(pl.multiple_of(y * 16, 16), 16)
        to_z(C2, lambda p: cs.at[pair], c2)
        drain(CQ, csq.at[pl.ds(0, NZ - 1)])
        drain(C2, c2.at[pl.ds(0, NZ - 1)])
        c2[z] = cs[pair, :]
        for t in range(2):
            ckvs[pl.ds(t, 8, stride=4), :] = jnp.dot(scaled, wkb[t], preferred_element_type=F32)
            ckvs[pl.ds(2 + t, 8, stride=4), :] = jnp.dot(scaled, wvb[t], preferred_element_type=F32)
        pair_kv = pl.ds(pl.multiple_of(y * 8, 8), 8)
        owner = y * NY

        @pl.when(z != owner)
        def _():
            send(CKV, CKV, ckvs.at[pair_kv], ckv.at[z], {"kv_0": owner})

        arrive(CQ, csq.at[pl.ds(0, NZ - 1)])
        square_line = total(csq, NZ)
        arrive(C2, c2.at[pl.ds(0, NZ - 1)])
        sums = total(c2, NZ)
        query_rows, factors = [], []
        lane1 = iota((1, LANES), 1)
        for s in range(2):
            square = jnp.sum(jnp.where(lane1 == 2 * y + s, square_line, 0.0), axis=1, keepdims=True)
            factors.append(lax.rsqrt(square / D + EPS))
            block = (sums[s * 8 : (s + 1) * 8] * factors[s]).astype(BF16).astype(F32)
            for h in range(8):
                query_rows += [block[h : h + 1], block[h : h + 1]]
        row32 = iota((32, LANES), 0)
        lane32 = iota((32, LANES), 1)
        component = lax.rem(row32, 2)
        queries = jnp.where((lane32 >= HEAD) == (component == 1), jnp.concatenate(query_rows, axis=0), 0.0)
        for t in range(2):
            c3s[t] = jnp.concatenate(
                [queries[t * 8 : t * 8 + 8], queries[16 + t * 8 : 24 + t * 8]], axis=0
            ).astype(BF16)
        send(C3, C3, c3s.at[0], c3, {"tp": 0})
        drain(C3, c3)
        load(3).wait()
        load(4).wait()
        arrive(KX, kbuf.at[pl.ds(0, NY - 1)])
        arrive(VX, vbuf.at[pl.ds(0, NY - 1)])
        attend(c3s[1])

        @pl.when(z == owner)
        def _():
            ckv[z] = ckvs[pair_kv, :]
            arrive(CKV, ckv.at[pl.ds(0, NZ - 1)])
            sums = total(ckv, NZ)
            key_rows, value_rows = [], []
            for s in range(2):
                block = (sums[s * 4 : s * 4 + 4] * factors[s]).astype(BF16).astype(F32)
                for t in range(2):
                    key_rows.append(jnp.broadcast_to(block[t : t + 1], (8, LANES)))
                    value_rows.append(jnp.broadcast_to(block[2 + t : 3 + t], (8, LANES)))
            products = queries * jnp.concatenate(key_rows, axis=0)
            scores = jnp.sum(products, axis=1, keepdims=True) * HEAD**-0.5
            for t in range(2):
                pair = jnp.where(lane < HEAD, scores[t * 8 : t * 8 + 8], scores[16 + t * 8 : 24 + t * 8])
                own[t] = jnp.where(lax.rem(lane, HEAD) < HEAD // 2, pair, 1.0)
            for k in range(4):
                own[2 + k] = value_rows[k]

        @pl.when(z != owner)
        def _():
            for t in range(2):
                own[t] = jnp.where(lax.rem(lane, HEAD) < HEAD // 2, -1e30, 0.0)
            for k in range(4):
                own[2 + k] = jnp.zeros((8, LANES), F32)

        arrive(LAM, lams.at[0])
        arrive(WO, pob.at[pl.ds(0, 112)])
        arrive(W1, wts.at[1, :, pl.ds(WEIGHT_ROWS, WEIGHT_ROWS)])
        arrive(D1, d1r)

        is_top = lax.rem(lane, HEAD) < HEAD // 2
        joined, line = [[], []], jnp.zeros((1, LANES), F32)
        for t in range(2):
            part = (d1r, d1s)[t]
            stats = [part[k, 16:24, :] for k in range(NY)] + [own[t]]
            blocks = [[part[k, s * 8 : s * 8 + 8, :] for s in range(2)] for k in range(NY)]
            blocks += [[own[2 + t], own[4 + t]]]
            top = functools.reduce(jnp.maximum, stats)
            weights = [jnp.where(is_top, jnp.exp(jnp.where(is_top, each - top, 0.0)), 0.0) for each in stats]
            count = functools.reduce(
                jnp.add, [pltpu.roll(w, HEAD // 2, 1) * each for w, each in zip(weights, stats)]
            )
            packed = jnp.where(is_top, top, count)
            line += jnp.sum(jnp.where(lax.rem(lane, HEAD // 2) == row + t * 8, packed, 0.0), axis=0, keepdims=True)
            for s in range(2):
                joined[s].append(
                    functools.reduce(
                        jnp.add, [w[:, s * HEAD : s * HEAD + 1] * each[s] for w, each in zip(weights, blocks)]
                    )
                )
        d2m[z] = line
        d2o[z] = jnp.concatenate(joined[0] + joined[1], axis=0).astype(BF16)
        to_z(D2M, lambda p: d2m.at[z], d2m)
        to_z(D2O, lambda p: d2o.at[z], d2o)
        drain(D2M, d2m.at[pl.ds(0, NZ - 1)])
        drain(D2O, d2o.at[pl.ds(0, NZ - 1)])
        arrive(D2M, d2m.at[pl.ds(0, NZ - 1)])
        spot = row32 // 16 * HEAD + lax.rem(row32, 16)
        tops = [jnp.sum(jnp.where(lane32 == spot, d2m[k], 0.0), axis=1, keepdims=True) for k in range(NZ)]
        counts = [
            jnp.sum(jnp.where(lane32 == spot + HEAD // 2, d2m[k], 0.0), axis=1, keepdims=True) for k in range(NZ)
        ]
        top = functools.reduce(jnp.maximum, tops)
        weights = [jnp.exp(t - top) for t in tops]
        count = functools.reduce(jnp.add, [w * s for w, s in zip(weights, counts)])
        arrive(D2O, d2o.at[pl.ds(0, NZ - 1)])
        values = functools.reduce(jnp.add, [weights[k] * d2o[k].astype(F32) for k in range(NZ)])
        ratio = values / count
        lambdas = jnp.concatenate([lams[0], lams[1], lams[0], lams[1]], axis=0)
        mixed = ratio - lambdas * pltpu.roll(ratio, 31, 0)
        scale = lax.rsqrt(jnp.mean(mixed * mixed, axis=1, keepdims=True) + EPS)
        hs[...] = mixed * scale * hgain[...]
        d3s[...] = hs[pl.ds(0, 16, stride=2), :].astype(BF16)
        to_y(D3, d3s, d3.at[y])
        drain(D3, d3.at[pl.ds(0, NY - 1)])
        d3[y] = d3s[...]
        arrive(D3, d3.at[pl.ds(0, NY - 1)])

        for k in range(NY):
            ps[k * 16 : (k + 1) * 16, :] = d3[k].astype(F32)
        heads = jnp.concatenate([ps[pl.ds(h, 8, stride=8), :] for h in range(8)], axis=1).astype(BF16)
        projected = lax.dot_general(heads, pob[...], NT, preferred_element_type=F32)
        stream_two = (stream_one + projected).astype(BF16)
        f2[z] = stream_two
        fs[...] = stream_two
        to_z(F2, lambda p: f2.at[z], f2)
        drain(F2, f2.at[pl.ds(0, NZ - 1)])
        send(FS, FS, fs, fs, {"tp": 0})
        drain(FS, fs)
        arrive(F2, f2.at[pl.ds(0, NZ - 1)])
        rows = jnp.concatenate([f2[k].astype(F32) for k in range(NZ)], axis=1)

        mixed = mix_part(rows, gains[2:3, :], [wts[1, m] for m in range(3)])
        for k in range(NZ):
            g1s[k] = mixed[:, k * LANES : (k + 1) * LANES]
        to_z(G1, lambda p: g1s.at[p], g1r)
        drain(G1, g1s.at[pl.ds(0, NZ - 1)])
        g1r[z] = g1s[z]
        arrive(G1, g1r.at[pl.ds(0, NZ - 1)])
        g2[y] = total(g1r, NZ)
        for k in Y_STEPS:
            send(G2S, G2, g2.at[y], g2.at[y], {"kv_1": y_peer(k), "tp": 0})
            send(G2, G2, g2.at[y], g2.at[y], {"kv_1": y_peer(k)})
        send(G2S, G2, g2.at[y], g2.at[y], {"tp": 0})
        sent_all()

        @pl.when(z != owner)
        def _():
            waits(CKV, CKV, ckv.at[0]).wait_send()

        drain(G2S, g2)
        drain(G2, g2.at[pl.ds(0, NY - 1)])
        arrive(G2, g2.at[pl.ds(0, NY - 1)])
        finish(stream_two)


PHASES = 26
(
    A1, A2, B1, B2, CQ, C2, CKV, C3, D1, D2O, D2M, D3, F2, FS, G1, G2, G2S, LAM, W0, W1, WQ, WK, WV, WO, KX, VX,
) = range(26)


def local(
    residual, norm_gains, ffn_gate, ffn_up, ffn_down, proj_query, proj_key, proj_value, proj_out,
    head_lambda, head_gain, cache_keys, cache_values, live_length,
):
    batch = residual.shape[0]
    hidden = ffn_gate.shape[1]
    span = cache_keys.shape[1]
    vmem = pl.BlockSpec(memory_space=pltpu.VMEM)
    hbm = pl.BlockSpec(memory_space=pl.ANY)
    updated = pl.pallas_call(
        layer_kernel,
        out_shape=pltpu.VMEM(residual.shape, F32),
        in_specs=[hbm] * 14,
        out_specs=vmem,
        scratch_shapes=[
            pltpu.VMEM(residual.shape, BF16),
            pltpu.VMEM(norm_gains.shape, F32),
            pltpu.SMEM(head_lambda.shape, F32),
            pltpu.VMEM((1, VDIM), F32),
            pltpu.SMEM(live_length.shape, jnp.int32),
            pltpu.VMEM((3, hidden, 2, D), BF16),
            pltpu.VMEM((2, 3, WEIGHT_ROWS, D), BF16),
            pltpu.VMEM((2, 3, 2 * WEIGHT_ROWS, D), BF16),
            pltpu.VMEM((2, LANES, 512), BF16),
            pltpu.VMEM((2, LANES, 128), BF16),
            pltpu.VMEM((2, LANES, 128), BF16),
            pltpu.VMEM((LANES, 1024), BF16),
            pltpu.VMEM((2, 8, LANES), F32),
            pltpu.VMEM((NY, batch // NY, span, 128), BF16),
            pltpu.VMEM((NY, batch // NY, span, VDIM), BF16),
            pltpu.VMEM((NYC, 8, LANES), BF16),
            pltpu.VMEM((NZ, 8, LANES), BF16),
            pltpu.VMEM((NZ, 8, LANES), F32),
            pltpu.VMEM((NZ, 8, LANES), F32),
            pltpu.VMEM((NY, 8, LANES), F32),
            pltpu.VMEM((64, LANES), F32),
            pltpu.VMEM((32, LANES), F32),
            pltpu.VMEM((NZ, 1, LANES), F32),
            pltpu.VMEM((NZ, 16, LANES), F32),
            pltpu.VMEM((NZ, 8, LANES), F32),
            pltpu.VMEM((6, 8, LANES), F32),
            pltpu.VMEM((2, 16, LANES), BF16),
            pltpu.VMEM((16, LANES), BF16),
            pltpu.VMEM((NY, 24, LANES), F32),
            pltpu.VMEM((NY, 24, LANES), F32),
            pltpu.VMEM((NZ, 32, LANES), BF16),
            pltpu.VMEM((NZ, 1, LANES), F32),
            pltpu.VMEM((32, LANES), F32),
            pltpu.VMEM((16, LANES), BF16),
            pltpu.VMEM((NY, 16, LANES), BF16),
            pltpu.VMEM((64, LANES), F32),
            pltpu.VMEM((NZ, 8, LANES), BF16),
            pltpu.VMEM((8, LANES), BF16),
            pltpu.VMEM((NZ, 8, LANES), F32),
            pltpu.VMEM((NZ, 8, LANES), F32),
            pltpu.VMEM((NY, 8, LANES), F32),
            pltpu.SemaphoreType.DMA((14,)),
            pltpu.SemaphoreType.DMA((PHASES,)),
            pltpu.SemaphoreType.DMA((PHASES,)),
            pltpu.SemaphoreType.REGULAR,
        ],
        compiler_params=pltpu.CompilerParams(
            collective_id=0, has_side_effects=True,
        ),
    )(
        residual, norm_gains,
        jnp.swapaxes(ffn_gate, 0, 1), jnp.swapaxes(ffn_up, 0, 1), jnp.swapaxes(ffn_down, 0, 1),
        proj_query, proj_key, proj_value, proj_out.T,
        head_lambda, head_gain.reshape(1, VDIM),
        cache_keys.reshape(batch, span, 128), cache_values.reshape(batch, span, VDIM), live_length,
    )
    return updated.astype(BF16)


def solution(mesh):
    split = Mesh(
        mesh.devices.reshape(mesh.shape["dp"], NZ, NY, mesh.shape["tp"]),
        ("dp", "kv_0", "kv_1", "tp"),
    )
    return jax.shard_map(
        local,
        mesh=split,
        in_specs=(
            P("dp", KV_TP),
            P(),
            P(None, KV_TP, None),
            P(None, KV_TP, None),
            P(None, KV_TP, None),
            P(KV, "tp"),
            P(KV, "tp"),
            P(KV, "tp"),
            P("tp", KV),
            P("tp"),
            P(),
            P("dp", KV, "tp", None),
            P("dp", KV, "tp", None),
            P("dp"),
        ),
        out_specs=P("dp", KV_TP),
        check_vma=False,
    )
```

```python
import functools

import jax
import jax.numpy as jnp
from jax import lax
from jax.experimental import pallas as pl
from jax.experimental.pallas import tpu as pltpu
from jax.sharding import Mesh
from jax.sharding import PartitionSpec as P

D = 2048
HEAD = 64
VDIM = 128
NZ = 16
NY = 4
NC = 2
NYC = NY * NC
LANES = 128
KV_TP = ("kv_0", "kv_1", "tp")
KV = ("kv_0", "kv_1")
MESH = pl.DeviceIdType.MESH
F32 = jnp.float32
BF16 = jnp.bfloat16
EPS = 1e-05
NT = (((1,), (1,)), ((), ()))

Z_STEPS = (8, 7, 9, 6, 10, 5, 11, 4, 12, 3, 13, 2, 14, 1, 15)
Y_STEPS = (2, 1, 3)
WEIGHT_ROWS = 48


def iota(shape, dim):
    return lax.broadcasted_iota(jnp.int32, shape, dim)


def mix_part(rows, gain, weights):
    scale = lax.rsqrt(jnp.mean(rows * rows, axis=1, keepdims=True) + EPS)
    normed = (rows * scale * gain).astype(BF16)
    gate = lax.dot_general(normed, weights[0], NT, preferred_element_type=F32)
    up = lax.dot_general(normed, weights[1], NT, preferred_element_type=F32)
    hidden = (gate / (1.0 + jnp.exp(-gate)) * up).astype(BF16)
    return 0.5 * jnp.dot(hidden, weights[2], preferred_element_type=F32)


def layer_kernel(
    res_h, gains_h, gate_h, up_h, down_h, wq_h, wk_h, wv_h, po_h, lam_h, hgain_h, ck_h, cv_h, live_h,
    out,
    res, gains, lam, hgain, live,
    raw, stage, wts, wqb, wkb, wvb, pob, lams, kbuf, vbuf,
    a1, a2, b1s, b1r, b2, cs, ckvs, csq, c2, ckv, own, c3s, d1s, d2o, d2m, hs, d3s, d3, ps, f2, fs, g1s, g1r, g2,
    hsem, ssem, rsem, hello,
):
    z = lax.axis_index("kv_0")
    y = lax.axis_index("kv_1")
    c = lax.axis_index("tp")
    hidden_rows = raw.shape[1]
    barrier = pltpu.get_barrier_semaphore()
    drains = []

    def z_peer(k):
        return lax.rem(z + k, NZ)

    def y_peer(k):
        return lax.rem(y + k, NY)

    def send(s, r, src, dst, device):
        pltpu.make_async_remote_copy(
            src_ref=src, dst_ref=dst, send_sem=ssem.at[s], recv_sem=rsem.at[r],
            device_id=device, device_id_type=MESH,
        ).start()

    def waits(s, r, ref):
        return pltpu.make_async_remote_copy(
            src_ref=ref, dst_ref=ref, send_sem=ssem.at[s], recv_sem=rsem.at[r],
            device_id={"kv_0": z}, device_id_type=MESH,
        )

    def arrive(r, ref):
        waits(r, r, ref).wait_recv()

    def drain(s, ref):
        drains.append(waits(s, s, ref))

    def signal(device):
        pl.semaphore_signal(barrier, inc=1, device_id=device, device_id_type=MESH)

    def to_z(phase, src_of, dst):
        for k in Z_STEPS:
            p = z_peer(k)
            send(phase, phase, src_of(p), dst.at[z], {"kv_0": p})

    def to_y(phase, src, dst):
        for k in Y_STEPS:
            send(phase, phase, src, dst, {"kv_1": y_peer(k)})

    def total(buf, count):
        acc = buf[0].astype(F32)
        for k in range(1, count):
            acc = acc + buf[k].astype(F32)
        return acc

    def load(k):
        if k < 3:
            return pltpu.make_async_copy((gate_h, up_h, down_h)[k], raw.at[k], hsem.at[k])
        src = (ck_h, cv_h, res_h, gains_h, lam_h, hgain_h, live_h)[k - 3]
        if k < 5:
            src = src.at[pl.ds(2 * y, 2)]
        return pltpu.make_async_copy(src, (kbuf.at[y * NC + 1], vbuf.at[y * NC + 1], res, gains, lam, hgain, live)[k - 3], hsem.at[k])

    def start_loads(which):
        for k in which:
            load(k).start()

    def own_tile():
        spread = (iota((16, LANES), 1) == iota((16, LANES), 0) + (y * NC + c) * 16).astype(F32).astype(BF16)
        return jnp.dot(res[...], spread, preferred_element_type=F32).astype(BF16)

    lane = iota((8, LANES), 1)
    row = iota((8, LANES), 0)

    def own_lambdas():
        head = row // 2
        return jnp.where(head == 0, lam[0], jnp.where(head == 1, lam[1], jnp.where(head == 2, lam[2], lam[3])))

    def attend():
        span = kbuf.shape[2]
        queries = [c3s[t].astype(F32) for t in range(NC)]
        cases = [(t, k, s) for t in range(NC) for k in range(NY) for s in range(2)]
        scores = jnp.concatenate(
            [
                lax.dot_general(
                    queries[t][s * 8 : s * 8 + 8].astype(BF16), kbuf[k * NC + t, s], NT, preferred_element_type=F32
                )
                for t, k, s in cases
            ],
            axis=0,
        ) * HEAD**-0.5
        place = z * NY * span + iota((8, span), 1)
        length = [live[2 * y], live[2 * y + 1]]
        alive = jnp.concatenate([(place + k * span < length[s]).astype(F32) for t, k, s in cases], axis=0) > 0.0
        highest = jnp.max(jnp.where(alive, scores, -1e30), axis=1, keepdims=True)
        terms = jnp.where(alive, jnp.exp(scores - highest), 0.0)
        weights = terms.astype(BF16)
        values = [
            jnp.dot(weights[b * 8 : b * 8 + 8], vbuf[k * NC + t, s], preferred_element_type=F32)
            for b, (t, k, s) in enumerate(cases)
        ]
        count = jnp.sum(terms, axis=1, keepdims=True)
        for b in range(0, len(cases), 2):
            t, k, _ = cases[b]
            pairs = [
                jnp.where(
                    lax.rem(lane, HEAD) < HEAD // 2, highest[a * 8 : a * 8 + 8], count[a * 8 : a * 8 + 8]
                )
                for a in (b, b + 1)
            ]
            d1s[t, k, 0:8, :] = values[b]
            d1s[t, k, 8:16, :] = values[b + 1]
            d1s[t, k, 16:24, :] = jnp.where(lane < HEAD, pairs[0], pairs[1])

    def give(phase, cache, buf, steps):
        for k in steps:
            p = y_peer(k)
            send(phase, phase, cache.at[pl.ds(2 * p, 2)], buf.at[y * NC + c], {"kv_1": p, "tp": 1})
        drain(phase, buf.at[pl.ds(0, len(steps))])

    def sent_all():
        for each in drains:
            each.wait_send()
        drains.clear()

    def finish(stream_two):
        updated = stream_two.astype(F32) + total(g2, NY)
        sent_all()
        out[...] = pltpu.roll(updated, lax.rem(LANES - (y * NC + c) * 16, LANES), 1)[:, :16]

    @pl.when(c == 0)
    def _():
        core1 = {"tp": 1}

        def all_core1(s, r, src, dst):
            for k in Y_STEPS + (0,):
                send(s, r, src, dst, {"kv_1": y_peer(k), "tp": 1})

        start_loads((5, 0, 1, 2, 7))
        load(5).wait()
        a1[y * NC] = own_tile()
        pl.semaphore_wait(barrier, NY)
        pl.semaphore_signal(hello, inc=1, device_id=core1, device_id_type=MESH)

        all_core1(A1, A1, a1.at[y * NC], a1.at[y * NC])
        drain(A1, a1.at[pl.ds(0, NY)])
        load(7).wait()
        lams[0] = own_lambdas()
        send(LAM, LAM, lams.at[0], lams.at[0], core1)
        drain(LAM, lams.at[0])
        stage[:, :, 40:WEIGHT_ROWS, :] = jnp.zeros((2, 3, WEIGHT_ROWS - 40, D), BF16)
        part = pl.ds(pl.multiple_of(y * 32, 32), 32)
        all_core1(WQ, WQ, wq_h, wqb.at[0, part])
        all_core1(WK, WK, wk_h, wkb.at[0, part])
        all_core1(WV, WV, wv_h, wvb.at[0, part])
        drain(WQ, wqb.at[0])
        drain(WK, wkb.at[0])
        drain(WV, wvb.at[0])
        for m in range(3):
            load(m).wait()

        @pl.loop(0, 3)
        def _(m):
            for half in range(2):
                stage[half, m, 0:hidden_rows, :] = raw.at[m][:, half, :]
                send(W0 + half, W0 + half, stage.at[half, m], wts.at[half, m, pl.ds(WEIGHT_ROWS, WEIGHT_ROWS)], core1)

        drain(W0, stage.at[0])
        drain(W1, stage.at[1])
        all_core1(WO, WO, po_h, pob.at[part, pl.ds(0, 512)])
        drain(WO, pob.at[:, pl.ds(0, 512)])
        give(KX, ck_h, kbuf, Y_STEPS + (0,))
        give(VX, cv_h, vbuf, Y_STEPS + (0,))

        sent_all()
        arrive(FS, fs)
        arrive(G2, g2)
        finish(fs[...])

    @pl.when(c == 1)
    def _():
        for k in Z_STEPS:
            signal({"kv_0": z_peer(k)})
        for k in Y_STEPS + (0,):
            signal({"kv_1": y_peer(k), "tp": 0})
        start_loads((5, 0, 1, 2, 7, 6, 8, 9, 3, 4))
        part = pl.ds(pl.multiple_of(y * 32, 32), 32)
        pulls = [
            pltpu.make_async_copy(wq_h, wqb.at[1, part], hsem.at[10]),
            pltpu.make_async_copy(wk_h, wkb.at[1, part], hsem.at[11]),
            pltpu.make_async_copy(wv_h, wvb.at[1, part], hsem.at[12]),
            pltpu.make_async_copy(po_h, pob.at[part, pl.ds(512, 512)], hsem.at[13]),
        ]
        for pull in pulls:
            pull.start()
        load(5).wait()
        a1[y * NC + 1] = own_tile()

        pl.semaphore_wait(hello, 1)

        to_y(A1, a1.at[y * NC + 1], a1.at[y * NC + 1])
        drain(A1, a1.at[pl.ds(0, NY - 1)])
        arrive(A1, a1.at[pl.ds(0, NYC - 1)])
        res_z = total(a1, NYC)
        a2[z] = res_z.astype(BF16)
        pl.semaphore_wait(barrier, NZ - 1)
        to_z(A2, lambda p: a2.at[z], a2)
        drain(A2, a2.at[pl.ds(0, NZ - 1)])
        to_y(WQ, wq_h, wqb.at[1, part])
        to_y(WK, wk_h, wkb.at[1, part])
        to_y(WV, wv_h, wvb.at[1, part])
        to_y(WO, po_h, pob.at[part, pl.ds(512, 512)])
        drain(WQ, wqb.at[1, pl.ds(0, 96)])
        drain(WK, wkb.at[1, pl.ds(0, 96)])
        drain(WV, wvb.at[1, pl.ds(0, 96)])
        drain(WO, pob.at[pl.ds(0, 96), pl.ds(512, 512)])
        give(KX, ck_h, kbuf, Y_STEPS)
        load(7).wait()
        lams[1] = own_lambdas()
        wts[:, :, 40:WEIGHT_ROWS, :] = jnp.zeros((2, 3, WEIGHT_ROWS - 40, D), BF16)
        for m in range(3):
            load(m).wait()

        @pl.loop(0, 3)
        def _(m):
            for half in range(2):
                wts[half, m, 0:hidden_rows, :] = raw.at[m][:, half, :]

        for k in (6, 8, 9):
            load(k).wait()
        for pull in pulls:
            pull.wait()
        arrive(W0, wts.at[0, :, pl.ds(WEIGHT_ROWS, WEIGHT_ROWS)])
        arrive(A2, a2.at[pl.ds(0, NZ - 1)])
        rows = jnp.concatenate([a2[k].astype(F32) for k in range(NZ)], axis=1)

        mixed = mix_part(rows, gains[0:1, :], [wts[0, m] for m in range(3)])
        for k in range(NZ):
            b1s[k] = mixed[:, k * LANES : (k + 1) * LANES]
        to_z(B1, lambda p: b1s.at[p], b1r)
        drain(B1, b1s.at[pl.ds(0, NZ - 1)])
        b1r[z] = b1s[z]
        arrive(B1, b1r.at[pl.ds(0, NZ - 1)])
        b2[y] = total(b1r, NZ)
        to_y(B2, b2.at[y], b2.at[y])
        drain(B2, b2.at[pl.ds(0, NY - 1)])
        give(VX, cv_h, vbuf, Y_STEPS)
        arrive(WQ, wqb.at[:, pl.ds(0, 112)])
        arrive(WK, wkb.at[:, pl.ds(0, 112)])
        arrive(WV, wvb.at[:, pl.ds(0, 112)])
        arrive(B2, b2.at[pl.ds(0, NY - 1)])
        stream_one = (res_z + total(b2, NY)).astype(BF16).astype(F32)

        gain_z = gains[1:2, pl.ds(pl.multiple_of(z * LANES, LANES), LANES)]
        scaled = (stream_one * gain_z).astype(BF16)
        query = [jnp.dot(scaled, wqb[t], preferred_element_type=F32) for t in range(2)]
        squares = jnp.sum(stream_one * stream_one, axis=1, keepdims=True)
        csq[z] = jnp.sum(jnp.where(lane == row, squares, 0.0), axis=0, keepdims=True)
        to_z(CQ, lambda p: csq.at[z], csq)
        for t in range(2):
            for g in range(4):
                cs[pl.ds(t * 4 + g, 8, stride=8), :] = query[t][:, g * LANES : (g + 1) * LANES]
        pair = pl.ds(pl.multiple_of(y * 16, 16), 16)
        to_z(C2, lambda p: cs.at[pair], c2)
        drain(CQ, csq.at[pl.ds(0, NZ - 1)])
        drain(C2, c2.at[pl.ds(0, NZ - 1)])
        c2[z] = cs[pair, :]
        for t in range(2):
            ckvs[pl.ds(t, 8, stride=4), :] = jnp.dot(scaled, wkb[t], preferred_element_type=F32)
            ckvs[pl.ds(2 + t, 8, stride=4), :] = jnp.dot(scaled, wvb[t], preferred_element_type=F32)
        pair_kv = pl.ds(pl.multiple_of(y * 8, 8), 8)
        owner = y * NY

        @pl.when(z != owner)
        def _():
            send(CKV, CKV, ckvs.at[pair_kv], ckv.at[z], {"kv_0": owner})

        arrive(CQ, csq.at[pl.ds(0, NZ - 1)])
        square_line = total(csq, NZ)
        arrive(C2, c2.at[pl.ds(0, NZ - 1)])
        sums = total(c2, NZ)
        query_rows, factors = [], []
        lane1 = iota((1, LANES), 1)
        for s in range(2):
            square = jnp.sum(jnp.where(lane1 == 2 * y + s, square_line, 0.0), axis=1, keepdims=True)
            factors.append(lax.rsqrt(square / D + EPS))
            block = (sums[s * 8 : (s + 1) * 8] * factors[s]).astype(BF16).astype(F32)
            for h in range(8):
                query_rows += [block[h : h + 1], block[h : h + 1]]
        row32 = iota((32, LANES), 0)
        lane32 = iota((32, LANES), 1)
        component = lax.rem(row32, 2)
        queries = jnp.where((lane32 >= HEAD) == (component == 1), jnp.concatenate(query_rows, axis=0), 0.0)
        for t in range(2):
            c3s[t] = jnp.concatenate(
                [queries[t * 8 : t * 8 + 8], queries[16 + t * 8 : 24 + t * 8]], axis=0
            ).astype(BF16)
        load(3).wait()
        load(4).wait()
        arrive(KX, kbuf.at[pl.ds(0, NYC - 1)])
        arrive(VX, vbuf.at[pl.ds(0, NYC - 1)])
        attend()

        @pl.when(z == owner)
        def _():
            ckv[z] = ckvs[pair_kv, :]
            arrive(CKV, ckv.at[pl.ds(0, NZ - 1)])
            sums = total(ckv, NZ)
            key_rows, value_rows = [], []
            for s in range(2):
                block = (sums[s * 4 : s * 4 + 4] * factors[s]).astype(BF16).astype(F32)
                for t in range(2):
                    key_rows.append(jnp.broadcast_to(block[t : t + 1], (8, LANES)))
                    value_rows.append(jnp.broadcast_to(block[2 + t : 3 + t], (8, LANES)))
            products = queries * jnp.concatenate(key_rows, axis=0)
            scores = jnp.sum(products, axis=1, keepdims=True) * HEAD**-0.5
            for t in range(2):
                pair = jnp.where(lane < HEAD, scores[t * 8 : t * 8 + 8], scores[16 + t * 8 : 24 + t * 8])
                own[t] = jnp.where(lax.rem(lane, HEAD) < HEAD // 2, pair, 1.0)
            for k in range(4):
                own[2 + k] = value_rows[k]

        @pl.when(z != owner)
        def _():
            for t in range(2):
                own[t] = jnp.where(lax.rem(lane, HEAD) < HEAD // 2, -1e30, 0.0)
            for k in range(4):
                own[2 + k] = jnp.zeros((8, LANES), F32)

        arrive(LAM, lams.at[0])
        arrive(WO, pob.at[pl.ds(0, 112)])
        arrive(W1, wts.at[1, :, pl.ds(WEIGHT_ROWS, WEIGHT_ROWS)])

        is_top = lax.rem(lane, HEAD) < HEAD // 2
        joined, line = [[], []], jnp.zeros((1, LANES), F32)
        for t in range(2):
            stats = [d1s[t, k, 16:24, :] for k in range(NY)] + [own[t]]
            blocks = [[d1s[t, k, s * 8 : s * 8 + 8, :] for s in range(2)] for k in range(NY)]
            blocks += [[own[2 + t], own[4 + t]]]
            top = functools.reduce(jnp.maximum, stats)
            weights = [jnp.where(is_top, jnp.exp(jnp.where(is_top, each - top, 0.0)), 0.0) for each in stats]
            count = functools.reduce(
                jnp.add, [pltpu.roll(w, HEAD // 2, 1) * each for w, each in zip(weights, stats)]
            )
            packed = jnp.where(is_top, top, count)
            line += jnp.sum(jnp.where(lax.rem(lane, HEAD // 2) == row + t * 8, packed, 0.0), axis=0, keepdims=True)
            for s in range(2):
                joined[s].append(
                    functools.reduce(
                        jnp.add, [w[:, s * HEAD : s * HEAD + 1] * each[s] for w, each in zip(weights, blocks)]
                    )
                )
        d2m[z] = line
        d2o[z] = jnp.concatenate(joined[0] + joined[1], axis=0).astype(BF16)
        to_z(D2M, lambda p: d2m.at[z], d2m)
        to_z(D2O, lambda p: d2o.at[z], d2o)
        drain(D2M, d2m.at[pl.ds(0, NZ - 1)])
        drain(D2O, d2o.at[pl.ds(0, NZ - 1)])
        arrive(D2M, d2m.at[pl.ds(0, NZ - 1)])
        spot = row32 // 16 * HEAD + lax.rem(row32, 16)
        tops = [jnp.sum(jnp.where(lane32 == spot, d2m[k], 0.0), axis=1, keepdims=True) for k in range(NZ)]
        counts = [
            jnp.sum(jnp.where(lane32 == spot + HEAD // 2, d2m[k], 0.0), axis=1, keepdims=True) for k in range(NZ)
        ]
        top = functools.reduce(jnp.maximum, tops)
        weights = [jnp.exp(t - top) for t in tops]
        count = functools.reduce(jnp.add, [w * s for w, s in zip(weights, counts)])
        arrive(D2O, d2o.at[pl.ds(0, NZ - 1)])
        values = functools.reduce(jnp.add, [weights[k] * d2o[k].astype(F32) for k in range(NZ)])
        ratio = values / count
        lambdas = jnp.concatenate([lams[0], lams[1], lams[0], lams[1]], axis=0)
        mixed = ratio - lambdas * pltpu.roll(ratio, 31, 0)
        scale = lax.rsqrt(jnp.mean(mixed * mixed, axis=1, keepdims=True) + EPS)
        hs[...] = mixed * scale * hgain[...]
        d3s[...] = hs[pl.ds(0, 16, stride=2), :].astype(BF16)
        to_y(D3, d3s, d3.at[y])
        drain(D3, d3.at[pl.ds(0, NY - 1)])
        d3[y] = d3s[...]
        arrive(D3, d3.at[pl.ds(0, NY - 1)])

        for k in range(NY):
            ps[k * 16 : (k + 1) * 16, :] = d3[k].astype(F32)
        heads = jnp.concatenate([ps[pl.ds(h, 8, stride=8), :] for h in range(8)], axis=1).astype(BF16)
        projected = lax.dot_general(heads, pob[...], NT, preferred_element_type=F32)
        stream_two = (stream_one + projected).astype(BF16)
        f2[z] = stream_two
        fs[...] = stream_two
        to_z(F2, lambda p: f2.at[z], f2)
        drain(F2, f2.at[pl.ds(0, NZ - 1)])
        send(FS, FS, fs, fs, {"tp": 0})
        drain(FS, fs)
        arrive(F2, f2.at[pl.ds(0, NZ - 1)])
        rows = jnp.concatenate([f2[k].astype(F32) for k in range(NZ)], axis=1)

        mixed = mix_part(rows, gains[2:3, :], [wts[1, m] for m in range(3)])
        for k in range(NZ):
            g1s[k] = mixed[:, k * LANES : (k + 1) * LANES]
        to_z(G1, lambda p: g1s.at[p], g1r)
        drain(G1, g1s.at[pl.ds(0, NZ - 1)])
        g1r[z] = g1s[z]
        arrive(G1, g1r.at[pl.ds(0, NZ - 1)])
        g2[y] = total(g1r, NZ)
        for k in Y_STEPS:
            send(G2S, G2, g2.at[y], g2.at[y], {"kv_1": y_peer(k), "tp": 0})
            send(G2, G2, g2.at[y], g2.at[y], {"kv_1": y_peer(k)})
        send(G2S, G2, g2.at[y], g2.at[y], {"tp": 0})
        sent_all()

        @pl.when(z != owner)
        def _():
            waits(CKV, CKV, ckv.at[0]).wait_send()

        drain(G2S, g2)
        drain(G2, g2.at[pl.ds(0, NY - 1)])
        arrive(G2, g2.at[pl.ds(0, NY - 1)])
        finish(stream_two)


PHASES = 24
(
    A1, A2, B1, B2, CQ, C2, CKV, D2O, D2M, D3, F2, FS, G1, G2, G2S, LAM, W0, W1, WQ, WK, WV, WO, KX, VX,
) = range(24)


def local(
    residual, norm_gains, ffn_gate, ffn_up, ffn_down, proj_query, proj_key, proj_value, proj_out,
    head_lambda, head_gain, cache_keys, cache_values, live_length,
):
    batch = residual.shape[0]
    hidden = ffn_gate.shape[1]
    span = cache_keys.shape[1]
    vmem = pl.BlockSpec(memory_space=pltpu.VMEM)
    hbm = pl.BlockSpec(memory_space=pl.ANY)
    updated = pl.pallas_call(
        layer_kernel,
        out_shape=pltpu.VMEM(residual.shape, F32),
        in_specs=[hbm] * 14,
        out_specs=vmem,
        scratch_shapes=[
            pltpu.VMEM(residual.shape, BF16),
            pltpu.VMEM(norm_gains.shape, F32),
            pltpu.SMEM(head_lambda.shape, F32),
            pltpu.VMEM((1, VDIM), F32),
            pltpu.SMEM(live_length.shape, jnp.int32),
            pltpu.VMEM((3, hidden, 2, D), BF16),
            pltpu.VMEM((2, 3, WEIGHT_ROWS, D), BF16),
            pltpu.VMEM((2, 3, 2 * WEIGHT_ROWS, D), BF16),
            pltpu.VMEM((2, LANES, 512), BF16),
            pltpu.VMEM((2, LANES, 128), BF16),
            pltpu.VMEM((2, LANES, 128), BF16),
            pltpu.VMEM((LANES, 1024), BF16),
            pltpu.VMEM((2, 8, LANES), F32),
            pltpu.VMEM((NYC, batch // NY, span, 128), BF16),
            pltpu.VMEM((NYC, batch // NY, span, VDIM), BF16),
            pltpu.VMEM((NYC, 8, LANES), BF16),
            pltpu.VMEM((NZ, 8, LANES), BF16),
            pltpu.VMEM((NZ, 8, LANES), F32),
            pltpu.VMEM((NZ, 8, LANES), F32),
            pltpu.VMEM((NY, 8, LANES), F32),
            pltpu.VMEM((64, LANES), F32),
            pltpu.VMEM((32, LANES), F32),
            pltpu.VMEM((NZ, 1, LANES), F32),
            pltpu.VMEM((NZ, 16, LANES), F32),
            pltpu.VMEM((NZ, 8, LANES), F32),
            pltpu.VMEM((6, 8, LANES), F32),
            pltpu.VMEM((2, 16, LANES), BF16),
            pltpu.VMEM((NC, NY, 24, LANES), F32),
            pltpu.VMEM((NZ, 32, LANES), BF16),
            pltpu.VMEM((NZ, 1, LANES), F32),
            pltpu.VMEM((32, LANES), F32),
            pltpu.VMEM((16, LANES), BF16),
            pltpu.VMEM((NY, 16, LANES), BF16),
            pltpu.VMEM((64, LANES), F32),
            pltpu.VMEM((NZ, 8, LANES), BF16),
            pltpu.VMEM((8, LANES), BF16),
            pltpu.VMEM((NZ, 8, LANES), F32),
            pltpu.VMEM((NZ, 8, LANES), F32),
            pltpu.VMEM((NY, 8, LANES), F32),
            pltpu.SemaphoreType.DMA((14,)),
            pltpu.SemaphoreType.DMA((PHASES,)),
            pltpu.SemaphoreType.DMA((PHASES,)),
            pltpu.SemaphoreType.REGULAR,
        ],
        compiler_params=pltpu.CompilerParams(
            collective_id=0, has_side_effects=True,
        ),
    )(
        residual, norm_gains,
        jnp.swapaxes(ffn_gate, 0, 1), jnp.swapaxes(ffn_up, 0, 1), jnp.swapaxes(ffn_down, 0, 1),
        proj_query, proj_key, proj_value, proj_out.T,
        head_lambda, head_gain.reshape(1, VDIM),
        cache_keys.reshape(batch, span, 128), cache_values.reshape(batch, span, VDIM), live_length,
    )
    return updated.astype(BF16)


def solution(mesh):
    split = Mesh(
        mesh.devices.reshape(mesh.shape["dp"], NZ, NY, mesh.shape["tp"]),
        ("dp", "kv_0", "kv_1", "tp"),
    )
    return jax.shard_map(
        local,
        mesh=split,
        in_specs=(
            P("dp", KV_TP),
            P(),
            P(None, KV_TP, None),
            P(None, KV_TP, None),
            P(None, KV_TP, None),
            P(KV, "tp"),
            P(KV, "tp"),
            P(KV, "tp"),
            P("tp", KV),
            P("tp"),
            P(),
            P("dp", KV, "tp", None),
            P("dp", KV, "tp", None),
            P("dp"),
        ),
        out_specs=P("dp", KV_TP),
        check_vma=False,
    )
```
